512 devices in a mesh: sp: 128 (over z, x, core), tp: 4 (over y).
Axes of the slice: x: 4, y: 4, z: 16, core: 2. Of those that a mesh axis runs over, the one named last changes fastest.
Arguments:
- inputs: bfloat16 [4, 16384, 1024], P(None, 'sp'), may hold values from -6 to 6
- norm_gain: float32 [1024], replicated, may hold values from 0.1 to 1.9
- query_weight: bfloat16 [1024, 3, 8, 64], P('sp', None, 'tp'), may hold values from -0.1875 to 0.1875
- key_weight: bfloat16 [1024, 3, 8, 64], P('sp', None, 'tp'), may hold values from -0.1875 to 0.1875
- value_weight: bfloat16 [1024, 3, 8, 64], P('sp', None, 'tp'), may hold values from -0.1875 to 0.1875
- query_gain: float32 [3, 64], replicated, may hold values from 0.1 to 1.9
- key_gain: float32 [3, 64], replicated, may hold values from 0.1 to 1.9
- out_weight: bfloat16 [8, 64, 1024], P('tp', None, 'sp'), may hold values from -0.75 to 0.75
Outputs:
- mixed: bfloat16 [4, 16384, 1024], P(None, 'sp', 'tp')
The draws below stay inside these ranges and needn't reach their ends.
All inputs are finite; a program needn't handle non-finite values.
Results may differ from the reference program's by a relative error of at most 0.02.
Values may be sent and summed in bfloat16 or wider, within the bound.
A program may use at most 64 MiB of HBM per device.

```python
import math
import jax
import jax.numpy as jnp
from jax import lax

D = 1024
GROUPS = 3
HPG = 8
DH = 64
BATCH = 4
SPAN_CLOSE = 32
SPREAD_CENTRAL = 4
SPAN_CENTRAL = 32
SPREAD_DISTANT = 16
SPAN_DISTANT = 16
TOKENS = 16384


def level_of(key, dims, split, least, largest):
    def one(position, shards_of):
        heights = jax.random.uniform(jax.random.fold_in(jax.random.fold_in(key, 6), position), (shards_of,), jnp.float32, least / len(split), largest / len(split))
        return jnp.repeat(jnp.exp(heights), dims[position] // shards_of).reshape((-1,) + (1,) * (len(dims) - position - 1))

    factor_of = one(*split[0])
    for cut in split[1:]:
        factor_of = factor_of * one(*cut)
    return factor_of


def centred(key, extent, deviation, bound, cuts=(), kind=jnp.bfloat16):
    drawn = deviation * jax.random.normal(key, extent, jnp.float32)
    if cuts:
        drawn = drawn * level_of(key, extent, cuts, -0.22, 0.18)
    return jnp.clip(drawn, -bound, bound).astype(kind)


def setup_inputs(seed: int = 0) -> dict:
    key_of = jax.random.split(jax.random.key(seed), 9)
    inputs = centred(key_of[0], (BATCH, TOKENS, D), 1.0, 6.0, ((1, 128),))
    norm_gain = jnp.clip(1.0 + 0.18 * jax.random.normal(key_of[1], (D,), jnp.float32), 0.1, 1.9)
    query_weight = centred(key_of[2], (D, GROUPS, HPG, DH), D ** -0.5, 0.1875, ((0, 128), (2, 4)))
    key_weight = centred(key_of[3], (D, GROUPS, HPG, DH), D ** -0.5, 0.1875, ((0, 128), (2, 4)))
    value_weight = centred(key_of[4], (D, GROUPS, HPG, DH), D ** -0.5, 0.1875, ((0, 128), (2, 4)))
    query_gain = jnp.clip(1.0 + 0.18 * jax.random.normal(key_of[5], (GROUPS, DH), jnp.float32), 0.1, 1.9)
    key_gain = jnp.clip(1.0 + 0.18 * jax.random.normal(key_of[6], (GROUPS, DH), jnp.float32), 0.1, 1.9)
    out_weight = centred(key_of[7], (HPG, DH, D), DH ** -0.5, 0.75, ((0, 4), (2, 128)))
    return dict(inputs=inputs, norm_gain=norm_gain, query_weight=query_weight, key_weight=key_weight, value_weight=value_weight, query_gain=query_gain, key_gain=key_gain, out_weight=out_weight)


eps = 1e-06
neg_fill = -1e+30
block_rows = 128

def row_norm(values, gain):
    scaled = values * lax.rsqrt(lax.optimization_barrier(jnp.mean(values * values, axis=-1, keepdims=True)) + eps)
    return scaled * gain

def band_attend(queries, keys, values, dilation, half, slopes):
    seq_len, heads, width = queries.shape
    sub_len = seq_len // dilation

    def to_sub(tensor):
        return tensor.reshape(sub_len, dilation, heads, width).transpose(1, 0, 2, 3)
    query_sub = to_sub(queries)
    key_sub = to_sub(keys)
    value_sub = to_sub(values)
    blocks = -(-sub_len // block_rows)
    padded_len = blocks * block_rows
    key_rows = block_rows + 2 * half
    query_sub = jnp.pad(query_sub, ((0, 0), (0, padded_len - sub_len), (0, 0), (0, 0)))
    key_pad = ((0, 0), (half, padded_len - sub_len + half), (0, 0), (0, 0))
    key_sub = jnp.pad(key_sub, key_pad)
    value_sub = jnp.pad(value_sub, key_pad)
    key_index = jnp.arange(blocks)[:, None] * block_rows + jnp.arange(key_rows)[None, :]
    key_blocks = key_sub[:, key_index]
    value_blocks = value_sub[:, key_index]
    query_blocks = query_sub.reshape(dilation, blocks, block_rows, heads, width)
    scores = jnp.einsum('nbqhe,nbkhe->nbhqk', query_blocks, key_blocks, precision=lax.Precision.HIGHEST) / math.sqrt(width)
    offset = jnp.arange(key_rows)[None, :] - half - jnp.arange(block_rows)[:, None]
    key_place = key_index - half
    allowed = (jnp.abs(offset)[None] <= half) & ((key_place >= 0) & (key_place < sub_len))[:, None, :]
    slant = -slopes[:, None, None] * (jnp.abs(offset).astype(jnp.float32) / float(half))[None]
    scores = jnp.where(allowed[None, :, None], scores + slant[None, None], neg_fill)
    log_total = jax.nn.logsumexp(scores, axis=-1)
    weights = jnp.exp(scores - log_total[..., None])
    result = jnp.einsum('nbhqk,nbkhe->nbqhe', weights, value_blocks, precision=lax.Precision.HIGHEST).reshape(dilation, padded_len, heads, width)[:, :sub_len]
    log_total = log_total.transpose(0, 1, 3, 2).reshape(dilation, padded_len, heads)[:, :sub_len]
    result = result.transpose(1, 0, 2, 3).reshape(seq_len, heads, width)
    log_total = log_total.transpose(1, 0, 2).reshape(seq_len, heads)
    return (result, log_total)

def reference(inputs, norm_gain, query_weight, key_weight, value_weight, query_gain, key_gain, out_weight):
    batch, seq_len, model_width = inputs.shape
    groups = query_weight.shape[1]
    heads = query_weight.shape[2]
    head_width = query_weight.shape[3]
    normed = row_norm(inputs.astype(jnp.float32), norm_gain).astype(jnp.bfloat16)
    normed = normed.reshape(batch * seq_len, model_width)

    def project(weight):
        product = jnp.dot(normed, weight.reshape(model_width, -1), preferred_element_type=jnp.float32)
        return product.astype(jnp.bfloat16).reshape(batch, seq_len, groups, heads, head_width)
    queries = project(query_weight)
    keys = project(key_weight)
    values = project(value_weight)
    slopes = jnp.exp2(-8.0 * jnp.arange(1, heads + 1).astype(jnp.float32) / heads)
    gap_layouts = ((1, SPAN_CLOSE), (SPREAD_CENTRAL, SPAN_CENTRAL), (SPREAD_DISTANT, SPAN_DISTANT))
    results = []
    totals = []
    for group in range(3):
        dilation, half = gap_layouts[group]
        query_group = row_norm(queries[:, :, group].astype(jnp.float32), query_gain[group])
        key_group = row_norm(keys[:, :, group].astype(jnp.float32), key_gain[group])
        value_group = values[:, :, group].astype(jnp.float32)

        def attend_one(trio, dilation=dilation, half=half):
            return band_attend(trio[0], trio[1], trio[2], dilation, half, slopes)
        result, log_total = lax.map(attend_one, (query_group, key_group, value_group))
        results.append(result)
        totals.append(log_total)
    weights = jax.nn.softmax(jnp.stack(totals, 0), axis=0)
    combined = lax.optimization_barrier(jnp.sum(weights[..., None] * jnp.stack(results, 0), axis=0))
    merged = combined.astype(jnp.bfloat16).reshape(batch * seq_len, heads * head_width)
    output = jnp.dot(merged, out_weight.reshape(heads * head_width, model_width), preferred_element_type=jnp.float32)
    return output.astype(jnp.bfloat16).reshape(batch, seq_len, model_width)
```

```python
import functools
import math

import jax
import jax.numpy as jnp
from jax import lax
from jax.experimental import pallas as pl
from jax.experimental.pallas import tpu as pltpu
from jax.sharding import PartitionSpec as P

GAPS = ((1, 32), (4, 32), (16, 16))
REACH = tuple(d * h for d, h in GAPS)
EPS = 1e-06
NEG = -1e30
LOG2E = 1.4426950408889634
MESH = pl.DeviceIdType.MESH
NZ, NX = 16, 4
CHIPS = NZ * NX
WA, WB = 384, 256


def layer_kernel(
    tp, batch, length, x_ref, gain_ref, slab_ref, qg_ref, kg_ref, out_ref,
    wa, wb, wk, wq, nb, win0, win1, win2, qn, bias, osum, oown, orecv, wo, mown, msend, mrecv, mg,
    pair_send, pair_recv, local_sem, z_send, z_recv, x_send, x_recv, nb_send, nb_recv, halo_send, halo_recv,
    o_send, o_recv, oy_send, oy_recv, m_send, m_recv, y_send, y_recv,
):
    me = lax.axis_index("sp")
    mine = lax.axis_index("tp")
    groups = len(GAPS)
    core = me % 2
    other = 1 - core
    chip = me // 2
    x = chip % NX
    z = chip // NX
    rows = 2 * length
    wins = (win0, win1, win2)
    bufs = (wa, wb)

    def at_z(offset):
        return {"sp": (((z + offset + NZ) % NZ) * NX + x) * 2 + core}

    def at_x(offset):
        return {"sp": (z * NX + (x + offset) % NX) * 2 + core}

    sibling = {"sp": chip * 2 + other}

    def at_chip(offset):
        return {"sp": ((chip + offset + CHIPS) % CHIPS) * 2 + core}

    def at_y(offset):
        return {"tp": (mine + offset) % tp}

    barrier = pltpu.get_barrier_semaphore()

    def greet(target):
        pl.semaphore_signal(barrier, inc=1, device_id=target, device_id_type=MESH)

    targets = [at_z(o) for o in (-3, 3, -2, 2, -1, 1)] + [at_y(o) for o in range(1, tp)]
    targets += [at_x(o) for o in range(1, NX)] + [at_chip(1), at_chip(-1), sibling]
    for target in targets:
        greet(target)
    pl.semaphore_wait(barrier, len(targets))

    cuts = (pl.ds(0, WA), pl.ds(WA, WB))

    def pair(chunk):
        return pltpu.make_async_remote_copy(
            src_ref=slab_ref.at[other, :, cuts[chunk]],
            dst_ref=bufs[chunk].at[chip, core],
            send_sem=pair_send.at[chunk],
            recv_sem=pair_recv.at[chunk],
            device_id=sibling,
            device_id_type=MESH,
        )

    def local(chunk):
        return pltpu.make_async_copy(
            slab_ref.at[core, :, cuts[chunk]], bufs[chunk].at[chip, core], local_sem.at[chunk]
        )

    def z_copy(chunk, origin, step):
        index = ((z + origin + NZ) % NZ) * NX + x
        rel = (origin - step) % NZ
        block = bufs[chunk].at[index]
        return pltpu.make_async_remote_copy(
            src_ref=block,
            dst_ref=block,
            send_sem=z_send.at[chunk, rel],
            recv_sem=z_recv.at[chunk, rel],
            device_id=at_z(step),
            device_id_type=MESH,
        )

    def z_wait(chunk, origin):
        index = ((z + origin + NZ) % NZ) * NX + x
        block = bufs[chunk].at[index]
        pltpu.make_async_remote_copy(
            src_ref=block,
            dst_ref=block,
            send_sem=z_send.at[chunk, origin % NZ],
            recv_sem=z_recv.at[chunk, origin % NZ],
            device_id=at_z(1),
            device_id_type=MESH,
        ).wait_recv()

    sends = []

    def z_start(chunk, origin, step):
        copy = z_copy(chunk, origin, step)
        copy.start()
        sends.append(copy)

    def x_copy(chunk, origin, shift):
        block = bufs[chunk].at[((z + origin + NZ) % NZ) * NX + x]
        return pltpu.make_async_remote_copy(
            src_ref=block,
            dst_ref=block,
            send_sem=x_send.at[chunk, origin % NZ, shift - 1],
            recv_sem=x_recv.at[chunk, origin % NZ, shift - 1],
            device_id=at_x(shift),
            device_id_type=MESH,
        )

    def x_start(chunk, origin):
        for shift in (1, 3, 2):
            copy = x_copy(chunk, origin, shift)
            copy.start()
            sends.append(copy)

    def x_wait(chunk, origin, shift):
        block = bufs[chunk].at[((z + origin + NZ) % NZ) * NX + (x + NX - shift) % NX]
        pltpu.make_async_remote_copy(
            src_ref=block,
            dst_ref=block,
            send_sem=x_send.at[chunk, origin % NZ, shift - 1],
            recv_sem=x_recv.at[chunk, origin % NZ, shift - 1],
            device_id=at_x(1),
            device_id_type=MESH,
        ).wait_recv()

    for chunk in range(2):
        local(chunk).start()
        pair(chunk).start()
    for chunk in range(2):
        local(chunk).wait()
        pair(chunk).wait_recv()
        for step in (3, -3, 2, -2, 1, -1):
            z_start(chunk, 0, step)
    x_start(0, 0)

    def nb_copy(b):
        return pltpu.make_async_remote_copy(
            src_ref=nb.at[b, core],
            dst_ref=nb.at[b, core],
            send_sem=nb_send.at[b],
            recv_sem=nb_recv.at[b],
            device_id=sibling,
            device_id_type=MESH,
        )

    def norm_step(b, carry):
        flat = x_ref[b].astype(jnp.float32)
        scale = lax.rsqrt(jnp.mean(flat * flat, axis=-1, keepdims=True) + EPS)
        nb[b, core] = (flat * scale * gain_ref[...]).astype(jnp.bfloat16)
        nb_copy(b).start()
        return carry

    lax.fori_loop(0, batch, norm_step, 0)

    def relay(chunk, origin, spread):
        z_wait(chunk, origin)
        if origin in (3, 6):
            for step in (-3, -2, -1) if origin == 3 else (-1,) + ((-2,) if chunk == 1 else ()):
                z_start(chunk, origin, step)
        if origin in (-3, -6):
            for step in (3, 2, 1) if origin == -3 else (1,) + ((2,) if chunk == 0 else ()):
                z_start(chunk, origin, step)
        if spread:
            x_start(chunk, origin)

    for origin in (1, -1, 2, -2):
        relay(0, origin, True)
    for chunk in range(2):
        for origin in (3, -3):
            relay(chunk, origin, chunk == 0)

    head = mine * 2 + core
    heads = 2 * tp
    power = -8.0 * (head + 1).astype(jnp.float32) / heads
    slope = jnp.exp2(jnp.full((8, 128), power, jnp.float32))[:1, :1] * LOG2E
    widths = [length + 2 * r for r in REACH]
    starts = [sum(widths[:g]) for g in range(groups)]
    total_rows = CHIPS * rows

    def bias_step(block, carry):
        for group, (dilation, half) in enumerate(GAPS):
            reach = REACH[group]
            shape = (length, widths[group])
            key = lax.broadcasted_iota(jnp.int32, shape, 1) - reach
            offset = jnp.abs(key - lax.broadcasted_iota(jnp.int32, shape, 0))
            at = key + (chip * rows + block * length)
            allowed = (offset <= reach) & (at >= 0) & (at < total_rows) & ((offset & (dilation - 1)) == 0)
            value = jnp.where(allowed, offset.astype(jnp.float32) * (-slope / float(reach)), NEG)
            bias[block, :, starts[group] : starts[group] + widths[group]] = value
        return carry

    lax.fori_loop(0, 2, bias_step, 0)

    for origin in (4, -4, 5, -5):
        relay(0, origin, True)
    for chunk in range(2):
        for origin in (6, -6):
            relay(chunk, origin, chunk == 0)
    for origin in (7, -7, 8):
        relay(0, origin, True)
    x_start(1, 0)
    for origin in (3, -3, 6, -6):
        x_start(1, origin)
    for origin in (1, -1, 2, -2, 4, -4, 5, -5, 7, -7, 8):
        relay(1, origin, True)

    lane = lax.broadcasted_iota(jnp.int32, (rows, 128), 1)
    low = lane < 64

    def all_origins(chunk):
        for origin in (0, 1, -1, 2, -2, 3, -3, 4, -4, 5, -5, 6, -6, 7, -7, 8):
            for shift in (1, 3, 2):
                x_wait(chunk, origin, shift)

    all_origins(0)
    wk[...] = wa[...].reshape(2 * CHIPS * 8, WA)
    for b in range(batch):
        nb_copy(b).wait_recv()

    def halo(b, group, up):
        reach = REACH[group]
        win = wins[group]
        if up:
            src = win.at[b, pl.ds(rows, reach), :]
            dst = win.at[b, pl.ds(0, reach), :]
        else:
            src = win.at[b, pl.ds(reach, reach), :]
            dst = win.at[b, pl.ds(reach + rows, reach), :]
        return pltpu.make_async_remote_copy(
            src_ref=src,
            dst_ref=dst,
            send_sem=halo_send.at[b, group, 0 if up else 1],
            recv_sem=halo_recv.at[b, group, 0 if up else 1],
            device_id=at_chip(1 if up else -1),
            device_id_type=MESH,
        )

    def each_halo(b):
        return [halo(b, group, up) for group in (2, 1, 0) for up in (True, False)]

    ones = jnp.ones((1, 64), jnp.float32)
    zeros = jnp.zeros((1, 64), jnp.float32)

    def kv_step(b, carry):
        out = jnp.dot(nb[b].reshape(rows, -1), wk[...], preferred_element_type=jnp.float32)
        out = out.astype(jnp.bfloat16).astype(jnp.float32)
        for group in range(groups):
            seg = out[:, 128 * group : 128 * (group + 1)]
            mean = jnp.sum(jnp.where(low, seg * seg, 0.0), axis=-1, keepdims=True) / 64.0
            gain = jnp.concatenate([kg_ref[group : group + 1, :], ones], axis=1)
            scaled = seg * jnp.where(low, lax.rsqrt(mean + EPS), 1.0) * gain
            wins[group][b, REACH[group] : REACH[group] + rows, :] = scaled.astype(jnp.bfloat16)
        for copy in each_halo(b):
            copy.start()
        return carry

    lax.fori_loop(0, batch, kv_step, 0)

    all_origins(1)
    wq[...] = wb[...].reshape(2 * CHIPS * 8, WB)

    tile = wq[:, 128:].astype(jnp.float32)
    high = lax.broadcasted_iota(jnp.int32, tile.shape, 1) >= 64
    tile = jnp.where(high, tile, 0.0)
    tile = jnp.where(core == 0, pltpu.roll(tile, 64, 1), tile)
    oown[...] = tile.astype(jnp.bfloat16)
    o_pair = pltpu.make_async_remote_copy(
        src_ref=oown,
        dst_ref=orecv,
        send_sem=o_send.at[0],
        recv_sem=o_recv.at[0],
        device_id=sibling,
        device_id_type=MESH,
    )
    o_pair.start()

    factor = LOG2E / 8.0

    def q_step(b, carry):
        out = jnp.dot(nb[b].reshape(rows, -1), wq[...], preferred_element_type=jnp.float32)
        out = out.astype(jnp.bfloat16).astype(jnp.float32)
        first, second = out[:, :128], out[:, 128:]
        for group, seg, here in ((0, first, low), (1, first, ~low), (2, second, low)):
            mean = jnp.sum(jnp.where(here, seg * seg, 0.0), axis=-1, keepdims=True) / 64.0
            gain = qg_ref[group : group + 1, :] * factor
            gain = jnp.concatenate([zeros, gain] if group == 1 else [gain, zeros], axis=1)
            scaled = jnp.where(here, seg * lax.rsqrt(mean + EPS) * gain, 0.0)
            if group == 1:
                scaled = pltpu.roll(scaled, 64, 1)
            qn[group, b] = scaled.astype(jnp.bfloat16)
        return carry

    lax.fori_loop(0, batch, q_step, 0)

    span = wo.shape[1]
    o_pair.wait_recv()
    osum[...] = (oown[...] + orecv[...]).reshape(osum.shape)
    wo[mine] = osum[mine]

    def o_copy(shift):
        target = (mine + shift) % tp
        return pltpu.make_async_remote_copy(
            src_ref=osum.at[target],
            dst_ref=wo.at[mine],
            send_sem=oy_send.at[shift - 1],
            recv_sem=oy_recv.at[shift - 1],
            device_id=at_y(shift),
            device_id_type=MESH,
        )

    def o_wait(shift):
        pltpu.make_async_remote_copy(
            src_ref=osum.at[mine],
            dst_ref=wo.at[(mine + tp - shift) % tp],
            send_sem=oy_send.at[shift - 1],
            recv_sem=oy_recv.at[shift - 1],
            device_id=at_y(shift),
            device_id_type=MESH,
        ).wait_recv()

    for shift in range(1, tp):
        o_copy(shift).start()

    keep = lax.broadcasted_iota(jnp.int32, (length, 128), 1) >= 64

    def attend(b, block):
        total = jnp.zeros((length, 1), jnp.float32)
        summed = jnp.zeros((length, 128), jnp.float32)
        begin = pl.multiple_of(block * length, length)
        for group in range(groups):
            query = qn[group, b, pl.ds(begin, length), :]
            window = wins[group][b, pl.ds(begin, widths[group]), :]
            scores = lax.dot_general(query, window, (((1,), (1,)), ((), ())), preferred_element_type=jnp.float32)
            grown = jnp.exp2(scores + bias[block, :, starts[group] : starts[group] + widths[group]])
            total = total + jnp.sum(grown, axis=-1, keepdims=True)
            summed = summed + jnp.dot(grown.astype(jnp.bfloat16), window, preferred_element_type=jnp.float32)
        merged = jnp.where(keep, summed / total, 0.0)
        return jnp.where(core == 0, pltpu.roll(merged, 64, 1), merged).astype(jnp.bfloat16)

    def m_copy(b):
        return pltpu.make_async_remote_copy(
            src_ref=msend.at[b],
            dst_ref=mrecv.at[b],
            send_sem=m_send.at[b],
            recv_sem=m_recv.at[b],
            device_id=sibling,
            device_id_type=MESH,
        )

    def y_copy(b, shift):
        return pltpu.make_async_remote_copy(
            src_ref=mg.at[mine, b],
            dst_ref=mg.at[mine, b],
            send_sem=y_send.at[b, shift - 1],
            recv_sem=y_recv.at[b, shift - 1],
            device_id=at_y(shift),
            device_id_type=MESH,
        )

    def y_wait(b, shift):
        block = mg.at[(mine + tp - shift) % tp, b]
        pltpu.make_async_remote_copy(
            src_ref=block,
            dst_ref=block,
            send_sem=y_send.at[b, shift - 1],
            recv_sem=y_recv.at[b, shift - 1],
            device_id=at_y(shift),
            device_id_type=MESH,
        ).wait_recv()

    def pass_on(b):
        m_copy(b).wait_recv()
        mg[mine, b] = mown[b] + mrecv[b]
        for shift in range(1, tp):
            y_copy(b, shift).start()

    def attend_step(b, carry):
        for copy in each_halo(b):
            copy.wait_recv()
        msend[b] = attend(b, other)
        m_copy(b).start()

        @pl.when(b >= 1)
        def _():
            pass_on(b - 1)

        mown[b] = attend(b, core)
        return carry

    lax.fori_loop(0, batch, attend_step, 0)
    pass_on(batch - 1)
    for shift in range(1, tp):
        o_wait(shift)

    def finish(b, carry):
        for shift in range(1, tp):
            y_wait(b, shift)
        final = jnp.zeros((length, span), jnp.float32)
        for part in range(tp):
            final = final + lax.dot_general(
                mg[part, b], wo[part], (((1,), (1,)), ((), ())), preferred_element_type=jnp.float32
            )
        out_ref[b] = final.astype(jnp.bfloat16)
        for shift in range(1, tp):
            y_copy(b, shift).wait_send()
        m_copy(b).wait_send()
        nb_copy(b).wait_send()
        for copy in each_halo(b):
            copy.wait_send()
        return carry

    lax.fori_loop(0, batch, finish, 0)
    for copy in sends:
        copy.wait_send()
    for chunk in range(2):
        pair(chunk).wait_send()
    o_pair.wait_send()
    for shift in range(1, tp):
        o_copy(shift).wait_send()


def body(tp, inputs, norm_gain, query_weight, key_weight, value_weight, query_gain, key_gain, out_weight):
    batch, length, model = inputs.shape
    share, groups, heads, width = query_weight.shape
    pairs = jnp.stack([key_weight, value_weight], axis=3).transpose(2, 0, 1, 3, 4).reshape(heads, share, WA)
    queries = query_weight.transpose(2, 0, 1, 3).reshape(heads, share, groups * width)
    slab = jnp.concatenate([pairs, queries, out_weight.transpose(0, 2, 1)], axis=2)
    span = model // tp
    rows = 2 * length
    total = sum(length + 2 * r for r in REACH)
    vmem = pl.BlockSpec(memory_space=pltpu.VMEM)
    bf16 = jnp.bfloat16
    dma = pltpu.SemaphoreType.DMA
    return pl.pallas_call(
        functools.partial(layer_kernel, tp, batch, length),
        out_shape=jax.ShapeDtypeStruct((batch, length, span), bf16),
        in_specs=[vmem] * 5,
        out_specs=vmem,
        scratch_shapes=[
            pltpu.VMEM((CHIPS, 2, share, WA), bf16),
            pltpu.VMEM((CHIPS, 2, share, WB), bf16),
            pltpu.VMEM((model, WA), bf16),
            pltpu.VMEM((model, WB), bf16),
            pltpu.VMEM((batch, 2, length, model), bf16),
            *[pltpu.VMEM((batch, rows + 2 * r, 128), bf16) for r in REACH],
            pltpu.VMEM((groups, batch, rows, 128), bf16),
            pltpu.VMEM((2, length, total), jnp.float32),
            pltpu.VMEM((tp, span, 128), bf16),
            pltpu.VMEM((model, 128), bf16),
            pltpu.VMEM((model, 128), bf16),
            pltpu.VMEM((tp, span, 128), bf16),
            pltpu.VMEM((batch, length, 128), bf16),
            pltpu.VMEM((batch, length, 128), bf16),
            pltpu.VMEM((batch, length, 128), bf16),
            pltpu.VMEM((tp, batch, length, 128), bf16),
            dma((2,)),
            dma((2,)),
            dma((2,)),
            dma((2, NZ)),
            dma((2, NZ)),
            dma((2, NZ, 3)),
            dma((2, NZ, 3)),
            dma((batch,)),
            dma((batch,)),
            dma((batch, groups, 2)),
            dma((batch, groups, 2)),
            dma((1,)),
            dma((1,)),
            dma((tp - 1,)),
            dma((tp - 1,)),
            dma((batch,)),
            dma((batch,)),
            dma((batch, tp - 1)),
            dma((batch, tp - 1)),
        ],
        compiler_params=pltpu.CompilerParams(collective_id=0, has_side_effects=True, vmem_limit_bytes=60 * 1024 * 1024),
        name="layer",
    )(
        inputs,
        norm_gain.reshape(1, model),
        slab,
        query_gain,
        key_gain,
    )


def solution(mesh):
    in_specs = (
        P(None, "sp", None),
        P(),
        P("sp", None, "tp", None),
        P("sp", None, "tp", None),
        P("sp", None, "tp", None),
        P(),
        P(),
        P("tp", None, "sp"),
    )
    out_specs = P(None, "sp", "tp")
    run = functools.partial(body, mesh.shape["tp"])
    return jax.shard_map(run, mesh=mesh, in_specs=in_specs, out_specs=out_specs, check_vma=False)
```

```python
import functools
import math

import jax
import jax.numpy as jnp
from jax import lax
from jax.experimental import pallas as pl
from jax.experimental.pallas import tpu as pltpu
from jax.sharding import PartitionSpec as P

GAPS = ((1, 32), (4, 32), (16, 16))
REACH = tuple(d * h for d, h in GAPS)
EPS = 1e-06
NEG = -1e30
LOG2E = 1.4426950408889634
MESH = pl.DeviceIdType.MESH
NZ, NX = 16, 4
CHIPS = NZ * NX
WB = 256


def layer_kernel(
    tp, batch, length, x_hbm, gain_hbm, qw_hbm, kw_hbm, vw_hbm, ow_hbm, qg_hbm, kg_hbm, out_ref,
    x_ref, gain_ref, qw_ref, kw_ref, vw_ref, ow_ref, qg_ref, kg_ref, slab_ref,
    w2, w01, wb, wk2, wk01, wq, nb, win0, win1, win2, qn, bias, osum, oown, orecv, wo, mown, msend, mrecv, mg,
    in_sem, pair_send, pair_recv, local_sem, za_send, za_recv, xa_send, xa_recv, zb_send, zb_recv, xb_send, xb_recv,
    nb_send, nb_recv, halo_send, halo_recv,
    o_send, o_recv, oy_send, oy_recv, m_send, m_recv, y_send, y_recv,
):
    me = lax.axis_index("sp")
    mine = lax.axis_index("tp")
    groups = len(GAPS)
    core = me % 2
    other = 1 - core
    chip = me // 2
    x = chip % NX
    z = chip // NX
    rows = 2 * length
    wins = (win0, win1, win2)
    bufs = (w2, w01, wb)

    def at_z(offset):
        return {"sp": (((z + offset + NZ) % NZ) * NX + x) * 2 + core}

    def at_x(offset):
        return {"sp": (z * NX + (x + offset) % NX) * 2 + core}

    sibling = {"sp": chip * 2 + other}

    def at_chip(offset):
        return {"sp": ((chip + offset + CHIPS) % CHIPS) * 2 + core}

    def at_y(offset):
        return {"tp": (mine + offset) % tp}

    barrier = pltpu.get_barrier_semaphore()

    def greet(target):
        pl.semaphore_signal(barrier, inc=1, device_id=target, device_id_type=MESH)

    targets = [at_z(o) for o in (-4, 4, -3, 3, -2, 2, -1, 1)] + [at_y(o) for o in range(1, tp)]
    targets += [at_x(o) for o in range(1, NX)] + [at_chip(1), at_chip(-1), sibling]
    for target in targets:
        greet(target)

    fetches = [
        pltpu.make_async_copy(src, dst, in_sem.at[i])
        for i, (src, dst) in enumerate(
            (
                (qw_hbm, qw_ref),
                (kw_hbm, kw_ref),
                (vw_hbm, vw_ref),
                (ow_hbm, ow_ref),
                (qg_hbm, qg_ref),
                (kg_hbm, kg_ref),
                (gain_hbm, gain_ref),
                (x_hbm, x_ref),
            )
        )
    ]
    for fetch in fetches:
        fetch.start()
    for fetch in fetches[:4]:
        fetch.wait()
    for head in range(2):
        pieces = []
        for group in (2, 0, 1):
            pieces += [kw_ref[:, group, head, :], vw_ref[:, group, head, :]]
        pieces += [qw_ref[:, group, head, :] for group in range(groups)]
        pieces = [piece.astype(jnp.float32) for piece in pieces + [ow_ref[head]]]
        slab_ref[head] = jnp.concatenate(pieces, axis=1).astype(jnp.bfloat16)

    pl.semaphore_wait(barrier, len(targets))

    cuts = (pl.ds(0, 128), pl.ds(128, 256), pl.ds(384, WB))

    def pair(chunk):
        return pltpu.make_async_remote_copy(
            src_ref=slab_ref.at[other, :, cuts[chunk]],
            dst_ref=bufs[chunk].at[chip, core],
            send_sem=pair_send.at[chunk],
            recv_sem=pair_recv.at[chunk],
            device_id=sibling,
            device_id_type=MESH,
        )

    def local(chunk):
        return pltpu.make_async_copy(
            slab_ref.at[core, :, cuts[chunk]], bufs[chunk].at[chip, core], local_sem.at[chunk]
        )

    def index_of(origin, column):
        return ((z + origin + NZ) % NZ) * NX + (x + column) % NX

    sends = []

    def move(block, send_sem, recv_sem, target):
        return pltpu.make_async_remote_copy(
            src_ref=block, dst_ref=block, send_sem=send_sem, recv_sem=recv_sem, device_id=target, device_id_type=MESH
        )

    def begin(copy):
        copy.start()
        sends.append(copy)

    def za_start(chunk, origin, step):
        rel = (origin - step) % NZ
        block = bufs[chunk].at[index_of(origin, 0)]
        begin(move(block, za_send.at[chunk, rel], za_recv.at[chunk, rel], at_z(step)))

    def za_wait(chunk, origin):
        rel = origin % NZ
        block = bufs[chunk].at[index_of(origin, 0)]
        move(block, za_send.at[chunk, rel], za_recv.at[chunk, rel], at_z(1)).wait_recv()

    def xa_start(chunk, origin):
        rel = origin % NZ
        block = bufs[chunk].at[index_of(origin, 0)]
        for shift in (1, 3, 2):
            begin(move(block, xa_send.at[chunk, rel, shift - 1], xa_recv.at[chunk, rel, shift - 1], at_x(shift)))

    def xa_wait(chunk, origin, shift):
        rel = origin % NZ
        block = bufs[chunk].at[index_of(origin, NX - shift)]
        move(block, xa_send.at[chunk, rel, shift - 1], xa_recv.at[chunk, rel, shift - 1], at_x(1)).wait_recv()

    def xb_start():
        block = wb.at[chip]
        for shift in (1, 3, 2):
            begin(move(block, xb_send.at[shift - 1], xb_recv.at[shift - 1], at_x(shift)))

    def xb_wait(shift):
        block = wb.at[index_of(0, NX - shift)]
        move(block, xb_send.at[shift - 1], xb_recv.at[shift - 1], at_x(1)).wait_recv()

    def zb_start(origin, step, column):
        rel = (origin - step) % NZ
        block = wb.at[index_of(origin, column)]
        begin(move(block, zb_send.at[rel, column], zb_recv.at[rel, column], at_z(step)))

    def zb_wait(origin, column):
        rel = origin % NZ
        block = wb.at[index_of(origin, column)]
        move(block, zb_send.at[rel, column], zb_recv.at[rel, column], at_z(1)).wait_recv()

    far = {4: ((-3, -1, -2), (-4, -3, -1, -2)), -4: ((4, 3, 1, 2), (3, 1, 2))}
    spread = (4, -4, 1, -1, 2, -2, 3, -3)

    for chunk in range(3):
        local(chunk).start()
        pair(chunk).start()
    for chunk in range(2):
        local(chunk).wait()
        pair(chunk).wait_recv()
        for step in spread:
            za_start(chunk, 0, step)
    local(2).wait()
    pair(2).wait_recv()
    xb_start()
    for chunk in range(2):
        xa_start(chunk, 0)
    for step in spread:
        zb_start(0, step, 0)

    def nb_copy(b):
        return pltpu.make_async_remote_copy(
            src_ref=nb.at[b, core],
            dst_ref=nb.at[b, core],
            send_sem=nb_send.at[b],
            recv_sem=nb_recv.at[b],
            device_id=sibling,
            device_id_type=MESH,
        )

    def norm_step(b, carry):
        flat = x_ref[b].astype(jnp.float32)
        scale = lax.rsqrt(jnp.mean(flat * flat, axis=-1, keepdims=True) + EPS)
        nb[b, core] = (flat * scale * gain_ref[...]).astype(jnp.bfloat16)
        nb_copy(b).start()
        return carry

    for fetch in fetches[4:]:
        fetch.wait()
    lax.fori_loop(0, batch, norm_step, 0)

    for origin in (1, -1, 2, -2):
        for chunk in range(2):
            za_wait(chunk, origin)
            xa_start(chunk, origin)
    for origin in (4, -4):
        for chunk in range(2):
            za_wait(chunk, origin)
            for step in far[origin][chunk]:
                za_start(chunk, origin, step)
            xa_start(chunk, origin)
    for origin in (3, -3):
        for chunk in range(2):
            za_wait(chunk, origin)
            xa_start(chunk, origin)
    for shift in (1, 3, 2):
        xb_wait(shift)
        for step in spread:
            zb_start(0, step, NX - shift)

    head = mine * 2 + core
    heads = 2 * tp
    power = -8.0 * (head + 1).astype(jnp.float32) / heads
    slope = jnp.exp2(jnp.full((8, 128), power, jnp.float32))[:1, :1] * LOG2E
    widths = [length + 2 * r for r in REACH]
    starts = [sum(widths[:g]) for g in range(groups)]
    total_rows = CHIPS * rows

    def bias_step(block, carry):
        for group, (dilation, half) in enumerate(GAPS):
            reach = REACH[group]
            shape = (length, widths[group])
            key = lax.broadcasted_iota(jnp.int32, shape, 1) - reach
            offset = jnp.abs(key - lax.broadcasted_iota(jnp.int32, shape, 0))
            at = key + (chip * rows + block * length)
            allowed = (offset <= reach) & (at >= 0) & (at < total_rows) & ((offset & (dilation - 1)) == 0)
            value = jnp.where(allowed, offset.astype(jnp.float32) * (-slope / float(reach)), NEG)
            bias[block, :, starts[group] : starts[group] + widths[group]] = value
        return carry

    lax.fori_loop(0, 2, bias_step, 0)

    late = (5, -5, 6, -6, 7, -7, 8)
    for origin in (4, -4):
        zb_wait(origin, 0)
        for step in far[origin][0]:
            zb_start(origin, step, 0)
    for origin in late:
        za_wait(0, origin)
        xa_start(0, origin)
    for column in (3, 1, 2):
        for origin in (4, -4):
            zb_wait(origin, column)
            for step in far[origin][column % 2]:
                zb_start(origin, step, column)
    for origin in late:
        za_wait(1, origin)
        xa_start(1, origin)

    lane = lax.broadcasted_iota(jnp.int32, (rows, 128), 1)
    low = lane < 64
    origins = (0, 1, -1, 2, -2, 3, -3, 4, -4) + late

    def all_keys(chunk):
        for origin in origins:
            for shift in (1, 3, 2):
                xa_wait(chunk, origin, shift)

    all_keys(0)
    wk2[...] = w2[...].reshape(wk2.shape)
    for b in range(batch):
        nb_copy(b).wait_recv()

    def halo(b, group, up):
        reach = REACH[group]
        win = wins[group]
        if up:
            src = win.at[b, pl.ds(rows, reach), :]
            dst = win.at[b, pl.ds(0, reach), :]
        else:
            src = win.at[b, pl.ds(reach, reach), :]
            dst = win.at[b, pl.ds(reach + rows, reach), :]
        return pltpu.make_async_remote_copy(
            src_ref=src,
            dst_ref=dst,
            send_sem=halo_send.at[b, group, 0 if up else 1],
            recv_sem=halo_recv.at[b, group, 0 if up else 1],
            device_id=at_chip(1 if up else -1),
            device_id_type=MESH,
        )

    def each_halo(b, only=(2, 1, 0)):
        return [halo(b, group, up) for group in only for up in (True, False)]

    ones = jnp.ones((1, 64), jnp.float32)
    zeros = jnp.zeros((1, 64), jnp.float32)

    def kv_step(weights, order):
        def step(b, carry):
            out = jnp.dot(nb[b].reshape(rows, -1), weights[...], preferred_element_type=jnp.float32)
            out = out.astype(jnp.bfloat16).astype(jnp.float32)
            for place, group in enumerate(order):
                seg = out[:, 128 * place : 128 * (place + 1)]
                mean = jnp.sum(jnp.where(low, seg * seg, 0.0), axis=-1, keepdims=True) / 64.0
                gain = jnp.concatenate([kg_ref[group : group + 1, :], ones], axis=1)
                scaled = seg * jnp.where(low, lax.rsqrt(mean + EPS), 1.0) * gain
                wins[group][b, REACH[group] : REACH[group] + rows, :] = scaled.astype(jnp.bfloat16)
            for copy in each_halo(b, order):
                copy.start()
            return carry

        return step

    lax.fori_loop(0, batch, kv_step(wk2, (2,)), 0)
    all_keys(1)
    wk01[...] = w01[...].reshape(wk01.shape)
    lax.fori_loop(0, batch, kv_step(wk01, (0, 1)), 0)

    for origin in (1, -1, 2, -2, 3, -3) + late:
        for column in range(NX):
            zb_wait(origin, column)
    wq[...] = wb[...].reshape(wq.shape)

    tile = wq[:, 128:].astype(jnp.float32)
    high = lax.broadcasted_iota(jnp.int32, tile.shape, 1) >= 64
    tile = jnp.where(high, tile, 0.0)
    tile = jnp.where(core == 0, pltpu.roll(tile, 64, 1), tile)
    oown[...] = tile.astype(jnp.bfloat16)
    o_pair = pltpu.make_async_remote_copy(
        src_ref=oown,
        dst_ref=orecv,
        send_sem=o_send.at[0],
        recv_sem=o_recv.at[0],
        device_id=sibling,
        device_id_type=MESH,
    )
    o_pair.start()

    factor = LOG2E / 8.0

    def q_step(b, carry):
        out = jnp.dot(nb[b].reshape(rows, -1), wq[...], preferred_element_type=jnp.float32)
        out = out.astype(jnp.bfloat16).astype(jnp.float32)
        first, second = out[:, :128], out[:, 128:]
        for group, seg, here in ((0, first, low), (1, first, ~low), (2, second, low)):
            mean = jnp.sum(jnp.where(here, seg * seg, 0.0), axis=-1, keepdims=True) / 64.0
            gain = qg_ref[group : group + 1, :] * factor
            gain = jnp.concatenate([zeros, gain] if group == 1 else [gain, zeros], axis=1)
            scaled = jnp.where(here, seg * lax.rsqrt(mean + EPS) * gain, 0.0)
            if group == 1:
                scaled = pltpu.roll(scaled, 64, 1)
            qn[group, b] = scaled.astype(jnp.bfloat16)
        return carry

    lax.fori_loop(0, batch, q_step, 0)

    span = wo.shape[1]
    o_pair.wait_recv()
    osum[...] = (oown[...] + orecv[...]).reshape(osum.shape)
    wo[mine] = osum[mine]

    def o_copy(shift):
        target = (mine + shift) % tp
        return pltpu.make_async_remote_copy(
            src_ref=osum.at[target],
            dst_ref=wo.at[mine],
            send_sem=oy_send.at[shift - 1],
            recv_sem=oy_recv.at[shift - 1],
            device_id=at_y(shift),
            device_id_type=MESH,
        )

    def o_wait(shift):
        pltpu.make_async_remote_copy(
            src_ref=osum.at[mine],
            dst_ref=wo.at[(mine + tp - shift) % tp],
            send_sem=oy_send.at[shift - 1],
            recv_sem=oy_recv.at[shift - 1],
            device_id=at_y(shift),
            device_id_type=MESH,
        ).wait_recv()

    for shift in range(1, tp):
        o_copy(shift).start()

    keep = lax.broadcasted_iota(jnp.int32, (length, 128), 1) >= 64

    def attend(b, block):
        total = jnp.zeros((length, 1), jnp.float32)
        summed = jnp.zeros((length, 128), jnp.float32)
        begin = pl.multiple_of(block * length, length)
        for group in range(groups):
            query = qn[group, b, pl.ds(begin, length), :]
            window = wins[group][b, pl.ds(begin, widths[group]), :]
            scores = lax.dot_general(query, window, (((1,), (1,)), ((), ())), preferred_element_type=jnp.float32)
            grown = jnp.exp2(scores + bias[block, :, starts[group] : starts[group] + widths[group]])
            total = total + jnp.sum(grown, axis=-1, keepdims=True)
            summed = summed + jnp.dot(grown.astype(jnp.bfloat16), window, preferred_element_type=jnp.float32)
        merged = jnp.where(keep, summed / total, 0.0)
        return jnp.where(core == 0, pltpu.roll(merged, 64, 1), merged).astype(jnp.bfloat16)

    def m_copy(b):
        return pltpu.make_async_remote_copy(
            src_ref=msend.at[b],
            dst_ref=mrecv.at[b],
            send_sem=m_send.at[b],
            recv_sem=m_recv.at[b],
            device_id=sibling,
            device_id_type=MESH,
        )

    def y_copy(b, shift):
        return pltpu.make_async_remote_copy(
            src_ref=mg.at[mine, b],
            dst_ref=mg.at[mine, b],
            send_sem=y_send.at[b, shift - 1],
            recv_sem=y_recv.at[b, shift - 1],
            device_id=at_y(shift),
            device_id_type=MESH,
        )

    def y_wait(b, shift):
        block = mg.at[(mine + tp - shift) % tp, b]
        pltpu.make_async_remote_copy(
            src_ref=block,
            dst_ref=block,
            send_sem=y_send.at[b, shift - 1],
            recv_sem=y_recv.at[b, shift - 1],
            device_id=at_y(shift),
            device_id_type=MESH,
        ).wait_recv()

    def pass_on(b):
        m_copy(b).wait_recv()
        mg[mine, b] = mown[b] + mrecv[b]
        for shift in range(1, tp):
            y_copy(b, shift).start()

    def attend_step(b, carry):
        for copy in each_halo(b):
            copy.wait_recv()
        msend[b] = attend(b, other)
        m_copy(b).start()

        @pl.when(b >= 1)
        def _():
            pass_on(b - 1)

        mown[b] = attend(b, core)
        return carry

    lax.fori_loop(0, batch, attend_step, 0)
    pass_on(batch - 1)
    for shift in range(1, tp):
        o_wait(shift)

    def finish(b, carry):
        for shift in range(1, tp):
            y_wait(b, shift)
        final = jnp.zeros((length, span), jnp.float32)
        for part in range(tp):
            final = final + lax.dot_general(
                mg[part, b], wo[part], (((1,), (1,)), ((), ())), preferred_element_type=jnp.float32
            )
        out_ref[b] = final.astype(jnp.bfloat16)
        for shift in range(1, tp):
            y_copy(b, shift).wait_send()
        m_copy(b).wait_send()
        nb_copy(b).wait_send()
        for copy in each_halo(b):
            copy.wait_send()
        return carry

    lax.fori_loop(0, batch, finish, 0)
    for copy in sends:
        copy.wait_send()
    for chunk in range(3):
        pair(chunk).wait_send()
    o_pair.wait_send()
    for shift in range(1, tp):
        o_copy(shift).wait_send()


def body(tp, inputs, norm_gain, query_weight, key_weight, value_weight, query_gain, key_gain, out_weight):
    batch, length, model = inputs.shape
    share, groups, heads, width = query_weight.shape
    span = model // tp
    rows = 2 * length
    total = sum(length + 2 * r for r in REACH)
    bf16 = jnp.bfloat16
    dma = pltpu.SemaphoreType.DMA
    operands = (
        inputs,
        norm_gain.reshape(1, model),
        query_weight,
        key_weight,
        value_weight,
        out_weight.transpose(0, 2, 1),
        query_gain,
        key_gain,
    )
    return pl.pallas_call(
        functools.partial(layer_kernel, tp, batch, length),
        out_shape=jax.ShapeDtypeStruct((batch, length, span), bf16),
        in_specs=[pl.BlockSpec(memory_space=pl.ANY)] * len(operands),
        out_specs=pl.BlockSpec(memory_space=pltpu.VMEM),
        scratch_shapes=[
            *[pltpu.VMEM(operand.shape, operand.dtype) for operand in operands],
            pltpu.VMEM((heads, share, 384 + WB), bf16),
            pltpu.VMEM((CHIPS, 2, share, 128), bf16),
            pltpu.VMEM((CHIPS, 2, share, 256), bf16),
            pltpu.VMEM((CHIPS, 2, share, WB), bf16),
            pltpu.VMEM((model, 128), bf16),
            pltpu.VMEM((model, 256), bf16),
            pltpu.VMEM((model, WB), bf16),
            pltpu.VMEM((batch, 2, length, model), bf16),
            *[pltpu.VMEM((batch, rows + 2 * r, 128), bf16) for r in REACH],
            pltpu.VMEM((groups, batch, rows, 128), bf16),
            pltpu.VMEM((2, length, total), jnp.float32),
            pltpu.VMEM((tp, span, 128), bf16),
            pltpu.VMEM((model, 128), bf16),
            pltpu.VMEM((model, 128), bf16),
            pltpu.VMEM((tp, span, 128), bf16),
            pltpu.VMEM((batch, length, 128), bf16),
            pltpu.VMEM((batch, length, 128), bf16),
            pltpu.VMEM((batch, length, 128), bf16),
            pltpu.VMEM((tp, batch, length, 128), bf16),
            dma((len(operands),)),
            dma((3,)),
            dma((3,)),
            dma((3,)),
            dma((2, NZ)),
            dma((2, NZ)),
            dma((2, NZ, 3)),
            dma((2, NZ, 3)),
            dma((NZ, NX)),
            dma((NZ, NX)),
            dma((3,)),
            dma((3,)),
            dma((batch,)),
            dma((batch,)),
            dma((batch, groups, 2)),
            dma((batch, groups, 2)),
            dma((1,)),
            dma((1,)),
            dma((tp - 1,)),
            dma((tp - 1,)),
            dma((batch,)),
            dma((batch,)),
            dma((batch, tp - 1)),
            dma((batch, tp - 1)),
        ],
        compiler_params=pltpu.CompilerParams(collective_id=0, has_side_effects=True, vmem_limit_bytes=60 * 1024 * 1024),
        name="layer",
    )(*operands)


def solution(mesh):
    in_specs = (
        P(None, "sp", None),
        P(),
        P("sp", None, "tp", None),
        P("sp", None, "tp", None),
        P("sp", None, "tp", None),
        P(),
        P(),
        P("tp", None, "sp"),
    )
    out_specs = P(None, "sp", "tp")
    run = functools.partial(body, mesh.shape["tp"])
    return jax.shard_map(run, mesh=mesh, in_specs=in_specs, out_specs=out_specs, check_vma=False)
```

```python
import functools
import math

import jax
import jax.numpy as jnp
from jax import lax
from jax.experimental import pallas as pl
from jax.experimental.pallas import tpu as pltpu
from jax.sharding import PartitionSpec as P

GAPS = ((1, 32), (4, 32), (16, 16))
REACH = tuple(d * h for d, h in GAPS)
EPS = 1e-06
NEG = -1e30
LOG2E = 1.4426950408889634
MESH = pl.DeviceIdType.MESH
NZ, NX = 16, 4
CHIPS = NZ * NX
WB = 256


def layer_kernel(
    tp, batch, length, x_hbm, gain_hbm, qw_hbm, kw_hbm, vw_hbm, ow_hbm, qg_hbm, kg_hbm, out_ref,
    x_ref, gain_ref, qw_ref, kw_ref, vw_ref, ow_ref, qg_ref, kg_ref, slab_ref,
    w2, w01, wb, wk2, wk01, wq, nb, win0, win1, win2, qn, bias, osum, oown, orecv, wo, mown, msend, mrecv, mg,
    in_sem, pair_send, pair_recv, local_sem, zh_send, zh_recv, za_send, za_recv, xa_send, xa_recv,
    nb_send, nb_recv, halo_send, halo_recv,
    o_send, o_recv, oy_send, oy_recv, m_send, m_recv, y_send, y_recv,
):
    me = lax.axis_index("sp")
    mine = lax.axis_index("tp")
    groups = len(GAPS)
    core = me % 2
    other = 1 - core
    chip = me // 2
    x = chip % NX
    z = chip // NX
    rows = 2 * length
    wins = (win0, win1, win2)
    bufs = (w2, w01, wb)

    def at_z(offset, on=core):
        return {"sp": (((z + offset + NZ) % NZ) * NX + x) * 2 + on}

    def at_x(offset):
        return {"sp": (z * NX + (x + offset) % NX) * 2 + core}

    sibling = {"sp": chip * 2 + other}

    def at_chip(offset):
        return {"sp": ((chip + offset + CHIPS) % CHIPS) * 2 + core}

    def at_y(offset):
        return {"tp": (mine + offset) % tp}

    barrier = pltpu.get_barrier_semaphore()

    def greet(target):
        pl.semaphore_signal(barrier, inc=1, device_id=target, device_id_type=MESH)

    targets = [at_z(o) for o in (-4, 4, -3, 3, -2, 2, -1, 1)] + [at_y(o) for o in range(1, tp)]
    targets += [at_x(o) for o in range(1, NX)] + [at_chip(1), at_chip(-1), sibling]
    targets += [at_z(o, other) for o in (-4, 4, -3, 3, -2, 2, -1, 1)]
    for target in targets:
        greet(target)

    fetches = [
        pltpu.make_async_copy(src, dst, in_sem.at[i])
        for i, (src, dst) in enumerate(
            (
                (qw_hbm, qw_ref),
                (kw_hbm, kw_ref),
                (vw_hbm, vw_ref),
                (ow_hbm, ow_ref),
                (qg_hbm, qg_ref),
                (kg_hbm, kg_ref),
                (gain_hbm, gain_ref),
                (x_hbm, x_ref),
            )
        )
    ]
    for fetch in fetches:
        fetch.start()
    for fetch in fetches[:4]:
        fetch.wait()
    for head in range(2):
        pieces = []
        for group in (2, 0, 1):
            pieces += [kw_ref[:, group, head, :], vw_ref[:, group, head, :]]
        pieces += [qw_ref[:, group, head, :] for group in range(groups)]
        pieces = [piece.astype(jnp.float32) for piece in pieces + [ow_ref[head]]]
        slab_ref[head] = jnp.concatenate(pieces, axis=1).astype(jnp.bfloat16)

    pl.semaphore_wait(barrier, len(targets))

    cuts = (pl.ds(0, 128), pl.ds(128, 256), pl.ds(384, WB))

    def pair(chunk):
        return pltpu.make_async_remote_copy(
            src_ref=slab_ref.at[other, :, cuts[chunk]],
            dst_ref=bufs[chunk].at[chip, core],
            send_sem=pair_send.at[chunk],
            recv_sem=pair_recv.at[chunk],
            device_id=sibling,
            device_id_type=MESH,
        )

    def local(chunk):
        return pltpu.make_async_copy(
            slab_ref.at[core, :, cuts[chunk]], bufs[chunk].at[chip, core], local_sem.at[chunk]
        )

    def index_of(origin, column):
        return ((z + origin + NZ) % NZ) * NX + (x + column) % NX

    sends = []

    def move(block, send_sem, recv_sem, target):
        return pltpu.make_async_remote_copy(
            src_ref=block, dst_ref=block, send_sem=send_sem, recv_sem=recv_sem, device_id=target, device_id_type=MESH
        )

    def begin(copy):
        copy.start()
        sends.append(copy)

    def zh_start(chunk, step):
        rel = -step % NZ
        for half, on in enumerate((core, other)):
            begin(
                pltpu.make_async_remote_copy(
                    src_ref=slab_ref.at[on, :, cuts[chunk]],
                    dst_ref=bufs[chunk].at[chip, core],
                    send_sem=zh_send.at[chunk, rel, half],
                    recv_sem=zh_recv.at[chunk, rel, half],
                    device_id=at_z(step, on),
                    device_id_type=MESH,
                )
            )

    def zh_wait(chunk, origin):
        rel = origin % NZ
        for half, parity in enumerate((core, other)):
            pltpu.make_async_remote_copy(
                src_ref=slab_ref.at[0, :, cuts[chunk]],
                dst_ref=bufs[chunk].at[index_of(origin, 0), parity],
                send_sem=zh_send.at[chunk, rel, half],
                recv_sem=zh_recv.at[chunk, rel, half],
                device_id=at_z(1),
                device_id_type=MESH,
            ).wait_recv()

    def za_start(chunk, origin, step):
        rel = (origin - step) % NZ
        block = bufs[chunk].at[index_of(origin, 0)]
        begin(move(block, za_send.at[chunk, rel], za_recv.at[chunk, rel], at_z(step)))

    def za_wait(chunk, origin):
        rel = origin % NZ
        block = bufs[chunk].at[index_of(origin, 0)]
        move(block, za_send.at[chunk, rel], za_recv.at[chunk, rel], at_z(1)).wait_recv()

    def xa_start(chunk, origin):
        rel = origin % NZ
        block = bufs[chunk].at[index_of(origin, 0)]
        for shift in (1, 3, 2):
            begin(move(block, xa_send.at[chunk, rel, shift - 1], xa_recv.at[chunk, rel, shift - 1], at_x(shift)))

    def xa_wait(chunk, origin, shift):
        rel = origin % NZ
        block = bufs[chunk].at[index_of(origin, NX - shift)]
        move(block, xa_send.at[chunk, rel, shift - 1], xa_recv.at[chunk, rel, shift - 1], at_x(1)).wait_recv()

    far = {4: ((-3, -1, -2), (-4, -3, -1, -2)), -4: ((4, 3, 1, 2), (3, 1, 2))}

    for chunk in range(3):
        for step in (4, -4, 3, -3, 1, -1, 2, -2):
            zh_start(chunk, step)
        local(chunk).start()
        pair(chunk).start()

    def nb_copy(b):
        return pltpu.make_async_remote_copy(
            src_ref=nb.at[b, core],
            dst_ref=nb.at[b, core],
            send_sem=nb_send.at[b],
            recv_sem=nb_recv.at[b],
            device_id=sibling,
            device_id_type=MESH,
        )

    def norm_step(b, carry):
        flat = x_ref[b].astype(jnp.float32)
        scale = lax.rsqrt(jnp.mean(flat * flat, axis=-1, keepdims=True) + EPS)
        nb[b, core] = (flat * scale * gain_ref[...]).astype(jnp.bfloat16)
        nb_copy(b).start()
        return carry

    for fetch in fetches[4:]:
        fetch.wait()
    lax.fori_loop(0, batch, norm_step, 0)

    for chunk in range(3):
        local(chunk).wait()
        pair(chunk).wait_recv()
        xa_start(chunk, 0)
    for origin in (1, -1, 2, -2):
        for chunk in range(3):
            zh_wait(chunk, origin)
            xa_start(chunk, origin)
    for origin in (4, -4):
        for chunk in range(3):
            zh_wait(chunk, origin)
            for step in far[origin][chunk % 2]:
                za_start(chunk, origin, step)
    for origin in (3, -3):
        for chunk in range(3):
            zh_wait(chunk, origin)
            xa_start(chunk, origin)
    for origin in (4, -4):
        for chunk in range(3):
            xa_start(chunk, origin)

    head = mine * 2 + core
    heads = 2 * tp
    power = -8.0 * (head + 1).astype(jnp.float32) / heads
    slope = jnp.exp2(jnp.full((8, 128), power, jnp.float32))[:1, :1] * LOG2E
    widths = [length + 2 * r for r in REACH]
    starts = [sum(widths[:g]) for g in range(groups)]
    total_rows = CHIPS * rows

    def bias_step(block, carry):
        for group, (dilation, half) in enumerate(GAPS):
            reach = REACH[group]
            shape = (length, widths[group])
            key = lax.broadcasted_iota(jnp.int32, shape, 1) - reach
            offset = jnp.abs(key - lax.broadcasted_iota(jnp.int32, shape, 0))
            at = key + (chip * rows + block * length)
            allowed = (offset <= reach) & (at >= 0) & (at < total_rows) & ((offset & (dilation - 1)) == 0)
            value = jnp.where(allowed, offset.astype(jnp.float32) * (-slope / float(reach)), NEG)
            bias[block, :, starts[group] : starts[group] + widths[group]] = value
        return carry

    lax.fori_loop(0, 2, bias_step, 0)

    late = (5, -5, 6, -6, 7, -7, 8)
    for origin in late:
        for chunk in range(3):
            za_wait(chunk, origin)
            xa_start(chunk, origin)

    lane = lax.broadcasted_iota(jnp.int32, (rows, 128), 1)
    low = lane < 64
    origins = (0, 1, -1, 2, -2, 3, -3, 4, -4) + late

    def all_blocks(chunk):
        for origin in origins:
            for shift in (1, 3, 2):
                xa_wait(chunk, origin, shift)

    all_blocks(0)
    wk2[...] = w2[...].reshape(wk2.shape)
    for b in range(batch):
        nb_copy(b).wait_recv()

    def halo(b, group, up):
        reach = REACH[group]
        win = wins[group]
        if up:
            src = win.at[b, pl.ds(rows, reach), :]
            dst = win.at[b, pl.ds(0, reach), :]
        else:
            src = win.at[b, pl.ds(reach, reach), :]
            dst = win.at[b, pl.ds(reach + rows, reach), :]
        return pltpu.make_async_remote_copy(
            src_ref=src,
            dst_ref=dst,
            send_sem=halo_send.at[b, group, 0 if up else 1],
            recv_sem=halo_recv.at[b, group, 0 if up else 1],
            device_id=at_chip(1 if up else -1),
            device_id_type=MESH,
        )

    def each_halo(b, only=(2, 1, 0)):
        return [halo(b, group, up) for group in only for up in (True, False)]

    ones = jnp.ones((1, 64), jnp.float32)
    zeros = jnp.zeros((1, 64), jnp.float32)

    def kv_step(weights, order):
        def step(b, carry):
            out = jnp.dot(nb[b].reshape(rows, -1), weights[...], preferred_element_type=jnp.float32)
            out = out.astype(jnp.bfloat16).astype(jnp.float32)
            for place, group in enumerate(order):
                seg = out[:, 128 * place : 128 * (place + 1)]
                mean = jnp.sum(jnp.where(low, seg * seg, 0.0), axis=-1, keepdims=True) / 64.0
                gain = jnp.concatenate([kg_ref[group : group + 1, :], ones], axis=1)
                scaled = seg * jnp.where(low, lax.rsqrt(mean + EPS), 1.0) * gain
                wins[group][b, REACH[group] : REACH[group] + rows, :] = scaled.astype(jnp.bfloat16)
            for copy in each_halo(b, order):
                copy.start()
            return carry

        return step

    lax.fori_loop(0, batch, kv_step(wk2, (2,)), 0)
    all_blocks(1)
    wk01[...] = w01[...].reshape(wk01.shape)
    lax.fori_loop(0, batch, kv_step(wk01, (0, 1)), 0)

    all_blocks(2)
    wq[...] = wb[...].reshape(wq.shape)

    tile = wq[:, 128:].astype(jnp.float32)
    high = lax.broadcasted_iota(jnp.int32, tile.shape, 1) >= 64
    tile = jnp.where(high, tile, 0.0)
    tile = jnp.where(core == 0, pltpu.roll(tile, 64, 1), tile)
    oown[...] = tile.astype(jnp.bfloat16)
    o_pair = pltpu.make_async_remote_copy(
        src_ref=oown,
        dst_ref=orecv,
        send_sem=o_send.at[0],
        recv_sem=o_recv.at[0],
        device_id=sibling,
        device_id_type=MESH,
    )
    o_pair.start()

    factor = LOG2E / 8.0

    def q_step(b, carry):
        out = jnp.dot(nb[b].reshape(rows, -1), wq[...], preferred_element_type=jnp.float32)
        out = out.astype(jnp.bfloat16).astype(jnp.float32)
        first, second = out[:, :128], out[:, 128:]
        for group, seg, here in ((0, first, low), (1, first, ~low), (2, second, low)):
            mean = jnp.sum(jnp.where(here, seg * seg, 0.0), axis=-1, keepdims=True) / 64.0
            gain = qg_ref[group : group + 1, :] * factor
            gain = jnp.concatenate([zeros, gain] if group == 1 else [gain, zeros], axis=1)
            scaled = jnp.where(here, seg * lax.rsqrt(mean + EPS) * gain, 0.0)
            if group == 1:
                scaled = pltpu.roll(scaled, 64, 1)
            qn[group, b] = scaled.astype(jnp.bfloat16)
        return carry

    lax.fori_loop(0, batch, q_step, 0)

    span = wo.shape[1]
    o_pair.wait_recv()
    osum[...] = (oown[...] + orecv[...]).reshape(osum.shape)
    wo[mine] = osum[mine]

    def o_copy(shift):
        target = (mine + shift) % tp
        return pltpu.make_async_remote_copy(
            src_ref=osum.at[target],
            dst_ref=wo.at[mine],
            send_sem=oy_send.at[shift - 1],
            recv_sem=oy_recv.at[shift - 1],
            device_id=at_y(shift),
            device_id_type=MESH,
        )

    def o_wait(shift):
        pltpu.make_async_remote_copy(
            src_ref=osum.at[mine],
            dst_ref=wo.at[(mine + tp - shift) % tp],
            send_sem=oy_send.at[shift - 1],
            recv_sem=oy_recv.at[shift - 1],
            device_id=at_y(shift),
            device_id_type=MESH,
        ).wait_recv()

    for shift in range(1, tp):
        o_copy(shift).start()

    keep = lax.broadcasted_iota(jnp.int32, (length, 128), 1) >= 64

    def attend(b, block):
        total = jnp.zeros((length, 1), jnp.float32)
        summed = jnp.zeros((length, 128), jnp.float32)
        begin = pl.multiple_of(block * length, length)
        for group in range(groups):
            query = qn[group, b, pl.ds(begin, length), :]
            window = wins[group][b, pl.ds(begin, widths[group]), :]
            scores = lax.dot_general(query, window, (((1,), (1,)), ((), ())), preferred_element_type=jnp.float32)
            grown = jnp.exp2(scores + bias[block, :, starts[group] : starts[group] + widths[group]])
            total = total + jnp.sum(grown, axis=-1, keepdims=True)
            summed = summed + jnp.dot(grown.astype(jnp.bfloat16), window, preferred_element_type=jnp.float32)
        merged = jnp.where(keep, summed / total, 0.0)
        return jnp.where(core == 0, pltpu.roll(merged, 64, 1), merged).astype(jnp.bfloat16)

    def m_copy(b):
        return pltpu.make_async_remote_copy(
            src_ref=msend.at[b],
            dst_ref=mrecv.at[b],
            send_sem=m_send.at[b],
            recv_sem=m_recv.at[b],
            device_id=sibling,
            device_id_type=MESH,
        )

    def y_copy(b, shift):
        return pltpu.make_async_remote_copy(
            src_ref=mg.at[mine, b],
            dst_ref=mg.at[mine, b],
            send_sem=y_send.at[b, shift - 1],
            recv_sem=y_recv.at[b, shift - 1],
            device_id=at_y(shift),
            device_id_type=MESH,
        )

    def y_wait(b, shift):
        block = mg.at[(mine + tp - shift) % tp, b]
        pltpu.make_async_remote_copy(
            src_ref=block,
            dst_ref=block,
            send_sem=y_send.at[b, shift - 1],
            recv_sem=y_recv.at[b, shift - 1],
            device_id=at_y(shift),
            device_id_type=MESH,
        ).wait_recv()

    def pass_on(b):
        m_copy(b).wait_recv()
        mg[mine, b] = mown[b] + mrecv[b]
        for shift in range(1, tp):
            y_copy(b, shift).start()

    def attend_step(b, carry):
        for copy in each_halo(b):
            copy.wait_recv()
        msend[b] = attend(b, other)
        m_copy(b).start()

        @pl.when(b >= 1)
        def _():
            pass_on(b - 1)

        mown[b] = attend(b, core)
        return carry

    lax.fori_loop(0, batch, attend_step, 0)
    pass_on(batch - 1)
    for shift in range(1, tp):
        o_wait(shift)

    def finish(b, carry):
        for shift in range(1, tp):
            y_wait(b, shift)
        final = jnp.zeros((length, span), jnp.float32)
        for part in range(tp):
            final = final + lax.dot_general(
                mg[part, b], wo[part], (((1,), (1,)), ((), ())), preferred_element_type=jnp.float32
            )
        out_ref[b] = final.astype(jnp.bfloat16)
        for shift in range(1, tp):
            y_copy(b, shift).wait_send()
        m_copy(b).wait_send()
        nb_copy(b).wait_send()
        for copy in each_halo(b):
            copy.wait_send()
        return carry

    lax.fori_loop(0, batch, finish, 0)
    for copy in sends:
        copy.wait_send()
    for chunk in range(3):
        pair(chunk).wait_send()
    o_pair.wait_send()
    for shift in range(1, tp):
        o_copy(shift).wait_send()


def body(tp, inputs, norm_gain, query_weight, key_weight, value_weight, query_gain, key_gain, out_weight):
    batch, length, model = inputs.shape
    share, groups, heads, width = query_weight.shape
    span = model // tp
    rows = 2 * length
    total = sum(length + 2 * r for r in REACH)
    bf16 = jnp.bfloat16
    dma = pltpu.SemaphoreType.DMA
    operands = (
        inputs,
        norm_gain.reshape(1, model),
        query_weight,
        key_weight,
        value_weight,
        out_weight.transpose(0, 2, 1),
        query_gain,
        key_gain,
    )
    return pl.pallas_call(
        functools.partial(layer_kernel, tp, batch, length),
        out_shape=jax.ShapeDtypeStruct((batch, length, span), bf16),
        in_specs=[pl.BlockSpec(memory_space=pl.ANY)] * len(operands),
        out_specs=pl.BlockSpec(memory_space=pltpu.VMEM),
        scratch_shapes=[
            *[pltpu.VMEM(operand.shape, operand.dtype) for operand in operands],
            pltpu.VMEM((heads, share, 384 + WB), bf16),
            pltpu.VMEM((CHIPS, 2, share, 128), bf16),
            pltpu.VMEM((CHIPS, 2, share, 256), bf16),
            pltpu.VMEM((CHIPS, 2, share, WB), bf16),
            pltpu.VMEM((model, 128), bf16),
            pltpu.VMEM((model, 256), bf16),
            pltpu.VMEM((model, WB), bf16),
            pltpu.VMEM((batch, 2, length, model), bf16),
            *[pltpu.VMEM((batch, rows + 2 * r, 128), bf16) for r in REACH],
            pltpu.VMEM((groups, batch, rows, 128), bf16),
            pltpu.VMEM((2, length, total), jnp.float32),
            pltpu.VMEM((tp, span, 128), bf16),
            pltpu.VMEM((model, 128), bf16),
            pltpu.VMEM((model, 128), bf16),
            pltpu.VMEM((tp, span, 128), bf16),
            pltpu.VMEM((batch, length, 128), bf16),
            pltpu.VMEM((batch, length, 128), bf16),
            pltpu.VMEM((batch, length, 128), bf16),
            pltpu.VMEM((tp, batch, length, 128), bf16),
            dma((len(operands),)),
            dma((3,)),
            dma((3,)),
            dma((3,)),
            dma((3, NZ, 2)),
            dma((3, NZ, 2)),
            dma((3, NZ)),
            dma((3, NZ)),
            dma((3, NZ, 3)),
            dma((3, NZ, 3)),
            dma((batch,)),
            dma((batch,)),
            dma((batch, groups, 2)),
            dma((batch, groups, 2)),
            dma((1,)),
            dma((1,)),
            dma((tp - 1,)),
            dma((tp - 1,)),
            dma((batch,)),
            dma((batch,)),
            dma((batch, tp - 1)),
            dma((batch, tp - 1)),
        ],
        compiler_params=pltpu.CompilerParams(collective_id=0, has_side_effects=True, vmem_limit_bytes=60 * 1024 * 1024),
        name="layer",
    )(*operands)


def solution(mesh):
    in_specs = (
        P(None, "sp", None),
        P(),
        P("sp", None, "tp", None),
        P("sp", None, "tp", None),
        P("sp", None, "tp", None),
        P(),
        P(),
        P("tp", None, "sp"),
    )
    out_specs = P(None, "sp", "tp")
    run = functools.partial(body, mesh.shape["tp"])
    return jax.shard_map(run, mesh=mesh, in_specs=in_specs, out_specs=out_specs, check_vma=False)
```

```python
import functools
import math

import jax
import jax.numpy as jnp
from jax import lax
from jax.experimental import pallas as pl
from jax.experimental.pallas import tpu as pltpu
from jax.sharding import PartitionSpec as P

FOLDED = (1, 2)
GAPS = ((1, 32), (4, 32), (16, 16))
REACH = tuple(d * h for d, h in GAPS)
EPS = 1e-06
NEG = -1e30
LOG2E = 1.4426950408889634
MESH = pl.DeviceIdType.MESH
NZ, NX = 16, 4
CHIPS = NZ * NX
WB = 256


def layer_kernel(
    tp, batch, length, x_hbm, gain_hbm, qw_hbm, kw_hbm, vw_hbm, ow_hbm, qg_hbm, kg_hbm, out_ref,
    x_ref, gain_ref, qw_ref, kw_ref, vw_ref, ow_ref, qg_ref, kg_ref, slab_ref,
    w2, w01, wb, wk, wq, nb, win0, win1, win2, qn, bias0, bias1, bias2, osum, oown, orecv, wo, mboth, mrecv, mg,
    in_sem, pair_send, pair_recv, local_sem, out_sem, zh_recv, xh_recv, za_recv, xa_recv,
    nb_send, nb_recv, halo_send, halo_recv,
    o_send, o_recv, oy_send, oy_recv, m_send, m_recv, y_send, y_recv,
):
    me = lax.axis_index("sp")
    mine = lax.axis_index("tp")
    groups = len(GAPS)
    core = me % 2
    other = 1 - core
    chip = me // 2
    x = chip % NX
    z = chip // NX
    rows = 2 * length
    wins = (win0, win1, win2)
    biases = (bias0, bias1, bias2)
    bufs = (w2, w01, wb)

    def at_z(offset, on=core):
        return {"sp": (((z + offset + NZ) % NZ) * NX + x) * 2 + on}

    def at_x(offset, on=core):
        return {"sp": (z * NX + (x + offset) % NX) * 2 + on}

    sibling = {"sp": chip * 2 + other}

    def at_chip(offset):
        return {"sp": ((chip + offset + CHIPS) % CHIPS) * 2 + core}

    def at_y(offset):
        return {"tp": (mine + offset) % tp}

    barrier = pltpu.get_barrier_semaphore()

    def greet(target):
        pl.semaphore_signal(barrier, inc=1, device_id=target, device_id_type=MESH)

    targets = [at_z(o) for o in (-4, 4, -3, 3, -2, 2, -1, 1)] + [at_y(o) for o in range(1, tp)]
    targets += [at_x(o) for o in range(1, NX)] + [at_chip(1), at_chip(-1), sibling]
    targets += [at_x(2, other)]
    targets += [at_z(o, other) for o in (-4, 4, -3, 3, -2, 2, -1, 1)]
    for target in targets:
        greet(target)

    fetches = [
        pltpu.make_async_copy(src, dst, in_sem.at[i])
        for i, (src, dst) in enumerate(
            (
                (qw_hbm, qw_ref),
                (kw_hbm, kw_ref),
                (vw_hbm, vw_ref),
                (ow_hbm, ow_ref),
                (qg_hbm, qg_ref),
                (kg_hbm, kg_ref),
                (gain_hbm, gain_ref),
                (x_hbm, x_ref),
            )
        )
    ]
    for fetch in fetches:
        fetch.start()
    for fetch in fetches[:4]:
        fetch.wait()
    for head in range(2):
        pieces = []
        for group in (2, 0, 1):
            pieces += [kw_ref[:, group, head, :], vw_ref[:, group, head, :]]
        pieces += [qw_ref[:, group, head, :] for group in range(groups)]
        pieces = [piece.astype(jnp.float32) for piece in pieces + [ow_ref[head]]]
        slab_ref[head] = jnp.concatenate(pieces, axis=1).astype(jnp.bfloat16)

    pl.semaphore_wait(barrier, len(targets))

    cuts = (pl.ds(0, 128), pl.ds(128, 256), pl.ds(384, WB))

    def pair(chunk):
        return pltpu.make_async_remote_copy(
            src_ref=slab_ref.at[other, :, cuts[chunk]],
            dst_ref=bufs[chunk].at[chip, core],
            send_sem=pair_send.at[chunk],
            recv_sem=pair_recv.at[chunk],
            device_id=sibling,
            device_id_type=MESH,
        )

    def local(chunk):
        return pltpu.make_async_copy(
            slab_ref.at[core, :, cuts[chunk]], bufs[chunk].at[chip, core], local_sem.at[chunk]
        )

    def index_of(origin, column):
        return ((z + origin + NZ) % NZ) * NX + (x + column) % NX

    def move(block, send_sem, recv_sem, target, land=None):
        return pltpu.make_async_remote_copy(
            src_ref=block,
            dst_ref=block if land is None else land,
            send_sem=send_sem,
            recv_sem=recv_sem,
            device_id=target,
            device_id_type=MESH,
        )

    def zh_start(chunk, step):
        for on in (core, other):
            move(
                slab_ref.at[on, :, cuts[chunk]],
                out_sem.at[chunk],
                zh_recv.at[chunk, 3 - step if step < 0 else step - 1],
                at_z(step, on),
                bufs[chunk].at[chip, core],
            ).start()

    def zh_wait(chunk, origin):
        block = bufs[chunk].at[index_of(origin, 0)]
        slot = 3 + origin if origin > 0 else -origin - 1
        move(block, out_sem.at[chunk], zh_recv.at[chunk, slot], at_z(1)).wait_recv()

    def xh_start(chunk):
        for on in (core, other):
            move(
                slab_ref.at[on, :, cuts[chunk]],
                out_sem.at[chunk],
                xh_recv.at[chunk],
                at_x(2, on),
                bufs[chunk].at[chip, core],
            ).start()

    def xh_wait(chunk):
        move(bufs[chunk].at[index_of(0, 2)], out_sem.at[chunk], xh_recv.at[chunk], at_x(1)).wait_recv()

    def slot_of(rel, fold):
        if fold == 0:
            return rel - 5
        return {4: 7, NZ - 4: 8}.get(rel, 9)

    def za_start(chunk, origin, step, fold=0):
        slot = slot_of((origin - step) % NZ, fold)
        block = bufs[chunk].at[index_of(origin, 2 * fold)]
        move(block, out_sem.at[chunk], za_recv.at[chunk, slot], at_z(step)).start()

    def za_wait(chunk, origin, fold=0):
        block = bufs[chunk].at[index_of(origin, 2 * fold)]
        move(block, out_sem.at[chunk], za_recv.at[chunk, slot_of(origin % NZ, fold)], at_z(1)).wait_recv()

    def shifts(chunk):
        return (1, 3) if chunk in FOLDED else (1, 3, 2)

    def xa_start(chunk, origin):
        block = bufs[chunk].at[index_of(origin, 0)]
        for shift in shifts(chunk):
            move(block, out_sem.at[chunk], xa_recv.at[chunk], at_x(shift)).start()

    far = {4: ((-3, -1, -2), (-4, -3, -1, -2)), -4: ((4, 3, 1, 2), (3, 1, 2))}

    for step in (4, -4, 3, -3, 1, -1, 2, -2):
        zh_start(0, step)
    for steps in ((4, -4), (1, -1, 2, -2, 3, -3)):
        for chunk in (1, 2):
            for step in steps:
                zh_start(chunk, step)
    for chunk in FOLDED:
        xh_start(chunk)
    for chunk in range(3):
        local(chunk).start()
        pair(chunk).start()

    def nb_copy(b):
        return move(nb.at[b, core], nb_send.at[0], nb_recv.at[0], sibling)

    def norm_step(b, carry):
        flat = x_ref[b].astype(jnp.float32)
        scale = lax.rsqrt(jnp.mean(flat * flat, axis=-1, keepdims=True) + EPS)
        nb[b, core] = (flat * scale * gain_ref[...]).astype(jnp.bfloat16)
        nb_copy(b).start()
        return carry

    for fetch in fetches[4:]:
        fetch.wait()
    lax.fori_loop(0, batch, norm_step, 0)

    for chunk in range(3):
        local(chunk).wait()
        pair(chunk).wait_recv()
        xa_start(chunk, 0)

    def near(chunk, spread):
        for origin in (1, -1, 2, -2):
            zh_wait(chunk, origin)
            if spread:
                xa_start(chunk, origin)
        for origin in (4, -4):
            zh_wait(chunk, origin)
            for step in far[origin][chunk % 2]:
                za_start(chunk, origin, step)
        for origin in (3, -3):
            zh_wait(chunk, origin)
            if spread:
                xa_start(chunk, origin)
        if spread:
            for origin in (4, -4):
                xa_start(chunk, origin)

    near(0, True)
    for chunk in FOLDED:
        xh_wait(chunk)
        for step in (4, -4, 3, -3, 1, -1, 2, -2):
            za_start(chunk, 0, step, 1)
    near(1, True)
    near(2, True)

    head = mine * 2 + core
    heads = 2 * tp
    power = -8.0 * (head + 1).astype(jnp.float32) / heads
    slope = jnp.exp2(jnp.full((8, 128), power, jnp.float32))[:1, :1] * LOG2E
    total_rows = CHIPS * rows

    def bias_of(group, count, first):
        dilation, half = GAPS[group]
        reach = REACH[group]
        shape = (count, count + 2 * reach)
        key = lax.broadcasted_iota(jnp.int32, shape, 1) - reach
        offset = jnp.abs(key - lax.broadcasted_iota(jnp.int32, shape, 0))
        at = key + (chip * rows + first)
        allowed = (offset <= reach) & (at >= 0) & (at < total_rows) & ((offset & (dilation - 1)) == 0)
        return jnp.where(allowed, offset.astype(jnp.float32) * (-slope / float(reach)), NEG)

    for block in range(2):
        bias0[block] = bias_of(0, length, block * length)
    for group in (1, 2):
        biases[group][...] = bias_of(group, rows, 0)

    late = (5, -5, 6, -6, 7, -7, 8)
    def fold_on(chunk):
        for origin in (4, -4):
            za_wait(chunk, origin, 1)
            for step in far[origin][1 - chunk % 2]:
                za_start(chunk, origin, step, 1)

    def late_on(chunk, part):
        for origin in part:
            za_wait(chunk, origin)
            xa_start(chunk, origin)

    late_on(0, late[:4])
    fold_on(1)
    late_on(0, late[4:])
    fold_on(2)
    late_on(1, late)
    late_on(2, late)

    lane = lax.broadcasted_iota(jnp.int32, (rows, 128), 1)
    low = lane < 64
    origins = (0, 1, -1, 2, -2, 3, -3, 4, -4) + late

    def all_blocks(chunk):
        several = bufs[chunk].at[pl.ds(0, NZ * len(shifts(chunk)))]
        move(several, out_sem.at[chunk], xa_recv.at[chunk], at_x(1)).wait_recv()
        if chunk in FOLDED:
            several = bufs[chunk].at[pl.ds(0, NZ - 3)]
            move(several, out_sem.at[chunk], za_recv.at[chunk, 9], at_x(1)).wait_recv()

    all_blocks(0)
    wk[:, :128] = w2[...].reshape(wk.shape[0], 128)
    nb_all = move(nb.at[:, 0], nb_send.at[0], nb_recv.at[0], sibling)
    nb_all.wait_recv()

    def halo(b, group, up):
        reach = REACH[group]
        begin_at, land_at = (rows, 0) if up else (reach, reach + rows)
        return pltpu.make_async_remote_copy(
            src_ref=wins[group].at[b, pl.ds(begin_at, reach), :],
            dst_ref=wins[group].at[b, pl.ds(land_at, reach), :],
            send_sem=halo_send.at[group],
            recv_sem=halo_recv.at[b, group],
            device_id=at_chip(1 if up else -1),
            device_id_type=MESH,
        )

    def halo_wait(b):
        for group in (2, 1, 0):
            both = wins[group].at[b, pl.ds(0, 2 * REACH[group]), :]
            move(both, halo_send.at[group], halo_recv.at[b, group], at_chip(1)).wait_recv()

    ones = jnp.ones((1, 64), jnp.float32)
    zeros = jnp.zeros((1, 64), jnp.float32)

    def key_norm(out, place, group):
        seg = out[:, 128 * place : 128 * (place + 1)].astype(jnp.bfloat16).astype(jnp.float32)
        mean = jnp.sum(jnp.where(low, seg * seg, 0.0), axis=-1, keepdims=True) / 64.0
        gain = jnp.concatenate([kg_ref[group : group + 1, :], ones], axis=1)
        return (seg * jnp.where(low, lax.rsqrt(mean + EPS), 1.0) * gain).astype(jnp.bfloat16)

    def key_step(b, first, order):
        out = jnp.dot(nb[b].reshape(rows, -1), wk[:, first : first + 128 * len(order)], preferred_element_type=jnp.float32)
        for place, group in enumerate(order):
            wins[group][b, REACH[group] : REACH[group] + rows, :] = key_norm(out, place, group)
        for group in order:
            for up in (True, False):
                halo(b, group, up).start()

    for b in range(batch):
        key_step(b, 0, (2,))
    all_blocks(1)
    wk[:, 128:] = w01[...].reshape(wk.shape[0], 256)
    for b in range(batch):
        key_step(b, 128, (0, 1))

    all_blocks(2)
    wq[...] = wb[...].reshape(wq.shape)

    tile = wq[:, 128:].astype(jnp.float32)
    high = lax.broadcasted_iota(jnp.int32, tile.shape, 1) >= 64
    tile = jnp.where(high, tile, 0.0)
    tile = jnp.where(core == 0, pltpu.roll(tile, 64, 1), tile)
    oown[...] = tile.astype(jnp.bfloat16)
    o_pair = pltpu.make_async_remote_copy(
        src_ref=oown,
        dst_ref=orecv,
        send_sem=o_send.at[0],
        recv_sem=o_recv.at[0],
        device_id=sibling,
        device_id_type=MESH,
    )
    o_pair.start()

    factor = LOG2E / 8.0

    def q_step(b, carry):
        out = jnp.dot(nb[b].reshape(rows, -1), wq[...], preferred_element_type=jnp.float32)
        out = out.astype(jnp.bfloat16).astype(jnp.float32)
        first, second = out[:, :128], out[:, 128:]
        for group, seg, here in ((0, first, low), (1, first, ~low), (2, second, low)):
            mean = jnp.sum(jnp.where(here, seg * seg, 0.0), axis=-1, keepdims=True) / 64.0
            gain = qg_ref[group : group + 1, :] * factor
            gain = jnp.concatenate([zeros, gain] if group == 1 else [gain, zeros], axis=1)
            scaled = jnp.where(here, seg * lax.rsqrt(mean + EPS) * gain, 0.0)
            if group == 1:
                scaled = pltpu.roll(scaled, 64, 1)
            qn[group, b] = scaled.astype(jnp.bfloat16)
        return carry

    for i in range(batch):
        q_step(i, 0)

    span = wo.shape[1]
    o_pair.wait_recv()
    osum[...] = (oown[...] + orecv[...]).reshape(osum.shape)
    wo[mine] = osum[mine]

    def o_copy(shift):
        return move(osum.at[(mine + shift) % tp], oy_send.at[0], oy_recv.at[0], at_y(shift), wo.at[mine])

    o_all = move(wo.at[pl.ds(0, tp - 1)], oy_send.at[0], oy_recv.at[0], at_y(1))

    for shift in range(1, tp):
        o_copy(shift).start()

    keep = lane >= 64

    def attend(b):
        total = jnp.zeros((rows, 1), jnp.float32)
        summed = jnp.zeros((rows, 128), jnp.float32)
        for group in (2, 1):
            window = wins[group][b]
            scores = lax.dot_general(
                qn[group, b], window, (((1,), (1,)), ((), ())), preferred_element_type=jnp.float32
            )
            grown = jnp.exp2(scores + biases[group][...])
            total = total + jnp.sum(grown, axis=-1, keepdims=True)
            summed = summed + jnp.dot(grown.astype(jnp.bfloat16), window, preferred_element_type=jnp.float32)
        close = length + 2 * REACH[0]
        totals, sums = [], []
        for block in range(2):
            window = win0[b, block * length : block * length + close, :]
            query = qn[0, b, block * length : (block + 1) * length, :]
            scores = lax.dot_general(query, window, (((1,), (1,)), ((), ())), preferred_element_type=jnp.float32)
            grown = jnp.exp2(scores + bias0[block])
            totals.append(jnp.sum(grown, axis=-1, keepdims=True))
            sums.append(jnp.dot(grown.astype(jnp.bfloat16), window, preferred_element_type=jnp.float32))
        total = total + jnp.concatenate(totals, axis=0)
        summed = summed + jnp.concatenate(sums, axis=0)
        merged = jnp.where(keep, summed / total, 0.0)
        merged = jnp.where(core == 0, pltpu.roll(merged, 64, 1), merged).astype(jnp.bfloat16)
        mboth[b] = merged.reshape(2, length, 128)

    def m_copy(b):
        return move(mboth.at[b, other], m_send.at[0], m_recv.at[b], sibling, mrecv.at[b])

    def y_copy(b, shift):
        return move(mg.at[mine, b], y_send.at[0], y_recv.at[b], at_y(shift))

    def y_wait(b):
        move(mg.at[pl.ds(0, tp - 1), b], y_send.at[0], y_recv.at[b], at_y(1)).wait_recv()

    def pass_on(b):
        m_copy(b).wait_recv()
        mg[mine, b] = mboth[b, core] + mrecv[b]
        for shift in range(1, tp):
            y_copy(b, shift).start()

    def attend_step(i, carry):
        b = i
        halo_wait(b)
        attend(b)
        m_copy(b).start()

        @pl.when(i >= 1)
        def _():
            pass_on(i - 1)

        return carry

    lax.fori_loop(0, batch, attend_step, 0)
    pass_on(batch - 1)
    o_all.wait_recv()

    def finish(b, carry):
        y_wait(b)
        final = jnp.zeros((length, span), jnp.float32)
        for part in range(tp):
            final = final + lax.dot_general(
                mg[part, b], wo[part], (((1,), (1,)), ((), ())), preferred_element_type=jnp.float32
            )
        out_ref[b] = final.astype(jnp.bfloat16)
        return carry

    lax.fori_loop(0, batch, finish, 0)
    for chunk in range(3):
        pair(chunk).wait_send()
        sent = bufs[chunk].at[pl.ds(0, CHIPS - 1)]
        move(sent, out_sem.at[chunk], xa_recv.at[chunk], at_x(1)).wait_send()
    nb_all.wait_send()
    for group in range(groups):
        both = wins[group].at[:, pl.ds(0, 2 * REACH[group]), :]
        move(both, halo_send.at[group], halo_recv.at[0, group], at_chip(1)).wait_send()
    o_pair.wait_send()
    o_all.wait_send()
    move(mrecv, m_send.at[0], m_recv.at[0], sibling).wait_send()
    move(mg.at[pl.ds(0, tp - 1)], y_send.at[0], y_recv.at[0], at_y(1)).wait_send()


def body(tp, inputs, norm_gain, query_weight, key_weight, value_weight, query_gain, key_gain, out_weight):
    batch, length, model = inputs.shape
    share, groups, heads, width = query_weight.shape
    span = model // tp
    rows = 2 * length
    bf16 = jnp.bfloat16
    dma = pltpu.SemaphoreType.DMA
    operands = (
        inputs,
        norm_gain.reshape(1, model),
        query_weight,
        key_weight,
        value_weight,
        out_weight.transpose(0, 2, 1),
        query_gain,
        key_gain,
    )
    return pl.pallas_call(
        functools.partial(layer_kernel, tp, batch, length),
        out_shape=jax.ShapeDtypeStruct((batch, length, span), bf16),
        in_specs=[pl.BlockSpec(memory_space=pl.ANY)] * len(operands),
        out_specs=pl.BlockSpec(memory_space=pltpu.VMEM),
        scratch_shapes=[
            *[pltpu.VMEM(operand.shape, operand.dtype) for operand in operands],
            pltpu.VMEM((heads, share, 384 + WB), bf16),
            pltpu.VMEM((CHIPS, 2, share, 128), bf16),
            pltpu.VMEM((CHIPS, 2, share, 256), bf16),
            pltpu.VMEM((CHIPS, 2, share, WB), bf16),
            pltpu.VMEM((model, 384), bf16),
            pltpu.VMEM((model, WB), bf16),
            pltpu.VMEM((batch, 2, length, model), bf16),
            *[pltpu.VMEM((batch, rows + 2 * r, 128), bf16) for r in REACH],
            pltpu.VMEM((groups, batch, rows, 128), bf16),
            pltpu.VMEM((2, length, length + 2 * REACH[0]), jnp.float32),
            *[pltpu.VMEM((rows, rows + 2 * r), jnp.float32) for r in REACH[1:]],
            pltpu.VMEM((tp, span, 128), bf16),
            pltpu.VMEM((model, 128), bf16),
            pltpu.VMEM((model, 128), bf16),
            pltpu.VMEM((tp, span, 128), bf16),
            pltpu.VMEM((batch, 2, length, 128), bf16),
            pltpu.VMEM((batch, length, 128), bf16),
            pltpu.VMEM((tp, batch, length, 128), bf16),
            dma((len(operands),)),
            dma((3,)),
            dma((3,)),
            dma((3,)),
            dma((3,)),
            dma((3, 8)),
            dma((3,)),
            dma((3, 10)),
            dma((3,)),
            dma((1,)),
            dma((1,)),
            dma((groups,)),
            dma((batch, groups)),
            dma((1,)),
            dma((1,)),
            dma((1,)),
            dma((1,)),
            dma((1,)),
            dma((batch,)),
            dma((1,)),
            dma((batch,)),
        ],
        compiler_params=pltpu.CompilerParams(collective_id=0, has_side_effects=True, vmem_limit_bytes=60 * 1024 * 1024),
        name="layer",
    )(*operands)


def solution(mesh):
    in_specs = (
        P(None, "sp", None),
        P(),
        P("sp", None, "tp", None),
        P("sp", None, "tp", None),
        P("sp", None, "tp", None),
        P(),
        P(),
        P("tp", None, "sp"),
    )
    out_specs = P(None, "sp", "tp")
    run = functools.partial(body, mesh.shape["tp"])
    return jax.shard_map(run, mesh=mesh, in_specs=in_specs, out_specs=out_specs, check_vma=False)
```

```python
import functools
import math

import jax
import jax.numpy as jnp
from jax import lax
from jax.experimental import pallas as pl
from jax.experimental.pallas import tpu as pltpu
from jax.sharding import PartitionSpec as P

FOLDED = (2,)
GAPS = ((1, 32), (4, 32), (16, 16))
REACH = tuple(d * h for d, h in GAPS)
EPS = 1e-06
NEG = -1e30
LOG2E = 1.4426950408889634
MESH = pl.DeviceIdType.MESH
NZ, NX = 16, 4
CHIPS = NZ * NX
WB = 256


def layer_kernel(
    tp, batch, length, x_hbm, gain_hbm, qw_hbm, kw_hbm, vw_hbm, ow_hbm, qg_hbm, kg_hbm, out_ref,
    x_ref, gain_ref, qw_ref, kw_ref, vw_ref, ow_ref, qg_ref, kg_ref, slab_ref,
    w2, w01, wb, wk, wq, nb, win0, win1, win2, qn, bias0, bias1, bias2, osum, oown, orecv, wo, mboth, mrecv, mg,
    in_sem, pair_send, pair_recv, local_sem, out_sem, zh_recv, xh_recv, za_recv, xa_recv,
    nb_send, nb_recv, halo_send, halo_recv,
    o_send, o_recv, oy_send, oy_recv, m_send, m_recv, y_send, y_recv,
):
    me = lax.axis_index("sp")
    mine = lax.axis_index("tp")
    groups = len(GAPS)
    core = me % 2
    other = 1 - core
    chip = me // 2
    x = chip % NX
    z = chip // NX
    rows = 2 * length
    wins = (win0, win1, win2)
    biases = (bias0, bias1, bias2)
    bufs = (w2, w01, wb)

    def at_z(offset, on=core):
        return {"sp": (((z + offset + NZ) % NZ) * NX + x) * 2 + on}

    def at_x(offset, on=core):
        return {"sp": (z * NX + (x + offset) % NX) * 2 + on}

    sibling = {"sp": chip * 2 + other}

    def at_chip(offset):
        return {"sp": ((chip + offset + CHIPS) % CHIPS) * 2 + core}

    def at_y(offset):
        return {"tp": (mine + offset) % tp}

    barrier = pltpu.get_barrier_semaphore()

    def greet(target):
        pl.semaphore_signal(barrier, inc=1, device_id=target, device_id_type=MESH)

    targets = [at_z(o) for o in (-4, 4, -3, 3, -2, 2, -1, 1)] + [at_y(o) for o in range(1, tp)]
    targets += [at_x(o) for o in range(1, NX)] + [at_chip(1), at_chip(-1), sibling]
    targets += [at_x(2, other)]
    targets += [at_z(o, other) for o in (-4, 4, -3, 3, -2, 2, -1, 1)]
    for target in targets:
        greet(target)

    fetches = [
        pltpu.make_async_copy(src, dst, in_sem.at[i])
        for i, (src, dst) in enumerate(
            (
                (qw_hbm, qw_ref),
                (kw_hbm, kw_ref),
                (vw_hbm, vw_ref),
                (ow_hbm, ow_ref),
                (qg_hbm, qg_ref),
                (kg_hbm, kg_ref),
                (gain_hbm, gain_ref),
                (x_hbm, x_ref),
            )
        )
    ]
    for fetch in fetches:
        fetch.start()
    for fetch in fetches[:4]:
        fetch.wait()
    for head in range(2):
        pieces = []
        for group in (2, 0, 1):
            pieces += [kw_ref[:, group, head, :], vw_ref[:, group, head, :]]
        pieces += [qw_ref[:, group, head, :] for group in range(groups)]
        pieces = [piece.astype(jnp.float32) for piece in pieces + [ow_ref[head]]]
        slab_ref[head] = jnp.concatenate(pieces, axis=1).astype(jnp.bfloat16)

    pl.semaphore_wait(barrier, len(targets))

    cuts = (pl.ds(0, 128), pl.ds(128, 256), pl.ds(384, WB))

    def pair(chunk):
        return pltpu.make_async_remote_copy(
            src_ref=slab_ref.at[other, :, cuts[chunk]],
            dst_ref=bufs[chunk].at[chip, core],
            send_sem=pair_send.at[chunk],
            recv_sem=pair_recv.at[chunk],
            device_id=sibling,
            device_id_type=MESH,
        )

    def local(chunk):
        return pltpu.make_async_copy(
            slab_ref.at[core, :, cuts[chunk]], bufs[chunk].at[chip, core], local_sem.at[chunk]
        )

    def index_of(origin, column):
        return ((z + origin + NZ) % NZ) * NX + (x + column) % NX

    def move(block, send_sem, recv_sem, target, land=None):
        return pltpu.make_async_remote_copy(
            src_ref=block,
            dst_ref=block if land is None else land,
            send_sem=send_sem,
            recv_sem=recv_sem,
            device_id=target,
            device_id_type=MESH,
        )

    def zh_start(chunk, step):
        for on in (core, other):
            move(
                slab_ref.at[on, :, cuts[chunk]],
                out_sem.at[chunk],
                zh_recv.at[chunk, 3 - step if step < 0 else step - 1],
                at_z(step, on),
                bufs[chunk].at[chip, core],
            ).start()

    def zh_wait(chunk, origin):
        block = bufs[chunk].at[index_of(origin, 0)]
        slot = 3 + origin if origin > 0 else -origin - 1
        move(block, out_sem.at[chunk], zh_recv.at[chunk, slot], at_z(1)).wait_recv()

    def xh_start(chunk):
        for on in (core, other):
            move(
                slab_ref.at[on, :, cuts[chunk]],
                out_sem.at[chunk],
                xh_recv.at[chunk],
                at_x(2, on),
                bufs[chunk].at[chip, core],
            ).start()

    def xh_wait(chunk):
        move(bufs[chunk].at[index_of(0, 2)], out_sem.at[chunk], xh_recv.at[chunk], at_x(1)).wait_recv()

    def slot_of(rel, fold):
        if fold == 0:
            return rel - 5
        return {4: 7, NZ - 4: 8}.get(rel, 9)

    def za_start(chunk, origin, step, fold=0):
        slot = slot_of((origin - step) % NZ, fold)
        block = bufs[chunk].at[index_of(origin, 2 * fold)]
        move(block, out_sem.at[chunk], za_recv.at[chunk, slot], at_z(step)).start()

    def za_wait(chunk, origin, fold=0):
        block = bufs[chunk].at[index_of(origin, 2 * fold)]
        move(block, out_sem.at[chunk], za_recv.at[chunk, slot_of(origin % NZ, fold)], at_z(1)).wait_recv()

    def shifts(chunk):
        return (1, 3) if chunk in FOLDED else (1, 3, 2)

    def xa_start(chunk, origin):
        block = bufs[chunk].at[index_of(origin, 0)]
        for shift in shifts(chunk):
            move(block, out_sem.at[chunk], xa_recv.at[chunk], at_x(shift)).start()

    far = {4: ((-3, -1, -2), (-4, -3, -1, -2)), -4: ((4, 3, 1, 2), (3, 1, 2))}

    for step in (4, -4, 3, -3, 1, -1, 2, -2):
        zh_start(0, step)
    for steps in ((4, -4), (1, -1, 2, -2, 3, -3)):
        for chunk in (1, 2):
            for step in steps:
                zh_start(chunk, step)
    for chunk in FOLDED:
        xh_start(chunk)
    for chunk in range(3):
        local(chunk).start()
        pair(chunk).start()

    def nb_copy(b):
        return move(nb.at[b, core], nb_send.at[0], nb_recv.at[0], sibling)

    def norm_step(b, carry):
        flat = x_ref[b].astype(jnp.float32)
        scale = lax.rsqrt(jnp.mean(flat * flat, axis=-1, keepdims=True) + EPS)
        nb[b, core] = (flat * scale * gain_ref[...]).astype(jnp.bfloat16)
        nb_copy(b).start()
        return carry

    for fetch in fetches[4:]:
        fetch.wait()
    lax.fori_loop(0, batch, norm_step, 0)

    for chunk in range(3):
        local(chunk).wait()
        pair(chunk).wait_recv()
        xa_start(chunk, 0)

    def near(chunk, spread):
        for origin in (1, -1, 2, -2):
            zh_wait(chunk, origin)
            if spread:
                xa_start(chunk, origin)
        for origin in (4, -4):
            zh_wait(chunk, origin)
            for step in far[origin][chunk % 2]:
                za_start(chunk, origin, step)
        for origin in (3, -3):
            zh_wait(chunk, origin)
            if spread:
                xa_start(chunk, origin)
        if spread:
            for origin in (4, -4):
                xa_start(chunk, origin)

    near(0, True)
    for chunk in FOLDED:
        xh_wait(chunk)
        for step in (4, -4, 3, -3, 1, -1, 2, -2):
            za_start(chunk, 0, step, 1)
    near(1, True)
    near(2, True)

    head = mine * 2 + core
    heads = 2 * tp
    power = -8.0 * (head + 1).astype(jnp.float32) / heads
    slope = jnp.exp2(jnp.full((8, 128), power, jnp.float32))[:1, :1] * LOG2E
    total_rows = CHIPS * rows

    def bias_of(group, count, first):
        dilation, half = GAPS[group]
        reach = REACH[group]
        shape = (count, count + 2 * reach)
        key = lax.broadcasted_iota(jnp.int32, shape, 1) - reach
        offset = jnp.abs(key - lax.broadcasted_iota(jnp.int32, shape, 0))
        at = key + (chip * rows + first)
        allowed = (offset <= reach) & (at >= 0) & (at < total_rows) & ((offset & (dilation - 1)) == 0)
        return jnp.where(allowed, offset.astype(jnp.float32) * (-slope / float(reach)), NEG)

    for block in range(2):
        bias0[block] = bias_of(0, length, block * length)
    for group in (1, 2):
        biases[group][...] = bias_of(group, rows, 0)

    late = (5, -5, 6, -6, 7, -7, 8)
    def fold_on(chunk):
        for origin in (4, -4):
            za_wait(chunk, origin, 1)
            for step in far[origin][1 - chunk % 2]:
                za_start(chunk, origin, step, 1)

    def late_on(chunk, part):
        for origin in part:
            za_wait(chunk, origin)
            xa_start(chunk, origin)

    late_on(0, late[:4])
    for chunk in FOLDED:
        fold_on(chunk)
    late_on(0, late[4:])
    late_on(1, late)
    late_on(2, late)

    lane = lax.broadcasted_iota(jnp.int32, (rows, 128), 1)
    low = lane < 64
    origins = (0, 1, -1, 2, -2, 3, -3, 4, -4) + late

    def all_blocks(chunk):
        several = bufs[chunk].at[pl.ds(0, NZ * len(shifts(chunk)))]
        move(several, out_sem.at[chunk], xa_recv.at[chunk], at_x(1)).wait_recv()
        if chunk in FOLDED:
            several = bufs[chunk].at[pl.ds(0, NZ - 3)]
            move(several, out_sem.at[chunk], za_recv.at[chunk, 9], at_x(1)).wait_recv()

    def sent_all(chunk):
        move(bufs[chunk].at[pl.ds(0, CHIPS - 1)], out_sem.at[chunk], xa_recv.at[chunk], at_x(1)).wait_send()

    all_blocks(0)
    wk[:, :128] = w2[...].reshape(wk.shape[0], 128)
    nb_all = move(nb.at[:, 0], nb_send.at[0], nb_recv.at[0], sibling)
    nb_all.wait_recv()

    def halo(b, group, up):
        reach = REACH[group]
        begin_at, land_at = (rows, 0) if up else (reach, reach + rows)
        return pltpu.make_async_remote_copy(
            src_ref=wins[group].at[b, pl.ds(begin_at, reach), :],
            dst_ref=wins[group].at[b, pl.ds(land_at, reach), :],
            send_sem=halo_send.at[group],
            recv_sem=halo_recv.at[b, group],
            device_id=at_chip(1 if up else -1),
            device_id_type=MESH,
        )

    def halo_wait(b):
        for group in (2, 1, 0):
            both = wins[group].at[b, pl.ds(0, 2 * REACH[group]), :]
            move(both, halo_send.at[group], halo_recv.at[b, group], at_chip(1)).wait_recv()

    ones = jnp.ones((1, 64), jnp.float32)
    zeros = jnp.zeros((1, 64), jnp.float32)

    def key_norm(out, place, group):
        seg = out[:, 128 * place : 128 * (place + 1)].astype(jnp.bfloat16).astype(jnp.float32)
        mean = jnp.sum(jnp.where(low, seg * seg, 0.0), axis=-1, keepdims=True) / 64.0
        gain = jnp.concatenate([kg_ref[group : group + 1, :], ones], axis=1)
        return (seg * jnp.where(low, lax.rsqrt(mean + EPS), 1.0) * gain).astype(jnp.bfloat16)

    def key_step(b, first, order):
        out = jnp.dot(nb[b].reshape(rows, -1), wk[:, first : first + 128 * len(order)], preferred_element_type=jnp.float32)
        for place, group in enumerate(order):
            wins[group][b, REACH[group] : REACH[group] + rows, :] = key_norm(out, place, group)
        for group in order:
            halo(b, group, False).start()
            if group == 2:

                @pl.when(x != NX - 1)
                def _():
                    halo(b, 2, True).start()

            else:
                halo(b, group, True).start()

    for b in range(batch):
        key_step(b, 0, (2,))
    all_blocks(1)
    sent_all(2)

    @pl.when(x == NX - 1)
    def _():
        for b in range(batch):
            halo(b, 2, True).start()

    wk[:, 128:] = w01[...].reshape(wk.shape[0], 256)
    for b in range(batch):
        key_step(b, 128, (0, 1))

    all_blocks(2)
    wq[...] = wb[...].reshape(wq.shape)

    tile = wq[:, 128:].astype(jnp.float32)
    high = lax.broadcasted_iota(jnp.int32, tile.shape, 1) >= 64
    tile = jnp.where(high, tile, 0.0)
    tile = jnp.where(core == 0, pltpu.roll(tile, 64, 1), tile)
    oown[...] = tile.astype(jnp.bfloat16)
    o_pair = pltpu.make_async_remote_copy(
        src_ref=oown,
        dst_ref=orecv,
        send_sem=o_send.at[0],
        recv_sem=o_recv.at[0],
        device_id=sibling,
        device_id_type=MESH,
    )
    o_pair.start()

    factor = LOG2E / 8.0

    def q_step(b, carry):
        out = jnp.dot(nb[b].reshape(rows, -1), wq[...], preferred_element_type=jnp.float32)
        out = out.astype(jnp.bfloat16).astype(jnp.float32)
        first, second = out[:, :128], out[:, 128:]
        for group, seg, here in ((0, first, low), (1, first, ~low), (2, second, low)):
            mean = jnp.sum(jnp.where(here, seg * seg, 0.0), axis=-1, keepdims=True) / 64.0
            gain = qg_ref[group : group + 1, :] * factor
            gain = jnp.concatenate([zeros, gain] if group == 1 else [gain, zeros], axis=1)
            scaled = jnp.where(here, seg * lax.rsqrt(mean + EPS) * gain, 0.0)
            if group == 1:
                scaled = pltpu.roll(scaled, 64, 1)
            qn[group, b] = scaled.astype(jnp.bfloat16)
        return carry

    for i in range(batch):
        q_step(i, 0)

    span = wo.shape[1]
    o_pair.wait_recv()
    osum[...] = (oown[...] + orecv[...]).reshape(osum.shape)
    wo[mine] = osum[mine]

    def o_copy(shift):
        return move(osum.at[(mine + shift) % tp], oy_send.at[0], oy_recv.at[0], at_y(shift), wo.at[mine])

    o_all = move(wo.at[pl.ds(0, tp - 1)], oy_send.at[0], oy_recv.at[0], at_y(1))

    for shift in range(1, tp):
        o_copy(shift).start()

    def merge(total, summed):
        merged = jnp.where(lax.broadcasted_iota(jnp.int32, summed.shape, 1) >= 64, summed / total, 0.0)
        return jnp.where(core == 0, pltpu.roll(merged, 64, 1), merged).astype(jnp.bfloat16)

    def close_part(b, block):
        begin = block * length if isinstance(block, int) else pl.multiple_of(block * length, length)
        window = win0[b, pl.ds(begin, length + 2 * REACH[0]), :]
        query = qn[0, b, pl.ds(begin, length), :]
        scores = lax.dot_general(query, window, (((1,), (1,)), ((), ())), preferred_element_type=jnp.float32)
        grown = jnp.exp2(scores + bias0[block])
        total = jnp.sum(grown, axis=-1, keepdims=True)
        return total, jnp.dot(grown.astype(jnp.bfloat16), window, preferred_element_type=jnp.float32)

    def wide_part(b, group, begin, count):
        window = wins[group][b, pl.ds(begin, count + 2 * REACH[group]), :]
        query = qn[group, b, pl.ds(begin, count), :]
        scores = lax.dot_general(query, window, (((1,), (1,)), ((), ())), preferred_element_type=jnp.float32)
        first = begin if isinstance(begin, int) else pl.multiple_of(begin, length)
        bias = biases[group][pl.ds(0, count), pl.ds(0, count + 2 * REACH[group])]
        if count != rows:
            bias = biases[group][pl.ds(first, count), pl.ds(first, count + 2 * REACH[group])]
        grown = jnp.exp2(scores + bias)
        total = jnp.sum(grown, axis=-1, keepdims=True)
        return total, jnp.dot(grown.astype(jnp.bfloat16), window, preferred_element_type=jnp.float32)

    def attend(b):
        total, summed = wide_part(b, 2, 0, rows)
        for part_total, part_sum in [
            wide_part(b, 1, 0, rows),
            [jnp.concatenate(both, axis=0) for both in zip(close_part(b, 0), close_part(b, 1))],
        ]:
            total, summed = total + part_total, summed + part_sum
        mboth[b] = merge(total, summed).reshape(2, length, 128)

    def attend_block(b, block):
        begin = pl.multiple_of(block * length, length)
        total, summed = wide_part(b, 2, begin, length)
        for part_total, part_sum in (wide_part(b, 1, begin, length), close_part(b, block)):
            total, summed = total + part_total, summed + part_sum
        mboth[b, block] = merge(total, summed)

    def m_copy(b):
        return move(mboth.at[b, other], m_send.at[0], m_recv.at[b], sibling, mrecv.at[b])

    def y_copy(b, shift):
        return move(mg.at[mine, b], y_send.at[0], y_recv.at[b], at_y(shift))

    def y_wait(b):
        move(mg.at[pl.ds(0, tp - 1), b], y_send.at[0], y_recv.at[b], at_y(1)).wait_recv()

    def pass_on(b):
        m_copy(b).wait_recv()
        mg[mine, b] = mboth[b, core] + mrecv[b]
        for shift in range(1, tp):
            y_copy(b, shift).start()

    def attend_step(i, carry):
        b = i
        halo_wait(b)
        attend(b)
        m_copy(b).start()

        @pl.when(i >= 1)
        def _():
            pass_on(i - 1)

        return carry

    lax.fori_loop(0, batch - 1, attend_step, 0)
    last = batch - 1
    halo_wait(last)
    attend_block(last, other)
    m_copy(last).start()
    pass_on(last - 1)
    attend_block(last, core)
    pass_on(batch - 1)
    o_all.wait_recv()

    def finish(b, carry):
        y_wait(b)
        final = jnp.zeros((length, span), jnp.float32)
        for part in range(tp):
            final = final + lax.dot_general(
                mg[part, b], wo[part], (((1,), (1,)), ((), ())), preferred_element_type=jnp.float32
            )
        out_ref[b] = final.astype(jnp.bfloat16)
        return carry

    lax.fori_loop(0, batch, finish, 0)
    for chunk in range(3):
        pair(chunk).wait_send()
        if chunk < 2:
            sent_all(chunk)
    nb_all.wait_send()
    for group in range(groups):
        both = wins[group].at[:, pl.ds(0, 2 * REACH[group]), :]
        move(both, halo_send.at[group], halo_recv.at[0, group], at_chip(1)).wait_send()
    o_pair.wait_send()
    o_all.wait_send()
    move(mrecv, m_send.at[0], m_recv.at[0], sibling).wait_send()
    move(mg.at[pl.ds(0, tp - 1)], y_send.at[0], y_recv.at[0], at_y(1)).wait_send()


def body(tp, inputs, norm_gain, query_weight, key_weight, value_weight, query_gain, key_gain, out_weight):
    batch, length, model = inputs.shape
    share, groups, heads, width = query_weight.shape
    span = model // tp
    rows = 2 * length
    bf16 = jnp.bfloat16
    dma = pltpu.SemaphoreType.DMA
    operands = (
        inputs,
        norm_gain.reshape(1, model),
        query_weight,
        key_weight,
        value_weight,
        out_weight.transpose(0, 2, 1),
        query_gain,
        key_gain,
    )
    return pl.pallas_call(
        functools.partial(layer_kernel, tp, batch, length),
        out_shape=jax.ShapeDtypeStruct((batch, length, span), bf16),
        in_specs=[pl.BlockSpec(memory_space=pl.ANY)] * len(operands),
        out_specs=pl.BlockSpec(memory_space=pltpu.VMEM),
        scratch_shapes=[
            *[pltpu.VMEM(operand.shape, operand.dtype) for operand in operands],
            pltpu.VMEM((heads, share, 384 + WB), bf16),
            pltpu.VMEM((CHIPS, 2, share, 128), bf16),
            pltpu.VMEM((CHIPS, 2, share, 256), bf16),
            pltpu.VMEM((CHIPS, 2, share, WB), bf16),
            pltpu.VMEM((model, 384), bf16),
            pltpu.VMEM((model, WB), bf16),
            pltpu.VMEM((batch, 2, length, model), bf16),
            *[pltpu.VMEM((batch, rows + 2 * r, 128), bf16) for r in REACH],
            pltpu.VMEM((groups, batch, rows, 128), bf16),
            pltpu.VMEM((2, length, length + 2 * REACH[0]), jnp.float32),
            *[pltpu.VMEM((rows, rows + 2 * r), jnp.float32) for r in REACH[1:]],
            pltpu.VMEM((tp, span, 128), bf16),
            pltpu.VMEM((model, 128), bf16),
            pltpu.VMEM((model, 128), bf16),
            pltpu.VMEM((tp, span, 128), bf16),
            pltpu.VMEM((batch, 2, length, 128), bf16),
            pltpu.VMEM((batch, length, 128), bf16),
            pltpu.VMEM((tp, batch, length, 128), bf16),
            dma((len(operands),)),
            dma((3,)),
            dma((3,)),
            dma((3,)),
            dma((3,)),
            dma((3, 8)),
            dma((3,)),
            dma((3, 10)),
            dma((3,)),
            dma((1,)),
            dma((1,)),
            dma((groups,)),
            dma((batch, groups)),
            dma((1,)),
            dma((1,)),
            dma((1,)),
            dma((1,)),
            dma((1,)),
            dma((batch,)),
            dma((1,)),
            dma((batch,)),
        ],
        compiler_params=pltpu.CompilerParams(collective_id=0, has_side_effects=True, vmem_limit_bytes=60 * 1024 * 1024),
        name="layer",
    )(*operands)


def solution(mesh):
    in_specs = (
        P(None, "sp", None),
        P(),
        P("sp", None, "tp", None),
        P("sp", None, "tp", None),
        P("sp", None, "tp", None),
        P(),
        P(),
        P("tp", None, "sp"),
    )
    out_specs = P(None, "sp", "tp")
    run = functools.partial(body, mesh.shape["tp"])
    return jax.shard_map(run, mesh=mesh, in_specs=in_specs, out_specs=out_specs, check_vma=False)
```

```python
import functools
import math

import jax
import jax.numpy as jnp
from jax import lax
from jax.experimental import pallas as pl
from jax.experimental.pallas import tpu as pltpu
from jax.sharding import PartitionSpec as P

FOLDED = (2,)
GAPS = ((1, 32), (4, 32), (16, 16))
REACH = tuple(d * h for d, h in GAPS)
EPS = 1e-06
NEG = -1e30
LOG2E = 1.4426950408889634
MESH = pl.DeviceIdType.MESH
NZ, NX = 16, 4
CHIPS = NZ * NX
WB = 256


def layer_kernel(
    tp, batch, length, x_hbm, gain_hbm, qw_hbm, kw_hbm, vw_hbm, ow_hbm, qg_hbm, kg_hbm, out_ref,
    x_ref, gain_ref, qw_ref, kw_ref, vw_ref, ow_ref, qg_ref, kg_ref, slab_ref,
    w2, w01, wb, wk, wq, nb, win0, win1, win2, qn, bias0, bias1, bias2, osum, oown, orecv, wo, mboth, mrecv, mg,
    in_sem, pair_send, pair_recv, local_sem, out_sem, zh_recv, xh_recv, za_recv, xa_recv,
    nb_send, nb_recv, halo_send, halo_recv,
    o_send, o_recv, oy_send, oy_recv, m_send, m_recv, y_send, y_recv, outs, out_move,
):
    me = lax.axis_index("sp")
    mine = lax.axis_index("tp")
    groups = len(GAPS)
    core = me % 2
    other = 1 - core
    chip = me // 2
    x = chip % NX
    z = chip // NX
    rows = 2 * length
    wins = (win0, win1, win2)
    biases = (bias0, bias1, bias2)
    bufs = (w2, w01, wb)

    def at_z(offset, on=core):
        return {"sp": (((z + offset + NZ) % NZ) * NX + x) * 2 + on}

    def at_x(offset, on=core):
        return {"sp": (z * NX + (x + offset) % NX) * 2 + on}

    sibling = {"sp": chip * 2 + other}

    def at_chip(offset):
        return {"sp": ((chip + offset + CHIPS) % CHIPS) * 2 + core}

    def at_y(offset):
        return {"tp": (mine + offset) % tp}

    barrier = pltpu.get_barrier_semaphore()

    def greet(target):
        pl.semaphore_signal(barrier, inc=1, device_id=target, device_id_type=MESH)

    targets = [at_z(o) for o in (-4, 4, -3, 3, -2, 2, -1, 1)] + [at_y(o) for o in range(1, tp)]
    targets += [at_x(o) for o in range(1, NX)] + [at_chip(1), at_chip(-1), sibling]
    targets += [at_x(2, other)]
    targets += [at_z(o, other) for o in (-4, 4, -3, 3, -2, 2, -1, 1)]
    for target in targets:
        greet(target)

    fetches = [
        pltpu.make_async_copy(src, dst, in_sem.at[i])
        for i, (src, dst) in enumerate(
            (
                (qw_hbm, qw_ref),
                (kw_hbm, kw_ref),
                (vw_hbm, vw_ref),
                (ow_hbm, ow_ref),
                (qg_hbm, qg_ref),
                (kg_hbm, kg_ref),
                (gain_hbm, gain_ref),
                (x_hbm, x_ref),
            )
        )
    ]
    for fetch in fetches:
        fetch.start()
    for fetch in fetches[:4]:
        fetch.wait()
    for head in range(2):
        pieces = []
        for group in (2, 0, 1):
            pieces += [kw_ref[:, group, head, :], vw_ref[:, group, head, :]]
        pieces += [qw_ref[:, group, head, :] for group in range(groups)]
        pieces = [piece.astype(jnp.float32) for piece in pieces + [ow_ref[head]]]
        slab_ref[head] = jnp.concatenate(pieces, axis=1).astype(jnp.bfloat16)

    pl.semaphore_wait(barrier, len(targets))

    cuts = (pl.ds(0, 128), pl.ds(128, 256), pl.ds(384, WB))

    def pair(chunk):
        return pltpu.make_async_remote_copy(
            src_ref=slab_ref.at[other, :, cuts[chunk]],
            dst_ref=bufs[chunk].at[chip, core],
            send_sem=pair_send.at[0],
            recv_sem=pair_recv.at[0],
            device_id=sibling,
            device_id_type=MESH,
        )

    def local(chunk):
        return pltpu.make_async_copy(
            slab_ref.at[core, :, cuts[chunk]], bufs[chunk].at[chip, core], local_sem.at[0]
        )

    def index_of(origin, column):
        return ((z + origin + NZ) % NZ) * NX + (x + column) % NX

    def move(block, send_sem, recv_sem, target, land=None):
        return pltpu.make_async_remote_copy(
            src_ref=block,
            dst_ref=block if land is None else land,
            send_sem=send_sem,
            recv_sem=recv_sem,
            device_id=target,
            device_id_type=MESH,
        )

    def zh_start(chunk, step):
        for on in (core, other):
            move(
                slab_ref.at[on, :, cuts[chunk]],
                out_sem.at[chunk],
                zh_recv.at[chunk, 3 - step if step < 0 else step - 1],
                at_z(step, on),
                bufs[chunk].at[chip, core],
            ).start()

    def zh_wait(chunk, origin):
        block = bufs[chunk].at[index_of(origin, 0)]
        slot = 3 + origin if origin > 0 else -origin - 1
        move(block, out_sem.at[chunk], zh_recv.at[chunk, slot], at_z(1)).wait_recv()

    def xh_start(chunk):
        for on in (core, other):
            move(
                slab_ref.at[on, :, cuts[chunk]],
                out_sem.at[chunk],
                xh_recv.at[chunk],
                at_x(2, on),
                bufs[chunk].at[chip, core],
            ).start()

    def xh_wait(chunk):
        move(bufs[chunk].at[index_of(0, 2)], out_sem.at[chunk], xh_recv.at[chunk], at_x(1)).wait_recv()

    def slot_of(rel, fold):
        if fold == 0:
            return rel - 5
        return {4: 7, NZ - 4: 8}.get(rel, 9)

    def za_start(chunk, origin, step, fold=0):
        slot = slot_of((origin - step) % NZ, fold)
        block = bufs[chunk].at[index_of(origin, 2 * fold)]
        move(block, out_sem.at[chunk], za_recv.at[chunk, slot], at_z(step)).start()

    def za_wait(chunk, origin, fold=0):
        block = bufs[chunk].at[index_of(origin, 2 * fold)]
        move(block, out_sem.at[chunk], za_recv.at[chunk, slot_of(origin % NZ, fold)], at_z(1)).wait_recv()

    def shifts(chunk):
        return (1, 3) if chunk in FOLDED else (1, 3, 2)

    def xa_start(chunk, origin):
        block = bufs[chunk].at[index_of(origin, 0)]
        for shift in shifts(chunk):
            move(block, out_sem.at[chunk], xa_recv.at[chunk], at_x(shift)).start()

    far = {4: ((-3, -1, -2), (-4, -3, -1, -2)), -4: ((4, 3, 1, 2), (3, 1, 2))}

    for step in (4, -4, 3, -3, 1, -1, 2, -2):
        zh_start(0, step)
    for steps in ((4, -4), (1, -1, 2, -2, 3, -3)):
        for chunk in (1, 2):
            for step in steps:
                zh_start(chunk, step)
    for chunk in FOLDED:
        xh_start(chunk)
    for chunk in range(3):
        local(chunk).start()
        pair(chunk).start()

    def nb_copy(b):
        return move(nb.at[b, core], nb_send.at[0], nb_recv.at[0], sibling)

    def norm_step(b, carry):
        flat = x_ref[b].astype(jnp.float32)
        scale = lax.rsqrt(jnp.mean(flat * flat, axis=-1, keepdims=True) + EPS)
        nb[b, core] = (flat * scale * gain_ref[...]).astype(jnp.bfloat16)
        nb_copy(b).start()
        return carry

    for fetch in fetches[4:]:
        fetch.wait()
    lax.fori_loop(0, batch, norm_step, 0)

    pair_all = move(slab_ref.at[0], pair_send.at[0], pair_recv.at[0], sibling)
    pltpu.make_async_copy(slab_ref.at[0], slab_ref.at[1], local_sem.at[0]).wait()
    pair_all.wait_recv()
    for chunk in range(3):
        xa_start(chunk, 0)

    def near(chunk, spread):
        for origin in (1, -1, 2, -2):
            zh_wait(chunk, origin)
            if spread:
                xa_start(chunk, origin)
        for origin in (4, -4):
            zh_wait(chunk, origin)
            for step in far[origin][chunk % 2]:
                za_start(chunk, origin, step)
        for origin in (3, -3):
            zh_wait(chunk, origin)
            if spread:
                xa_start(chunk, origin)
        if spread:
            for origin in (4, -4):
                xa_start(chunk, origin)

    near(0, True)
    for chunk in FOLDED:
        xh_wait(chunk)
        for step in (4, -4, 3, -3, 1, -1, 2, -2):
            za_start(chunk, 0, step, 1)
    near(1, True)
    near(2, True)

    head = mine * 2 + core
    heads = 2 * tp
    power = -8.0 * (head + 1).astype(jnp.float32) / heads
    slope = jnp.exp2(jnp.full((8, 128), power, jnp.float32))[:1, :1] * LOG2E
    total_rows = CHIPS * rows

    def bias_of(group, count, first):
        dilation, half = GAPS[group]
        reach = REACH[group]
        shape = (count, count + 2 * reach)
        key = lax.broadcasted_iota(jnp.int32, shape, 1) - reach
        offset = jnp.abs(key - lax.broadcasted_iota(jnp.int32, shape, 0))
        at = key + (chip * rows + first)
        allowed = (offset <= reach) & (at >= 0) & (at < total_rows) & ((offset & (dilation - 1)) == 0)
        return jnp.where(allowed, offset.astype(jnp.float32) * (-slope / float(reach)), NEG)

    for block in range(2):
        bias0[block] = bias_of(0, length, block * length)
    for group in (1, 2):
        biases[group][...] = bias_of(group, rows, 0)

    late = (5, -5, 6, -6, 7, -7, 8)
    def fold_on(chunk):
        for origin in (4, -4):
            za_wait(chunk, origin, 1)
            for step in far[origin][1 - chunk % 2]:
                za_start(chunk, origin, step, 1)

    def late_on(chunk, part):
        for origin in part:
            za_wait(chunk, origin)
            xa_start(chunk, origin)

    late_on(0, late[:4])
    for chunk in FOLDED:
        fold_on(chunk)
    late_on(0, late[4:])
    late_on(1, late)
    late_on(2, late)

    lane = lax.broadcasted_iota(jnp.int32, (rows, 128), 1)
    low = lane < 64
    origins = (0, 1, -1, 2, -2, 3, -3, 4, -4) + late

    def all_blocks(chunk):
        several = bufs[chunk].at[pl.ds(0, NZ * len(shifts(chunk)))]
        move(several, out_sem.at[chunk], xa_recv.at[chunk], at_x(1)).wait_recv()
        if chunk in FOLDED:
            several = bufs[chunk].at[pl.ds(0, NZ - 3)]
            move(several, out_sem.at[chunk], za_recv.at[chunk, 9], at_x(1)).wait_recv()

    def sent_all(chunk):
        move(bufs[chunk].at[pl.ds(0, CHIPS - 1)], out_sem.at[chunk], xa_recv.at[chunk], at_x(1)).wait_send()

    all_blocks(0)
    wk[:, :128] = w2[...].reshape(wk.shape[0], 128)
    nb_all = move(nb.at[:, 0], nb_send.at[0], nb_recv.at[0], sibling)
    nb_all.wait_recv()

    def halo(b, group, up):
        reach = REACH[group]
        begin_at, land_at = (rows, 0) if up else (reach, reach + rows)
        return pltpu.make_async_remote_copy(
            src_ref=wins[group].at[b, pl.ds(begin_at, reach), :],
            dst_ref=wins[group].at[b, pl.ds(land_at, reach), :],
            send_sem=halo_send.at[group],
            recv_sem=halo_recv.at[b, group],
            device_id=at_chip(1 if up else -1),
            device_id_type=MESH,
        )

    def halo_wait(b):
        for group in (2, 1, 0):
            both = wins[group].at[b, pl.ds(0, 2 * REACH[group]), :]
            move(both, halo_send.at[group], halo_recv.at[b, group], at_chip(1)).wait_recv()

    ones = jnp.ones((1, 64), jnp.float32)
    zeros = jnp.zeros((1, 64), jnp.float32)

    def key_norm(out, place, group):
        seg = out[:, 128 * place : 128 * (place + 1)].astype(jnp.bfloat16).astype(jnp.float32)
        mean = jnp.sum(jnp.where(low, seg * seg, 0.0), axis=-1, keepdims=True) / 64.0
        gain = jnp.concatenate([kg_ref[group : group + 1, :], ones], axis=1)
        return (seg * jnp.where(low, lax.rsqrt(mean + EPS), 1.0) * gain).astype(jnp.bfloat16)

    def key_step(b, first, order):
        out = jnp.dot(nb[b].reshape(rows, -1), wk[:, first : first + 128 * len(order)], preferred_element_type=jnp.float32)
        for place, group in enumerate(order):
            wins[group][b, REACH[group] : REACH[group] + rows, :] = key_norm(out, place, group)
        for group in order:
            for up in (True, False):
                if group == 2:

                    @pl.when(x != (NX - 1 if up else 0))
                    def _(up=up):
                        halo(b, 2, up).start()

                else:
                    halo(b, group, up).start()

    for b in range(batch):
        key_step(b, 0, (2,))
    all_blocks(1)
    sent_all(2)

    for up in (True, False):

        @pl.when(x == (NX - 1 if up else 0))
        def _(up=up):
            for b in range(batch):
                halo(b, 2, up).start()

    wk[:, 128:] = w01[...].reshape(wk.shape[0], 256)
    for b in range(batch):
        key_step(b, 128, (0, 1))

    all_blocks(2)
    wq[...] = wb[...].reshape(wq.shape)

    tile = wq[:, 128:].astype(jnp.float32)
    high = lax.broadcasted_iota(jnp.int32, tile.shape, 1) >= 64
    tile = jnp.where(high, tile, 0.0)
    tile = jnp.where(core == 0, pltpu.roll(tile, 64, 1), tile)
    oown[...] = tile.astype(jnp.bfloat16)
    o_pair = pltpu.make_async_remote_copy(
        src_ref=oown,
        dst_ref=orecv,
        send_sem=o_send.at[0],
        recv_sem=o_recv.at[0],
        device_id=sibling,
        device_id_type=MESH,
    )
    o_pair.start()

    factor = LOG2E / 8.0

    def q_step(b, carry):
        out = jnp.dot(nb[b].reshape(rows, -1), wq[...], preferred_element_type=jnp.float32)
        out = out.astype(jnp.bfloat16).astype(jnp.float32)
        first, second = out[:, :128], out[:, 128:]
        for group, seg, here in ((0, first, low), (1, first, ~low), (2, second, low)):
            mean = jnp.sum(jnp.where(here, seg * seg, 0.0), axis=-1, keepdims=True) / 64.0
            gain = qg_ref[group : group + 1, :] * factor
            gain = jnp.concatenate([zeros, gain] if group == 1 else [gain, zeros], axis=1)
            scaled = jnp.where(here, seg * lax.rsqrt(mean + EPS) * gain, 0.0)
            if group == 1:
                scaled = pltpu.roll(scaled, 64, 1)
            qn[group, b] = scaled.astype(jnp.bfloat16)
        return carry

    for i in range(batch):
        q_step(i, 0)

    span = wo.shape[1]
    o_pair.wait_recv()
    osum[...] = (oown[...] + orecv[...]).reshape(osum.shape)
    wo[mine] = osum[mine]

    def o_copy(shift):
        return move(osum.at[(mine + shift) % tp], oy_send.at[0], oy_recv.at[0], at_y(shift), wo.at[mine])

    o_all = move(wo.at[pl.ds(0, tp - 1)], oy_send.at[0], oy_recv.at[0], at_y(1))

    for shift in range(1, tp):
        o_copy(shift).start()

    def merge(total, summed):
        merged = jnp.where(lax.broadcasted_iota(jnp.int32, summed.shape, 1) >= 64, summed / total, 0.0)
        return jnp.where(core == 0, pltpu.roll(merged, 64, 1), merged).astype(jnp.bfloat16)

    def close_part(b, block):
        begin = block * length if isinstance(block, int) else pl.multiple_of(block * length, length)
        window = win0[b, pl.ds(begin, length + 2 * REACH[0]), :]
        query = qn[0, b, pl.ds(begin, length), :]
        scores = lax.dot_general(query, window, (((1,), (1,)), ((), ())), preferred_element_type=jnp.float32)
        grown = jnp.exp2(scores + bias0[block])
        total = jnp.sum(grown, axis=-1, keepdims=True)
        return total, jnp.dot(grown.astype(jnp.bfloat16), window, preferred_element_type=jnp.float32)

    def wide_part(b, group, begin, count):
        window = wins[group][b, pl.ds(begin, count + 2 * REACH[group]), :]
        query = qn[group, b, pl.ds(begin, count), :]
        scores = lax.dot_general(query, window, (((1,), (1,)), ((), ())), preferred_element_type=jnp.float32)
        first = begin if isinstance(begin, int) else pl.multiple_of(begin, length)
        bias = biases[group][pl.ds(0, count), pl.ds(0, count + 2 * REACH[group])]
        if count != rows:
            bias = biases[group][pl.ds(first, count), pl.ds(first, count + 2 * REACH[group])]
        grown = jnp.exp2(scores + bias)
        total = jnp.sum(grown, axis=-1, keepdims=True)
        return total, jnp.dot(grown.astype(jnp.bfloat16), window, preferred_element_type=jnp.float32)

    def attend(b):
        total, summed = wide_part(b, 2, 0, rows)
        for part_total, part_sum in [
            wide_part(b, 1, 0, rows),
            [jnp.concatenate(both, axis=0) for both in zip(close_part(b, 0), close_part(b, 1))],
        ]:
            total, summed = total + part_total, summed + part_sum
        mboth[b] = merge(total, summed).reshape(2, length, 128)

    def attend_block(b, block):
        begin = pl.multiple_of(block * length, length)
        total, summed = wide_part(b, 2, begin, length)
        for part_total, part_sum in (wide_part(b, 1, begin, length), close_part(b, block)):
            total, summed = total + part_total, summed + part_sum
        mboth[b, block] = merge(total, summed)

    def m_copy(b):
        return move(mboth.at[b, other], m_send.at[0], m_recv.at[b], sibling, mrecv.at[b])

    def y_copy(b, shift):
        return move(mg.at[mine, b], y_send.at[0], y_recv.at[b], at_y(shift))

    def y_wait(b):
        move(mg.at[pl.ds(0, tp - 1), b], y_send.at[0], y_recv.at[b], at_y(1)).wait_recv()

    def pass_on(b):
        m_copy(b).wait_recv()
        mg[mine, b] = mboth[b, core] + mrecv[b]
        for shift in range(1, tp):
            y_copy(b, shift).start()

    def attend_step(i, carry):
        b = i
        halo_wait(b)
        attend(b)
        m_copy(b).start()

        @pl.when(i >= 1)
        def _():
            pass_on(i - 1)

        return carry

    lax.fori_loop(0, batch - 1, attend_step, 0)
    last = batch - 1
    halo_wait(last)
    attend_block(last, other)
    m_copy(last).start()
    pass_on(last - 1)
    attend_block(last, core)
    pass_on(batch - 1)
    o_all.wait_recv()

    def out_copy(b):
        return pltpu.make_async_copy(outs.at[b], out_ref.at[b], out_move.at[0])

    def finish(b, carry):
        y_wait(b)
        final = jnp.zeros((length, span), jnp.float32)
        for part in range(tp):
            final = final + lax.dot_general(
                mg[part, b], wo[part], (((1,), (1,)), ((), ())), preferred_element_type=jnp.float32
            )
        outs[b] = final.astype(jnp.bfloat16)
        out_copy(b).start()
        return carry

    lax.fori_loop(0, batch, finish, 0)
    pltpu.make_async_copy(outs, out_ref, out_move.at[0]).wait()
    pair_all.wait_send()
    for chunk in range(2):
        sent_all(chunk)
    nb_all.wait_send()
    for group in range(groups):
        both = wins[group].at[:, pl.ds(0, 2 * REACH[group]), :]
        move(both, halo_send.at[group], halo_recv.at[0, group], at_chip(1)).wait_send()
    o_pair.wait_send()
    o_all.wait_send()
    move(mrecv, m_send.at[0], m_recv.at[0], sibling).wait_send()
    move(mg.at[pl.ds(0, tp - 1)], y_send.at[0], y_recv.at[0], at_y(1)).wait_send()


def body(tp, inputs, norm_gain, query_weight, key_weight, value_weight, query_gain, key_gain, out_weight):
    batch, length, model = inputs.shape
    share, groups, heads, width = query_weight.shape
    span = model // tp
    rows = 2 * length
    bf16 = jnp.bfloat16
    dma = pltpu.SemaphoreType.DMA
    operands = (
        inputs,
        norm_gain.reshape(1, model),
        query_weight,
        key_weight,
        value_weight,
        out_weight.transpose(0, 2, 1),
        query_gain,
        key_gain,
    )
    return pl.pallas_call(
        functools.partial(layer_kernel, tp, batch, length),
        out_shape=jax.ShapeDtypeStruct((batch, length, span), bf16),
        in_specs=[pl.BlockSpec(memory_space=pltpu.HBM)] * len(operands),
        out_specs=pl.BlockSpec(memory_space=pl.ANY),
        scratch_shapes=[
            *[pltpu.VMEM(operand.shape, operand.dtype) for operand in operands],
            pltpu.VMEM((heads, share, 384 + WB), bf16),
            pltpu.VMEM((CHIPS, 2, share, 128), bf16),
            pltpu.VMEM((CHIPS, 2, share, 256), bf16),
            pltpu.VMEM((CHIPS, 2, share, WB), bf16),
            pltpu.VMEM((model, 384), bf16),
            pltpu.VMEM((model, WB), bf16),
            pltpu.VMEM((batch, 2, length, model), bf16),
            *[pltpu.VMEM((batch, rows + 2 * r, 128), bf16) for r in REACH],
            pltpu.VMEM((groups, batch, rows, 128), bf16),
            pltpu.VMEM((2, length, length + 2 * REACH[0]), jnp.float32),
            *[pltpu.VMEM((rows, rows + 2 * r), jnp.float32) for r in REACH[1:]],
            pltpu.VMEM((tp, span, 128), bf16),
            pltpu.VMEM((model, 128), bf16),
            pltpu.VMEM((model, 128), bf16),
            pltpu.VMEM((tp, span, 128), bf16),
            pltpu.VMEM((batch, 2, length, 128), bf16),
            pltpu.VMEM((batch, length, 128), bf16),
            pltpu.VMEM((tp, batch, length, 128), bf16),
            dma((len(operands),)),
            dma((1,)),
            dma((1,)),
            dma((1,)),
            dma((3,)),
            dma((3, 8)),
            dma((3,)),
            dma((3, 10)),
            dma((3,)),
            dma((1,)),
            dma((1,)),
            dma((groups,)),
            dma((batch, groups)),
            dma((1,)),
            dma((1,)),
            dma((1,)),
            dma((1,)),
            dma((1,)),
            dma((batch,)),
            dma((1,)),
            dma((batch,)),
            pltpu.VMEM((batch, length, span), bf16),
            dma((1,)),
        ],
        compiler_params=pltpu.CompilerParams(collective_id=0, has_side_effects=True, vmem_limit_bytes=24 * 1024 * 1024),
        name="layer",
    )(*[pltpu.with_memory_space_constraint(operand, pltpu.HBM) for operand in operands])


def solution(mesh):
    in_specs = (
        P(None, "sp", None),
        P(),
        P("sp", None, "tp", None),
        P("sp", None, "tp", None),
        P("sp", None, "tp", None),
        P(),
        P(),
        P("tp", None, "sp"),
    )
    out_specs = P(None, "sp", "tp")
    run = functools.partial(body, mesh.shape["tp"])
    return jax.shard_map(run, mesh=mesh, in_specs=in_specs, out_specs=out_specs, check_vma=False)
```

```python
import functools
import math

import jax
import jax.numpy as jnp
from jax import lax
from jax.experimental import pallas as pl
from jax.experimental.pallas import tpu as pltpu
from jax.sharding import PartitionSpec as P

FOLDED = (2,)
GAPS = ((1, 32), (4, 32), (16, 16))
REACH = tuple(d * h for d, h in GAPS)
EPS = 1e-06
NEG = -1e30
LOG2E = 1.4426950408889634
MESH = pl.DeviceIdType.MESH
NZ, NX = 16, 4
CHIPS = NZ * NX
WB = 256


def layer_kernel(
    tp, batch, length, x_hbm, gain_hbm, qw_hbm, kw_hbm, vw_hbm, ow_hbm, qg_hbm, kg_hbm, out_ref,
    x_ref, gain_ref, qw_ref, kw_ref, vw_ref, ow_ref, qg_ref, kg_ref, slab_ref,
    w2, w01, wb, wk, wq, nb, win0, win1, win2, qn, bias0, bias1, bias2, osum, oown, orecv, wo, mboth, mrecv, mg,
    in_sem, pair_send, pair_recv, local_sem, out_sem, zh_recv, xh_recv, za_recv, xa_recv,
    nb_send, nb_recv, halo_send, halo_recv,
    o_send, o_recv, oy_send, oy_recv, m_send, m_recv, y_send, y_recv, outs, out_move,
):
    me = lax.axis_index("sp")
    mine = lax.axis_index("tp")
    groups = len(GAPS)
    core = me % 2
    other = 1 - core
    chip = me // 2
    x = chip % NX
    z = chip // NX
    rows = 2 * length
    wins = (win0, win1, win2)
    biases = (bias0, bias1, bias2)
    bufs = (w2, w01, wb)

    def at_z(offset, on=core):
        return {"sp": (((z + offset + NZ) % NZ) * NX + x) * 2 + on}

    def at_x(offset, on=core):
        return {"sp": (z * NX + (x + offset) % NX) * 2 + on}

    sibling = {"sp": chip * 2 + other}

    def at_chip(offset):
        return {"sp": ((chip + offset + CHIPS) % CHIPS) * 2 + core}

    def at_y(offset):
        return {"tp": (mine + offset) % tp}

    barrier = pltpu.get_barrier_semaphore()

    def greet(target):
        pl.semaphore_signal(barrier, inc=1, device_id=target, device_id_type=MESH)

    targets = [at_z(o) for o in (-4, 4, -3, 3, -2, 2, -1, 1)] + [at_y(o) for o in range(1, tp)]
    targets += [at_x(o) for o in range(1, NX)] + [at_chip(1), at_chip(-1), sibling]
    targets += [at_x(2, other)]
    targets += [at_z(o, other) for o in (-4, 4, -3, 3, -2, 2, -1, 1)]
    for target in targets:
        greet(target)

    fetches = [
        pltpu.make_async_copy(src, dst, in_sem.at[i])
        for i, (src, dst) in enumerate(
            (
                (qw_hbm, qw_ref),
                (kw_hbm, kw_ref),
                (vw_hbm, vw_ref),
                (ow_hbm, ow_ref),
                (qg_hbm, qg_ref),
                (kg_hbm, kg_ref),
                (gain_hbm, gain_ref),
                (x_hbm, x_ref),
            )
        )
    ]
    for fetch in fetches:
        fetch.start()
    for fetch in fetches[:4]:
        fetch.wait()
    for head in range(2):
        pieces = []
        for group in (2, 0, 1):
            pieces += [kw_ref[:, group, head, :], vw_ref[:, group, head, :]]
        pieces += [qw_ref[:, group, head, :] for group in range(groups)]
        pieces = [piece.astype(jnp.float32) for piece in pieces + [ow_ref[head]]]
        slab_ref[head] = jnp.concatenate(pieces, axis=1).astype(jnp.bfloat16)

    pl.semaphore_wait(barrier, len(targets))

    cuts = (pl.ds(0, 128), pl.ds(128, 256), pl.ds(384, WB))

    def pair(chunk):
        return pltpu.make_async_remote_copy(
            src_ref=slab_ref.at[other, :, cuts[chunk]],
            dst_ref=bufs[chunk].at[chip, core],
            send_sem=pair_send.at[0],
            recv_sem=pair_recv.at[0],
            device_id=sibling,
            device_id_type=MESH,
        )

    def local(chunk):
        return pltpu.make_async_copy(
            slab_ref.at[core, :, cuts[chunk]], bufs[chunk].at[chip, core], local_sem.at[0]
        )

    def index_of(origin, column):
        return ((z + origin + NZ) % NZ) * NX + (x + column) % NX

    def move(block, send_sem, recv_sem, target, land=None):
        return pltpu.make_async_remote_copy(
            src_ref=block,
            dst_ref=block if land is None else land,
            send_sem=send_sem,
            recv_sem=recv_sem,
            device_id=target,
            device_id_type=MESH,
        )

    def zh_start(chunk, step):
        for on in (core, other):
            move(
                slab_ref.at[on, :, cuts[chunk]],
                out_sem.at[chunk],
                zh_recv.at[chunk, 3 - step if step < 0 else step - 1],
                at_z(step, on),
                bufs[chunk].at[chip, core],
            ).start()

    def zh_wait(chunk, origin):
        block = bufs[chunk].at[index_of(origin, 0)]
        slot = 3 + origin if origin > 0 else -origin - 1
        move(block, out_sem.at[chunk], zh_recv.at[chunk, slot], at_z(1)).wait_recv()

    def xh_start(chunk):
        for on in (core, other):
            move(
                slab_ref.at[on, :, cuts[chunk]],
                out_sem.at[chunk],
                xh_recv.at[chunk],
                at_x(2, on),
                bufs[chunk].at[chip, core],
            ).start()

    def xh_wait(chunk):
        move(bufs[chunk].at[index_of(0, 2)], out_sem.at[chunk], xh_recv.at[chunk], at_x(1)).wait_recv()

    def slot_of(rel, fold):
        if fold == 0:
            return rel - 5
        return {4: 7, NZ - 4: 8}.get(rel, 9)

    def za_start(chunk, origin, step, fold=0):
        slot = slot_of((origin - step) % NZ, fold)
        block = bufs[chunk].at[index_of(origin, 2 * fold)]
        move(block, out_sem.at[chunk], za_recv.at[chunk, slot], at_z(step)).start()

    def za_wait(chunk, origin, fold=0):
        block = bufs[chunk].at[index_of(origin, 2 * fold)]
        move(block, out_sem.at[chunk], za_recv.at[chunk, slot_of(origin % NZ, fold)], at_z(1)).wait_recv()

    def shifts(chunk):
        return (1, 3) if chunk in FOLDED else (2, 1, 3)

    def xa_start(chunk, origin):
        block = bufs[chunk].at[index_of(origin, 0)]
        for shift in shifts(chunk):
            move(block, out_sem.at[chunk], xa_recv.at[chunk], at_x(shift)).start()

    far = {4: ((-3, -1, -2), (-4, -3, -1, -2)), -4: ((4, 3, 1, 2), (3, 1, 2))}

    for step in (4, -4, 3, -3, 1, -1, 2, -2):
        zh_start(0, step)
    for steps in ((4, -4), (1, -1, 2, -2, 3, -3)):
        for chunk in (1, 2):
            for step in steps:
                zh_start(chunk, step)
    for chunk in FOLDED:
        xh_start(chunk)
    for chunk in range(3):
        local(chunk).start()
        pair(chunk).start()

    def nb_copy(b):
        return move(nb.at[b, core], nb_send.at[0], nb_recv.at[0], sibling)

    def norm_step(b, carry):
        flat = x_ref[b].astype(jnp.float32)
        scale = lax.rsqrt(jnp.mean(flat * flat, axis=-1, keepdims=True) + EPS)
        nb[b, core] = (flat * scale * gain_ref[...]).astype(jnp.bfloat16)
        nb_copy(b).start()
        return carry

    for fetch in fetches[4:]:
        fetch.wait()
    lax.fori_loop(0, batch, norm_step, 0)

    pair_all = move(slab_ref.at[0], pair_send.at[0], pair_recv.at[0], sibling)
    pltpu.make_async_copy(slab_ref.at[0], slab_ref.at[1], local_sem.at[0]).wait()
    pair_all.wait_recv()
    for chunk in range(3):
        xa_start(chunk, 0)

    def near(chunk, spread):
        for origin in (1, -1, 2, -2):
            zh_wait(chunk, origin)
            if spread:
                xa_start(chunk, origin)
        for origin in (4, -4):
            zh_wait(chunk, origin)
            for step in far[origin][chunk % 2]:
                za_start(chunk, origin, step)
        for origin in (3, -3):
            zh_wait(chunk, origin)
            if spread:
                xa_start(chunk, origin)
        if spread:
            for origin in (4, -4):
                xa_start(chunk, origin)

    near(0, True)
    for chunk in FOLDED:
        xh_wait(chunk)
        for step in (4, -4, 3, -3, 1, -1, 2, -2):
            za_start(chunk, 0, step, 1)
    near(1, True)
    near(2, True)

    head = mine * 2 + core
    heads = 2 * tp
    power = -8.0 * (head + 1).astype(jnp.float32) / heads
    slope = jnp.exp2(jnp.full((8, 128), power, jnp.float32))[:1, :1] * LOG2E
    total_rows = CHIPS * rows

    def bias_of(group, count, first):
        dilation, half = GAPS[group]
        reach = REACH[group]
        shape = (count, count + 2 * reach)
        key = lax.broadcasted_iota(jnp.int32, shape, 1) - reach
        offset = jnp.abs(key - lax.broadcasted_iota(jnp.int32, shape, 0))
        at = key + (chip * rows + first)
        allowed = (offset <= reach) & (at >= 0) & (at < total_rows) & ((offset & (dilation - 1)) == 0)
        return jnp.where(allowed, offset.astype(jnp.float32) * (-slope / float(reach)), NEG)

    for block in range(2):
        bias0[block] = bias_of(0, length, block * length)
    for group in (1, 2):
        biases[group][...] = bias_of(group, rows, 0)

    late = (5, -5, 6, -6, 7, -7, 8)
    def fold_on(chunk):
        for origin in (4, -4):
            za_wait(chunk, origin, 1)
            for step in far[origin][1 - chunk % 2]:
                za_start(chunk, origin, step, 1)

    def late_on(chunk, part):
        for origin in part:
            za_wait(chunk, origin)
            xa_start(chunk, origin)

    late_on(0, late[:4])
    for chunk in FOLDED:
        fold_on(chunk)
    late_on(0, late[4:])
    late_on(1, late)
    late_on(2, late)

    lane = lax.broadcasted_iota(jnp.int32, (rows, 128), 1)
    low = lane < 64
    origins = (0, 1, -1, 2, -2, 3, -3, 4, -4) + late

    def all_blocks(chunk):
        several = bufs[chunk].at[pl.ds(0, NZ * len(shifts(chunk)))]
        move(several, out_sem.at[chunk], xa_recv.at[chunk], at_x(1)).wait_recv()
        if chunk in FOLDED:
            several = bufs[chunk].at[pl.ds(0, NZ - 3)]
            move(several, out_sem.at[chunk], za_recv.at[chunk, 9], at_x(1)).wait_recv()

    def sent_all(chunk):
        move(bufs[chunk].at[pl.ds(0, CHIPS - 1)], out_sem.at[chunk], xa_recv.at[chunk], at_x(1)).wait_send()

    all_blocks(0)
    wk[:, :128] = w2[...].reshape(wk.shape[0], 128)
    nb_all = move(nb.at[:, 0], nb_send.at[0], nb_recv.at[0], sibling)
    nb_all.wait_recv()

    def halo(b, group, up):
        reach = REACH[group]
        begin_at, land_at = (rows, 0) if up else (reach, reach + rows)
        return pltpu.make_async_remote_copy(
            src_ref=wins[group].at[b, pl.ds(begin_at, reach), :],
            dst_ref=wins[group].at[b, pl.ds(land_at, reach), :],
            send_sem=halo_send.at[group],
            recv_sem=halo_recv.at[b, group],
            device_id=at_chip(1 if up else -1),
            device_id_type=MESH,
        )

    def halo_wait(b):
        for group in (2, 1, 0):
            both = wins[group].at[b, pl.ds(0, 2 * REACH[group]), :]
            move(both, halo_send.at[group], halo_recv.at[b, group], at_chip(1)).wait_recv()

    ones = jnp.ones((1, 64), jnp.float32)
    zeros = jnp.zeros((1, 64), jnp.float32)

    def key_norm(out, place, group):
        seg = out[:, 128 * place : 128 * (place + 1)].astype(jnp.bfloat16).astype(jnp.float32)
        mean = jnp.sum(jnp.where(low, seg * seg, 0.0), axis=-1, keepdims=True) / 64.0
        gain = jnp.concatenate([kg_ref[group : group + 1, :], ones], axis=1)
        return (seg * jnp.where(low, lax.rsqrt(mean + EPS), 1.0) * gain).astype(jnp.bfloat16)

    def key_step(b, first, order):
        out = jnp.dot(nb[b].reshape(rows, -1), wk[:, first : first + 128 * len(order)], preferred_element_type=jnp.float32)
        for place, group in enumerate(order):
            wins[group][b, REACH[group] : REACH[group] + rows, :] = key_norm(out, place, group)
        for group in order:
            for up in (True, False):
                if group != 2:
                    halo(b, group, up).start()
                elif b < 2:

                    @pl.when(x != (NX - 1 if up else 0))
                    def _(up=up):
                        halo(b, 2, up).start()

    for b in range(batch):
        key_step(b, 0, (2,))
    all_blocks(1)
    sent_all(2)

    for up in (True, False):

        @pl.when(x == (NX - 1 if up else 0))
        def _(up=up):
            for b in range(2):
                halo(b, 2, up).start()

    wk[:, 128:] = w01[...].reshape(wk.shape[0], 256)
    for b in range(batch):
        key_step(b, 128, (0, 1))
        if 1 <= b < batch - 1:
            for up in (True, False):
                halo(b + 1, 2, up).start()

    all_blocks(2)
    wq[...] = wb[...].reshape(wq.shape)

    tile = wq[:, 128:].astype(jnp.float32)
    high = lax.broadcasted_iota(jnp.int32, tile.shape, 1) >= 64
    tile = jnp.where(high, tile, 0.0)
    tile = jnp.where(core == 0, pltpu.roll(tile, 64, 1), tile)
    oown[...] = tile.astype(jnp.bfloat16)
    o_pair = pltpu.make_async_remote_copy(
        src_ref=oown,
        dst_ref=orecv,
        send_sem=o_send.at[0],
        recv_sem=o_recv.at[0],
        device_id=sibling,
        device_id_type=MESH,
    )
    o_pair.start()

    factor = LOG2E / 8.0

    def q_step(b, carry):
        out = jnp.dot(nb[b].reshape(rows, -1), wq[...], preferred_element_type=jnp.float32)
        out = out.astype(jnp.bfloat16).astype(jnp.float32)
        first, second = out[:, :128], out[:, 128:]
        for group, seg, here in ((0, first, low), (1, first, ~low), (2, second, low)):
            mean = jnp.sum(jnp.where(here, seg * seg, 0.0), axis=-1, keepdims=True) / 64.0
            gain = qg_ref[group : group + 1, :] * factor
            gain = jnp.concatenate([zeros, gain] if group == 1 else [gain, zeros], axis=1)
            scaled = jnp.where(here, seg * lax.rsqrt(mean + EPS) * gain, 0.0)
            if group == 1:
                scaled = pltpu.roll(scaled, 64, 1)
            qn[group, b] = scaled.astype(jnp.bfloat16)
        return carry

    for i in range(batch):
        q_step(i, 0)

    span = wo.shape[1]
    o_pair.wait_recv()
    osum[...] = (oown[...] + orecv[...]).reshape(osum.shape)
    wo[mine] = osum[mine]

    def o_copy(shift):
        return move(osum.at[(mine + shift) % tp], oy_send.at[0], oy_recv.at[0], at_y(shift), wo.at[mine])

    o_all = move(wo.at[pl.ds(0, tp - 1)], oy_send.at[0], oy_recv.at[0], at_y(1))

    for shift in range(1, tp):
        o_copy(shift).start()

    def merge(total, summed):
        merged = jnp.where(lax.broadcasted_iota(jnp.int32, summed.shape, 1) >= 64, summed / total, 0.0)
        return jnp.where(core == 0, pltpu.roll(merged, 64, 1), merged).astype(jnp.bfloat16)

    def close_part(b, block):
        begin = block * length if isinstance(block, int) else pl.multiple_of(block * length, length)
        window = win0[b, pl.ds(begin, length + 2 * REACH[0]), :]
        query = qn[0, b, pl.ds(begin, length), :]
        scores = lax.dot_general(query, window, (((1,), (1,)), ((), ())), preferred_element_type=jnp.float32)
        grown = jnp.exp2(scores + bias0[block])
        total = jnp.sum(grown, axis=-1, keepdims=True)
        return total, jnp.dot(grown.astype(jnp.bfloat16), window, preferred_element_type=jnp.float32)

    def wide_part(b, group, begin, count):
        window = wins[group][b, pl.ds(begin, count + 2 * REACH[group]), :]
        query = qn[group, b, pl.ds(begin, count), :]
        scores = lax.dot_general(query, window, (((1,), (1,)), ((), ())), preferred_element_type=jnp.float32)
        first = begin if isinstance(begin, int) else pl.multiple_of(begin, length)
        bias = biases[group][pl.ds(0, count), pl.ds(0, count + 2 * REACH[group])]
        if count != rows:
            bias = biases[group][pl.ds(first, count), pl.ds(first, count + 2 * REACH[group])]
        grown = jnp.exp2(scores + bias)
        total = jnp.sum(grown, axis=-1, keepdims=True)
        return total, jnp.dot(grown.astype(jnp.bfloat16), window, preferred_element_type=jnp.float32)

    def attend(b):
        total, summed = wide_part(b, 2, 0, rows)
        for part_total, part_sum in [
            wide_part(b, 1, 0, rows),
            [jnp.concatenate(both, axis=0) for both in zip(close_part(b, 0), close_part(b, 1))],
        ]:
            total, summed = total + part_total, summed + part_sum
        mboth[b] = merge(total, summed).reshape(2, length, 128)

    def attend_block(b, block):
        begin = pl.multiple_of(block * length, length)
        total, summed = wide_part(b, 2, begin, length)
        for part_total, part_sum in (wide_part(b, 1, begin, length), close_part(b, block)):
            total, summed = total + part_total, summed + part_sum
        mboth[b, block] = merge(total, summed)

    def m_copy(b):
        return move(mboth.at[b, other], m_send.at[0], m_recv.at[b], sibling, mrecv.at[b])

    def y_copy(b, shift):
        return move(mg.at[mine, b], y_send.at[0], y_recv.at[b], at_y(shift))

    def y_wait(b):
        move(mg.at[pl.ds(0, tp - 1), b], y_send.at[0], y_recv.at[b], at_y(1)).wait_recv()

    def pass_on(b):
        m_copy(b).wait_recv()
        mg[mine, b] = mboth[b, core] + mrecv[b]
        for shift in (2, 1, 3):
            y_copy(b, shift).start()

    def attend_step(i, carry):
        b = i
        halo_wait(b)
        attend(b)
        m_copy(b).start()

        @pl.when(i >= 1)
        def _():
            pass_on(i - 1)

        return carry

    lax.fori_loop(0, batch - 1, attend_step, 0)
    last = batch - 1
    halo_wait(last)
    attend_block(last, other)
    m_copy(last).start()
    pass_on(last - 1)
    attend_block(last, core)
    pass_on(batch - 1)
    o_all.wait_recv()

    def out_copy(b):
        return pltpu.make_async_copy(outs.at[b], out_ref.at[b], out_move.at[0])

    def finish(b, carry):
        y_wait(b)
        final = jnp.zeros((length, span), jnp.float32)
        for part in range(tp):
            final = final + lax.dot_general(
                mg[part, b], wo[part], (((1,), (1,)), ((), ())), preferred_element_type=jnp.float32
            )
        outs[b] = final.astype(jnp.bfloat16)
        out_copy(b).start()
        return carry

    lax.fori_loop(0, batch, finish, 0)
    pltpu.make_async_copy(outs, out_ref, out_move.at[0]).wait()
    pair_all.wait_send()
    for chunk in range(2):
        sent_all(chunk)
    nb_all.wait_send()
    for group in range(groups):
        both = wins[group].at[:, pl.ds(0, 2 * REACH[group]), :]
        move(both, halo_send.at[group], halo_recv.at[0, group], at_chip(1)).wait_send()
    o_pair.wait_send()
    o_all.wait_send()
    move(mrecv, m_send.at[0], m_recv.at[0], sibling).wait_send()
    move(mg.at[pl.ds(0, tp - 1)], y_send.at[0], y_recv.at[0], at_y(1)).wait_send()


def body(tp, inputs, norm_gain, query_weight, key_weight, value_weight, query_gain, key_gain, out_weight):
    batch, length, model = inputs.shape
    share, groups, heads, width = query_weight.shape
    span = model // tp
    rows = 2 * length
    bf16 = jnp.bfloat16
    dma = pltpu.SemaphoreType.DMA
    operands = (
        inputs,
        norm_gain.reshape(1, model),
        query_weight,
        key_weight,
        value_weight,
        out_weight.transpose(0, 2, 1),
        query_gain,
        key_gain,
    )
    return pl.pallas_call(
        functools.partial(layer_kernel, tp, batch, length),
        out_shape=jax.ShapeDtypeStruct((batch, length, span), bf16),
        in_specs=[pl.BlockSpec(memory_space=pltpu.HBM)] * len(operands),
        out_specs=pl.BlockSpec(memory_space=pl.ANY),
        scratch_shapes=[
            *[pltpu.VMEM(operand.shape, operand.dtype) for operand in operands],
            pltpu.VMEM((heads, share, 384 + WB), bf16),
            pltpu.VMEM((CHIPS, 2, share, 128), bf16),
            pltpu.VMEM((CHIPS, 2, share, 256), bf16),
            pltpu.VMEM((CHIPS, 2, share, WB), bf16),
            pltpu.VMEM((model, 384), bf16),
            pltpu.VMEM((model, WB), bf16),
            pltpu.VMEM((batch, 2, length, model), bf16),
            *[pltpu.VMEM((batch, rows + 2 * r, 128), bf16) for r in REACH],
            pltpu.VMEM((groups, batch, rows, 128), bf16),
            pltpu.VMEM((2, length, length + 2 * REACH[0]), jnp.float32),
            *[pltpu.VMEM((rows, rows + 2 * r), jnp.float32) for r in REACH[1:]],
            pltpu.VMEM((tp, span, 128), bf16),
            pltpu.VMEM((model, 128), bf16),
            pltpu.VMEM((model, 128), bf16),
            pltpu.VMEM((tp, span, 128), bf16),
            pltpu.VMEM((batch, 2, length, 128), bf16),
            pltpu.VMEM((batch, length, 128), bf16),
            pltpu.VMEM((tp, batch, length, 128), bf16),
            dma((len(operands),)),
            dma((1,)),
            dma((1,)),
            dma((1,)),
            dma((3,)),
            dma((3, 8)),
            dma((3,)),
            dma((3, 10)),
            dma((3,)),
            dma((1,)),
            dma((1,)),
            dma((groups,)),
            dma((batch, groups)),
            dma((1,)),
            dma((1,)),
            dma((1,)),
            dma((1,)),
            dma((1,)),
            dma((batch,)),
            dma((1,)),
            dma((batch,)),
            pltpu.VMEM((batch, length, span), bf16),
            dma((1,)),
        ],
        compiler_params=pltpu.CompilerParams(collective_id=0, has_side_effects=True, vmem_limit_bytes=24 * 1024 * 1024),
        name="layer",
    )(*[pltpu.with_memory_space_constraint(operand, pltpu.HBM) for operand in operands])


def solution(mesh):
    in_specs = (
        P(None, "sp", None),
        P(),
        P("sp", None, "tp", None),
        P("sp", None, "tp", None),
        P("sp", None, "tp", None),
        P(),
        P(),
        P("tp", None, "sp"),
    )
    out_specs = P(None, "sp", "tp")
    run = functools.partial(body, mesh.shape["tp"])
    return jax.shard_map(run, mesh=mesh, in_specs=in_specs, out_specs=out_specs, check_vma=False)
```

```python
import functools
import math

import jax
import jax.numpy as jnp
from jax import lax
from jax.experimental import pallas as pl
from jax.experimental.pallas import tpu as pltpu
from jax.sharding import PartitionSpec as P

FOLDED = (2,)
GAPS = ((1, 32), (4, 32), (16, 16))
REACH = tuple(d * h for d, h in GAPS)
EPS = 1e-06
NEG = -1e30
LOG2E = 1.4426950408889634
MESH = pl.DeviceIdType.MESH
NZ, NX = 16, 4
CHIPS = NZ * NX
WB = 256


def layer_kernel(
    tp, batch, length, x_hbm, gain_hbm, qw_hbm, kw_hbm, vw_hbm, ow_hbm, qg_hbm, kg_hbm, out_ref,
    x_ref, gain_ref, qw_ref, kw_ref, vw_ref, ow_ref, qg_ref, kg_ref, slab_ref,
    w2, w01, wb, wk, wq, nb, win0, win1, win2, qn, bias0, bias1, bias2, osum, oown, orecv, wo, mboth, mrecv, mg,
    in_sem, pair_send, pair_recv, local_sem, out_sem, zh_recv, xh_recv, za_recv, xa_recv,
    nb_send, nb_recv, halo_send, halo_recv,
    o_send, o_recv, oy_send, oy_recv, m_send, m_recv, y_send, y_recv, outs, out_move,
):
    me = lax.axis_index("sp")
    mine = lax.axis_index("tp")
    groups = len(GAPS)
    core = me % 2
    other = 1 - core
    chip = me // 2
    x = chip % NX
    z = chip // NX
    rows = 2 * length
    wins = (win0, win1, win2)
    biases = (bias0, bias1, bias2)
    bufs = (w2, w01, wb)

    def at_z(offset, on=core):
        return {"sp": (((z + offset + NZ) % NZ) * NX + x) * 2 + on}

    def at_x(offset, on=core):
        return {"sp": (z * NX + (x + offset) % NX) * 2 + on}

    sibling = {"sp": chip * 2 + other}

    def at_chip(offset):
        return {"sp": ((chip + offset + CHIPS) % CHIPS) * 2 + core}

    def at_y(offset):
        return {"tp": (mine + offset) % tp}

    barrier = pltpu.get_barrier_semaphore()

    def greet(target):
        pl.semaphore_signal(barrier, inc=1, device_id=target, device_id_type=MESH)

    targets = [at_z(o) for o in (-4, 4, -3, 3, -2, 2, -1, 1)] + [at_y(o) for o in range(1, tp)]
    targets += [at_x(o) for o in range(1, NX)] + [at_chip(1), at_chip(-1), sibling]
    targets += [at_x(2, other)]
    targets += [at_z(o, other) for o in (-4, 4, -3, 3, -2, 2, -1, 1)]
    for target in targets:
        greet(target)

    fetches = [
        pltpu.make_async_copy(src, dst, in_sem.at[i])
        for i, (src, dst) in enumerate(
            (
                (qw_hbm, qw_ref),
                (kw_hbm, kw_ref),
                (vw_hbm, vw_ref),
                (ow_hbm, ow_ref),
                (qg_hbm, qg_ref),
                (kg_hbm, kg_ref),
                (gain_hbm, gain_ref),
                (x_hbm, x_ref),
            )
        )
    ]
    for fetch in fetches:
        fetch.start()
    for fetch in fetches[:4]:
        fetch.wait()
    for head in range(2):
        pieces = []
        for group in (2, 0, 1):
            pieces += [kw_ref[:, group, head, :], vw_ref[:, group, head, :]]
        pieces += [qw_ref[:, group, head, :] for group in range(groups)]
        pieces = [piece.astype(jnp.float32) for piece in pieces + [ow_ref[head]]]
        slab_ref[head] = jnp.concatenate(pieces, axis=1).astype(jnp.bfloat16)

    pl.semaphore_wait(barrier, len(targets))

    cuts = (pl.ds(0, 128), pl.ds(128, 256), pl.ds(384, WB))

    def pair(chunk):
        return pltpu.make_async_remote_copy(
            src_ref=slab_ref.at[other, :, cuts[chunk]],
            dst_ref=bufs[chunk].at[chip, core],
            send_sem=pair_send.at[0],
            recv_sem=pair_recv.at[0],
            device_id=sibling,
            device_id_type=MESH,
        )

    def local(chunk):
        return pltpu.make_async_copy(
            slab_ref.at[core, :, cuts[chunk]], bufs[chunk].at[chip, core], local_sem.at[0]
        )

    def index_of(origin, column):
        return ((z + origin + NZ) % NZ) * NX + (x + column) % NX

    def move(block, send_sem, recv_sem, target, land=None):
        return pltpu.make_async_remote_copy(
            src_ref=block,
            dst_ref=block if land is None else land,
            send_sem=send_sem,
            recv_sem=recv_sem,
            device_id=target,
            device_id_type=MESH,
        )

    def zh_start(chunk, step):
        for on in (core, other):
            move(
                slab_ref.at[on, :, cuts[chunk]],
                out_sem.at[chunk],
                zh_recv.at[chunk, 3 - step if step < 0 else step - 1],
                at_z(step, on),
                bufs[chunk].at[chip, core],
            ).start()

    def zh_wait(chunk, origin):
        block = bufs[chunk].at[index_of(origin, 0)]
        slot = 3 + origin if origin > 0 else -origin - 1
        move(block, out_sem.at[chunk], zh_recv.at[chunk, slot], at_z(1)).wait_recv()

    def xh_start(chunk):
        for on in (core, other):
            move(
                slab_ref.at[on, :, cuts[chunk]],
                out_sem.at[chunk],
                xh_recv.at[chunk],
                at_x(2, on),
                bufs[chunk].at[chip, core],
            ).start()

    def xh_wait(chunk):
        move(bufs[chunk].at[index_of(0, 2)], out_sem.at[chunk], xh_recv.at[chunk], at_x(1)).wait_recv()

    def slot_of(rel, fold):
        if fold == 0:
            return rel - 5
        return {4: 7, NZ - 4: 8}.get(rel, 9)

    def za_start(chunk, origin, step, fold=0):
        slot = slot_of((origin - step) % NZ, fold)
        block = bufs[chunk].at[index_of(origin, 2 * fold)]
        move(block, out_sem.at[chunk], za_recv.at[chunk, slot], at_z(step)).start()

    def za_wait(chunk, origin, fold=0):
        block = bufs[chunk].at[index_of(origin, 2 * fold)]
        move(block, out_sem.at[chunk], za_recv.at[chunk, slot_of(origin % NZ, fold)], at_z(1)).wait_recv()

    def shifts(chunk):
        return (1, 3) if chunk in FOLDED else (2, 1, 3)

    def xa_start(chunk, origin):
        block = bufs[chunk].at[index_of(origin, 0)]
        for shift in shifts(chunk):
            move(block, out_sem.at[chunk], xa_recv.at[chunk], at_x(shift)).start()

    far = {4: ((-3, -1, -2), (-4, -3, -1, -2)), -4: ((4, 3, 1, 2), (3, 1, 2))}

    for step in (4, -4, 3, -3, 1, -1, 2, -2):
        zh_start(0, step)
    for steps in ((4, -4), (1, -1, 2, -2, 3, -3)):
        for chunk in (1, 2):
            for step in steps:
                zh_start(chunk, step)
    for chunk in FOLDED:
        xh_start(chunk)
    for chunk in range(3):
        local(chunk).start()
        pair(chunk).start()

    def nb_copy(b):
        return move(nb.at[b, core], nb_send.at[0], nb_recv.at[0], sibling)

    def norm_step(b, carry):
        flat = x_ref[b].astype(jnp.float32)
        scale = lax.rsqrt(jnp.mean(flat * flat, axis=-1, keepdims=True) + EPS)
        nb[b, core] = (flat * scale * gain_ref[...]).astype(jnp.bfloat16)
        nb_copy(b).start()
        return carry

    for fetch in fetches[4:]:
        fetch.wait()
    lax.fori_loop(0, batch, norm_step, 0)

    pair_all = move(slab_ref.at[0], pair_send.at[0], pair_recv.at[0], sibling)
    pltpu.make_async_copy(slab_ref.at[0], slab_ref.at[1], local_sem.at[0]).wait()
    pair_all.wait_recv()
    for chunk in range(3):
        xa_start(chunk, 0)

    def near(chunk, spread):
        for origin in (1, -1, 2, -2):
            zh_wait(chunk, origin)
            if spread:
                xa_start(chunk, origin)
        for origin in (4, -4):
            zh_wait(chunk, origin)
            for step in far[origin][chunk % 2]:
                za_start(chunk, origin, step)
        for origin in (3, -3):
            zh_wait(chunk, origin)
            if spread:
                xa_start(chunk, origin)
        if spread:
            for origin in (4, -4):
                xa_start(chunk, origin)

    near(0, True)
    for chunk in FOLDED:
        xh_wait(chunk)
        for step in (4, -4, 3, -3, 1, -1, 2, -2):
            za_start(chunk, 0, step, 1)
    near(1, True)
    near(2, True)

    head = mine * 2 + core
    heads = 2 * tp
    power = -8.0 * (head + 1).astype(jnp.float32) / heads
    slope = jnp.exp2(jnp.full((8, 128), power, jnp.float32))[:1, :1] * LOG2E
    total_rows = CHIPS * rows

    def bias_of(group, count, first):
        dilation, half = GAPS[group]
        reach = REACH[group]
        shape = (count, count + 2 * reach)
        key = lax.broadcasted_iota(jnp.int32, shape, 1) - reach
        offset = jnp.abs(key - lax.broadcasted_iota(jnp.int32, shape, 0))
        at = key + (chip * rows + first)
        allowed = (offset <= reach) & (at >= 0) & (at < total_rows) & ((offset & (dilation - 1)) == 0)
        return jnp.where(allowed, offset.astype(jnp.float32) * (-slope / float(reach)), NEG)

    for block in range(2):
        bias0[block] = bias_of(0, length, block * length)
    for group in (1, 2):
        biases[group][...] = bias_of(group, rows, 0)

    late = (5, -5, 6, -6, 7, -7, 8)
    def fold_on(chunk):
        for origin in (4, -4):
            za_wait(chunk, origin, 1)
            for step in far[origin][1 - chunk % 2]:
                za_start(chunk, origin, step, 1)

    def late_on(chunk, part):
        for origin in part:
            za_wait(chunk, origin)
            xa_start(chunk, origin)

    late_on(0, late[:4])
    for chunk in FOLDED:
        fold_on(chunk)
    late_on(0, late[4:])
    late_on(1, late)
    late_on(2, late)

    lane = lax.broadcasted_iota(jnp.int32, (rows, 128), 1)
    low = lane < 64
    origins = (0, 1, -1, 2, -2, 3, -3, 4, -4) + late

    def all_blocks(chunk):
        several = bufs[chunk].at[pl.ds(0, NZ * len(shifts(chunk)))]
        move(several, out_sem.at[chunk], xa_recv.at[chunk], at_x(1)).wait_recv()
        if chunk in FOLDED:
            several = bufs[chunk].at[pl.ds(0, NZ - 3)]
            move(several, out_sem.at[chunk], za_recv.at[chunk, 9], at_x(1)).wait_recv()

    def sent_all(chunk):
        move(bufs[chunk].at[pl.ds(0, CHIPS - 1)], out_sem.at[chunk], xa_recv.at[chunk], at_x(1)).wait_send()

    all_blocks(0)
    wk[:, :128] = w2[...].reshape(wk.shape[0], 128)
    nb_all = move(nb.at[:, 0], nb_send.at[0], nb_recv.at[0], sibling)
    nb_all.wait_recv()

    def halo(b, group, up):
        reach = REACH[group]
        begin_at, land_at = (rows, 0) if up else (reach, reach + rows)
        return pltpu.make_async_remote_copy(
            src_ref=wins[group].at[b, pl.ds(begin_at, reach), :],
            dst_ref=wins[group].at[b, pl.ds(land_at, reach), :],
            send_sem=halo_send.at[group],
            recv_sem=halo_recv.at[b, group],
            device_id=at_chip(1 if up else -1),
            device_id_type=MESH,
        )

    def halo_wait(b, only=(2, 1, 0)):
        for group in only:
            both = wins[group].at[b, pl.ds(0, 2 * REACH[group]), :]
            move(both, halo_send.at[group], halo_recv.at[b, group], at_chip(1)).wait_recv()

    ones = jnp.ones((1, 64), jnp.float32)
    zeros = jnp.zeros((1, 64), jnp.float32)

    def key_norm(out, place, group):
        seg = out[:, 128 * place : 128 * (place + 1)].astype(jnp.bfloat16).astype(jnp.float32)
        mean = jnp.sum(jnp.where(low, seg * seg, 0.0), axis=-1, keepdims=True) / 64.0
        gain = jnp.concatenate([kg_ref[group : group + 1, :], ones], axis=1)
        return (seg * jnp.where(low, lax.rsqrt(mean + EPS), 1.0) * gain).astype(jnp.bfloat16)

    def key_step(b, first, order):
        out = jnp.dot(nb[b].reshape(rows, -1), wk[:, first : first + 128 * len(order)], preferred_element_type=jnp.float32)
        for place, group in enumerate(order):
            wins[group][b, REACH[group] : REACH[group] + rows, :] = key_norm(out, place, group)
        for group in order:
            for up in (True, False):
                if group != 2:
                    halo(b, group, up).start()
                elif b < 2:

                    @pl.when(x != (NX - 1 if up else 0))
                    def _(up=up):
                        halo(b, 2, up).start()

    for b in range(batch):
        key_step(b, 0, (2,))
    sent_all(2)

    for up in (True, False):

        @pl.when(x == (NX - 1 if up else 0))
        def _(up=up):
            for b in range(2):
                halo(b, 2, up).start()

    all_blocks(1)
    wk[:, 128:] = w01[...].reshape(wk.shape[0], 256)
    for b in range(batch):
        key_step(b, 128, (0, 1))
        if 1 <= b < batch - 1:
            for up in (True, False):
                halo(b + 1, 2, up).start()

    all_blocks(2)
    wq[...] = wb[...].reshape(wq.shape)

    tile = wq[:, 128:].astype(jnp.float32)
    high = lax.broadcasted_iota(jnp.int32, tile.shape, 1) >= 64
    tile = jnp.where(high, tile, 0.0)
    tile = jnp.where(core == 0, pltpu.roll(tile, 64, 1), tile)
    oown[...] = tile.astype(jnp.bfloat16)
    o_pair = pltpu.make_async_remote_copy(
        src_ref=oown,
        dst_ref=orecv,
        send_sem=o_send.at[0],
        recv_sem=o_recv.at[0],
        device_id=sibling,
        device_id_type=MESH,
    )
    o_pair.start()

    factor = LOG2E / 8.0

    def q_step(b, carry):
        out = jnp.dot(nb[b].reshape(rows, -1), wq[...], preferred_element_type=jnp.float32)
        out = out.astype(jnp.bfloat16).astype(jnp.float32)
        first, second = out[:, :128], out[:, 128:]
        for group, seg, here in ((0, first, low), (1, first, ~low), (2, second, low)):
            mean = jnp.sum(jnp.where(here, seg * seg, 0.0), axis=-1, keepdims=True) / 64.0
            gain = qg_ref[group : group + 1, :] * factor
            gain = jnp.concatenate([zeros, gain] if group == 1 else [gain, zeros], axis=1)
            scaled = jnp.where(here, seg * lax.rsqrt(mean + EPS) * gain, 0.0)
            if group == 1:
                scaled = pltpu.roll(scaled, 64, 1)
            qn[group, b] = scaled.astype(jnp.bfloat16)
        return carry

    for i in range(batch):
        q_step(i, 0)

    span = wo.shape[1]
    o_pair.wait_recv()
    osum[...] = (oown[...] + orecv[...]).reshape(osum.shape)
    wo[mine] = osum[mine]

    def o_copy(shift):
        return move(osum.at[(mine + shift) % tp], oy_send.at[0], oy_recv.at[0], at_y(shift), wo.at[mine])

    o_all = move(wo.at[pl.ds(0, tp - 1)], oy_send.at[0], oy_recv.at[0], at_y(1))

    for shift in range(1, tp):
        o_copy(shift).start()

    def merge(total, summed):
        merged = jnp.where(lax.broadcasted_iota(jnp.int32, summed.shape, 1) >= 64, summed / total, 0.0)
        return jnp.where(core == 0, pltpu.roll(merged, 64, 1), merged).astype(jnp.bfloat16)

    def close_part(b, block):
        begin = block * length if isinstance(block, int) else pl.multiple_of(block * length, length)
        window = win0[b, pl.ds(begin, length + 2 * REACH[0]), :]
        query = qn[0, b, pl.ds(begin, length), :]
        scores = lax.dot_general(query, window, (((1,), (1,)), ((), ())), preferred_element_type=jnp.float32)
        grown = jnp.exp2(scores + bias0[block])
        total = jnp.sum(grown, axis=-1, keepdims=True)
        return total, jnp.dot(grown.astype(jnp.bfloat16), window, preferred_element_type=jnp.float32)

    def wide_part(b, group, begin, count):
        window = wins[group][b, pl.ds(begin, count + 2 * REACH[group]), :]
        query = qn[group, b, pl.ds(begin, count), :]
        scores = lax.dot_general(query, window, (((1,), (1,)), ((), ())), preferred_element_type=jnp.float32)
        first = begin if isinstance(begin, int) else pl.multiple_of(begin, length)
        bias = biases[group][pl.ds(0, count), pl.ds(0, count + 2 * REACH[group])]
        if count != rows:
            bias = biases[group][pl.ds(first, count), pl.ds(first, count + 2 * REACH[group])]
        grown = jnp.exp2(scores + bias)
        total = jnp.sum(grown, axis=-1, keepdims=True)
        return total, jnp.dot(grown.astype(jnp.bfloat16), window, preferred_element_type=jnp.float32)

    def attend(b):
        total, summed = wide_part(b, 2, 0, rows)
        for part_total, part_sum in [
            wide_part(b, 1, 0, rows),
            [jnp.concatenate(both, axis=0) for both in zip(close_part(b, 0), close_part(b, 1))],
        ]:
            total, summed = total + part_total, summed + part_sum
        mboth[b] = merge(total, summed).reshape(2, length, 128)

    def attend_block(b, block, total, summed):
        begin = pl.multiple_of(block * length, length)
        for part_total, part_sum in (wide_part(b, 1, begin, length), close_part(b, block)):
            total, summed = total + part_total, summed + part_sum
        mboth[b, block] = merge(total, summed)

    def m_copy(b):
        return move(mboth.at[b, other], m_send.at[0], m_recv.at[b], sibling, mrecv.at[b])

    def y_copy(b, shift):
        return move(mg.at[mine, b], y_send.at[0], y_recv.at[b], at_y(shift))

    def y_wait(b):
        move(mg.at[pl.ds(0, tp - 1), b], y_send.at[0], y_recv.at[b], at_y(1)).wait_recv()

    def pass_on(b):
        m_copy(b).wait_recv()
        mg[mine, b] = mboth[b, core] + mrecv[b]
        for shift in (2, 1, 3):
            y_copy(b, shift).start()

    def attend_step(i, carry):
        b = i
        halo_wait(b)
        attend(b)
        m_copy(b).start()

        @pl.when(i >= 1)
        def _():
            pass_on(i - 1)

        return carry

    lax.fori_loop(0, batch - 1, attend_step, 0)
    last = batch - 1
    halo_wait(last, (2,))
    far_parts = [wide_part(last, 2, pl.multiple_of(block * length, length), length) for block in (other, core)]
    pass_on(last - 1)
    halo_wait(last, (1, 0))
    attend_block(last, other, *far_parts[0])
    m_copy(last).start()
    attend_block(last, core, *far_parts[1])
    pass_on(batch - 1)
    o_all.wait_recv()

    def out_copy(b):
        return pltpu.make_async_copy(outs.at[b], out_ref.at[b], out_move.at[0])

    def finish(b, carry):
        y_wait(b)
        final = jnp.zeros((length, span), jnp.float32)
        for part in range(tp):
            final = final + lax.dot_general(
                mg[part, b], wo[part], (((1,), (1,)), ((), ())), preferred_element_type=jnp.float32
            )
        outs[b] = final.astype(jnp.bfloat16)
        out_copy(b).start()
        return carry

    lax.fori_loop(0, batch, finish, 0)
    pltpu.make_async_copy(outs, out_ref, out_move.at[0]).wait()
    pair_all.wait_send()
    for chunk in range(2):
        sent_all(chunk)
    nb_all.wait_send()
    for group in range(groups):
        both = wins[group].at[:, pl.ds(0, 2 * REACH[group]), :]
        move(both, halo_send.at[group], halo_recv.at[0, group], at_chip(1)).wait_send()
    o_pair.wait_send()
    o_all.wait_send()
    move(mrecv, m_send.at[0], m_recv.at[0], sibling).wait_send()
    move(mg.at[pl.ds(0, tp - 1)], y_send.at[0], y_recv.at[0], at_y(1)).wait_send()


def body(tp, inputs, norm_gain, query_weight, key_weight, value_weight, query_gain, key_gain, out_weight):
    batch, length, model = inputs.shape
    share, groups, heads, width = query_weight.shape
    span = model // tp
    rows = 2 * length
    bf16 = jnp.bfloat16
    dma = pltpu.SemaphoreType.DMA
    operands = (
        inputs,
        norm_gain.reshape(1, model),
        query_weight,
        key_weight,
        value_weight,
        out_weight.transpose(0, 2, 1),
        query_gain,
        key_gain,
    )
    return pl.pallas_call(
        functools.partial(layer_kernel, tp, batch, length),
        out_shape=jax.ShapeDtypeStruct((batch, length, span), bf16),
        in_specs=[pl.BlockSpec(memory_space=pltpu.HBM)] * len(operands),
        out_specs=pl.BlockSpec(memory_space=pl.ANY),
        scratch_shapes=[
            *[pltpu.VMEM(operand.shape, operand.dtype) for operand in operands],
            pltpu.VMEM((heads, share, 384 + WB), bf16),
            pltpu.VMEM((CHIPS, 2, share, 128), bf16),
            pltpu.VMEM((CHIPS, 2, share, 256), bf16),
            pltpu.VMEM((CHIPS, 2, share, WB), bf16),
            pltpu.VMEM((model, 384), bf16),
            pltpu.VMEM((model, WB), bf16),
            pltpu.VMEM((batch, 2, length, model), bf16),
            *[pltpu.VMEM((batch, rows + 2 * r, 128), bf16) for r in REACH],
            pltpu.VMEM((groups, batch, rows, 128), bf16),
            pltpu.VMEM((2, length, length + 2 * REACH[0]), jnp.float32),
            *[pltpu.VMEM((rows, rows + 2 * r), jnp.float32) for r in REACH[1:]],
            pltpu.VMEM((tp, span, 128), bf16),
            pltpu.VMEM((model, 128), bf16),
            pltpu.VMEM((model, 128), bf16),
            pltpu.VMEM((tp, span, 128), bf16),
            pltpu.VMEM((batch, 2, length, 128), bf16),
            pltpu.VMEM((batch, length, 128), bf16),
            pltpu.VMEM((tp, batch, length, 128), bf16),
            dma((len(operands),)),
            dma((1,)),
            dma((1,)),
            dma((1,)),
            dma((3,)),
            dma((3, 8)),
            dma((3,)),
            dma((3, 10)),
            dma((3,)),
            dma((1,)),
            dma((1,)),
            dma((groups,)),
            dma((batch, groups)),
            dma((1,)),
            dma((1,)),
            dma((1,)),
            dma((1,)),
            dma((1,)),
            dma((batch,)),
            dma((1,)),
            dma((batch,)),
            pltpu.VMEM((batch, length, span), bf16),
            dma((1,)),
        ],
        compiler_params=pltpu.CompilerParams(collective_id=0, has_side_effects=True, vmem_limit_bytes=24 * 1024 * 1024),
        name="layer",
    )(*[pltpu.with_memory_space_constraint(operand, pltpu.HBM) for operand in operands])


def solution(mesh):
    in_specs = (
        P(None, "sp", None),
        P(),
        P("sp", None, "tp", None),
        P("sp", None, "tp", None),
        P("sp", None, "tp", None),
        P(),
        P(),
        P("tp", None, "sp"),
    )
    out_specs = P(None, "sp", "tp")
    run = functools.partial(body, mesh.shape["tp"])
    return jax.shard_map(run, mesh=mesh, in_specs=in_specs, out_specs=out_specs, check_vma=False)
```

```python
import functools
import math

import jax
import jax.numpy as jnp
from jax import lax
from jax.experimental import pallas as pl
from jax.experimental.pallas import tpu as pltpu
from jax.sharding import PartitionSpec as P

FOLDED = (2,)
GAPS = ((1, 32), (4, 32), (16, 16))
REACH = tuple(d * h for d, h in GAPS)
EPS = 1e-06
NEG = -1e30
LOG2E = 1.4426950408889634
MESH = pl.DeviceIdType.MESH
NZ, NX = 16, 4
CHIPS = NZ * NX
WB = 256


def layer_kernel(
    tp, batch, length, x_hbm, gain_hbm, qw_hbm, kw_hbm, vw_hbm, ow_hbm, qg_hbm, kg_hbm, out_ref,
    x_ref, gain_ref, qw_ref, kw_ref, vw_ref, ow_ref, qg_ref, kg_ref, slab_ref,
    w2, w01, wb, wk, wq, nb, win0, win1, win2, qn, bias0, bias1, bias2, osum, oown, orecv, wo, mboth, mrecv, mg,
    in_sem, pair_send, pair_recv, local_sem, out_sem, zh_recv, xh_recv, za_recv, xa_recv,
    nb_send, nb_recv, halo_send, halo_recv,
    o_send, o_recv, oy_send, oy_recv, m_send, m_recv, y_send, y_recv, outs, out_move,
):
    me = lax.axis_index("sp")
    mine = lax.axis_index("tp")
    groups = len(GAPS)
    core = me % 2
    other = 1 - core
    chip = me // 2
    x = chip % NX
    z = chip // NX
    rows = 2 * length
    wins = (win0, win1, win2)
    biases = (bias0, bias1, bias2)
    bufs = (w2, w01, wb)

    def at_z(offset, on=core):
        return {"sp": (((z + offset + NZ) % NZ) * NX + x) * 2 + on}

    def at_x(offset, on=core):
        return {"sp": (z * NX + (x + offset) % NX) * 2 + on}

    sibling = {"sp": chip * 2 + other}

    def at_chip(offset):
        return {"sp": ((chip + offset + CHIPS) % CHIPS) * 2 + core}

    def at_y(offset):
        return {"tp": (mine + offset) % tp}

    barrier = pltpu.get_barrier_semaphore()

    def greet(target):
        pl.semaphore_signal(barrier, inc=1, device_id=target, device_id_type=MESH)

    targets = [at_z(o) for o in (-4, 4, -3, 3, -2, 2, -1, 1)] + [at_y(o) for o in range(1, tp)]
    targets += [at_x(o) for o in range(1, NX)] + [at_chip(1), at_chip(-1), sibling]
    targets += [at_x(2, other)]
    targets += [at_z(o, other) for o in (-4, 4, -3, 3, -2, 2, -1, 1)]
    for target in targets:
        greet(target)

    fetches = [
        pltpu.make_async_copy(src, dst, in_sem.at[i])
        for i, (src, dst) in enumerate(
            (
                (qw_hbm, qw_ref),
                (kw_hbm, kw_ref),
                (vw_hbm, vw_ref),
                (ow_hbm, ow_ref),
                (qg_hbm, qg_ref),
                (kg_hbm, kg_ref),
                (gain_hbm, gain_ref),
                (x_hbm, x_ref),
            )
        )
    ]
    for fetch in fetches:
        fetch.start()
    for fetch in fetches[:4]:
        fetch.wait()
    for head in range(2):
        pieces = []
        for group in (2, 0, 1):
            pieces += [kw_ref[:, group, head, :], vw_ref[:, group, head, :]]
        pieces += [qw_ref[:, group, head, :] for group in range(groups)]
        pieces = [piece.astype(jnp.float32) for piece in pieces + [ow_ref[head]]]
        slab_ref[head] = jnp.concatenate(pieces, axis=1).astype(jnp.bfloat16)

    pl.semaphore_wait(barrier, len(targets))

    cuts = (pl.ds(0, 128), pl.ds(128, 256), pl.ds(384, WB))

    def pair(chunk):
        return pltpu.make_async_remote_copy(
            src_ref=slab_ref.at[other, :, cuts[chunk]],
            dst_ref=bufs[chunk].at[chip, core],
            send_sem=pair_send.at[0],
            recv_sem=pair_recv.at[0],
            device_id=sibling,
            device_id_type=MESH,
        )

    def local(chunk):
        return pltpu.make_async_copy(
            slab_ref.at[core, :, cuts[chunk]], bufs[chunk].at[chip, core], local_sem.at[0]
        )

    def index_of(origin, column):
        return ((z + origin + NZ) % NZ) * NX + (x + column) % NX

    def move(block, send_sem, recv_sem, target, land=None):
        return pltpu.make_async_remote_copy(
            src_ref=block,
            dst_ref=block if land is None else land,
            send_sem=send_sem,
            recv_sem=recv_sem,
            device_id=target,
            device_id_type=MESH,
        )

    def zh_start(chunk, step):
        for on in (core, other):
            move(
                slab_ref.at[on, :, cuts[chunk]],
                out_sem.at[chunk],
                zh_recv.at[chunk, 3 - step if step < 0 else step - 1],
                at_z(step, on),
                bufs[chunk].at[chip, core],
            ).start()

    def zh_wait(chunk, origin):
        block = bufs[chunk].at[index_of(origin, 0)]
        slot = 3 + origin if origin > 0 else -origin - 1
        move(block, out_sem.at[chunk], zh_recv.at[chunk, slot], at_z(1)).wait_recv()

    def xh_start(chunk):
        for on in (core, other):
            move(
                slab_ref.at[on, :, cuts[chunk]],
                out_sem.at[chunk],
                xh_recv.at[chunk],
                at_x(2, on),
                bufs[chunk].at[chip, core],
            ).start()

    def xh_wait(chunk):
        move(bufs[chunk].at[index_of(0, 2)], out_sem.at[chunk], xh_recv.at[chunk], at_x(1)).wait_recv()

    def slot_of(rel, fold):
        if fold == 0:
            return rel - 5
        return {4: 7, NZ - 4: 8}.get(rel, 9)

    def za_start(chunk, origin, step, fold=0):
        slot = slot_of((origin - step) % NZ, fold)
        block = bufs[chunk].at[index_of(origin, 2 * fold)]
        move(block, out_sem.at[chunk], za_recv.at[chunk, slot], at_z(step)).start()

    def za_wait(chunk, origin, fold=0):
        block = bufs[chunk].at[index_of(origin, 2 * fold)]
        move(block, out_sem.at[chunk], za_recv.at[chunk, slot_of(origin % NZ, fold)], at_z(1)).wait_recv()

    def shifts(chunk):
        return (1, 3) if chunk in FOLDED else (2, 1, 3)

    def xa_start(chunk, origin):
        block = bufs[chunk].at[index_of(origin, 0)]
        for shift in shifts(chunk):
            move(block, out_sem.at[chunk], xa_recv.at[chunk], at_x(shift)).start()

    far = {4: ((-3, -1, -2), (-4, -3, -1, -2)), -4: ((4, 3, 1, 2), (3, 1, 2))}

    for step in (4, -4, 3, -3, 1, -1, 2, -2):
        zh_start(0, step)
    for steps in ((4, -4), (1, -1, 2, -2, 3, -3)):
        for chunk in (1, 2):
            for step in steps:
                zh_start(chunk, step)
    for chunk in FOLDED:
        xh_start(chunk)
    for chunk in range(3):
        local(chunk).start()
        pair(chunk).start()

    def nb_copy(b):
        return move(nb.at[b, core], nb_send.at[0], nb_recv.at[0], sibling)

    def norm_step(b, carry):
        flat = x_ref[b].astype(jnp.float32)
        scale = lax.rsqrt(jnp.mean(flat * flat, axis=-1, keepdims=True) + EPS)
        nb[b, core] = (flat * scale * gain_ref[...]).astype(jnp.bfloat16)
        nb_copy(b).start()
        return carry

    for fetch in fetches[4:]:
        fetch.wait()
    lax.fori_loop(0, batch, norm_step, 0)

    pair_all = move(slab_ref.at[0], pair_send.at[0], pair_recv.at[0], sibling)
    pltpu.make_async_copy(slab_ref.at[0], slab_ref.at[1], local_sem.at[0]).wait()
    pair_all.wait_recv()
    for chunk in range(3):
        xa_start(chunk, 0)

    def near(chunk, spread):
        for origin in (1, -1, 2, -2):
            zh_wait(chunk, origin)
            if spread:
                xa_start(chunk, origin)
        for origin in (4, -4):
            zh_wait(chunk, origin)
            for step in far[origin][chunk % 2]:
                za_start(chunk, origin, step)
        for origin in (3, -3):
            zh_wait(chunk, origin)
            if spread:
                xa_start(chunk, origin)
        if spread:
            for origin in (4, -4):
                xa_start(chunk, origin)

    near(0, True)
    for chunk in FOLDED:
        xh_wait(chunk)
        for step in (4, -4, 3, -3, 1, -1, 2, -2):
            za_start(chunk, 0, step, 1)
    near(1, True)
    near(2, True)

    head = mine * 2 + core
    heads = 2 * tp
    power = -8.0 * (head + 1).astype(jnp.float32) / heads
    slope = jnp.exp2(jnp.full((8, 128), power, jnp.float32))[:1, :1] * LOG2E
    total_rows = CHIPS * rows

    def bias_of(group, count, first):
        dilation, half = GAPS[group]
        reach = REACH[group]
        shape = (count, count + 2 * reach)
        key = lax.broadcasted_iota(jnp.int32, shape, 1) - reach
        offset = jnp.abs(key - lax.broadcasted_iota(jnp.int32, shape, 0))
        at = key + (chip * rows + first)
        allowed = (offset <= reach) & (at >= 0) & (at < total_rows) & ((offset & (dilation - 1)) == 0)
        return jnp.where(allowed, offset.astype(jnp.float32) * (-slope / float(reach)), NEG)

    for block in range(2):
        bias0[block] = bias_of(0, length, block * length)
    for group in (1, 2):
        biases[group][...] = bias_of(group, rows, 0)

    late = (5, -5, 6, -6, 7, -7, 8)
    def fold_on(chunk):
        for origin in (4, -4):
            za_wait(chunk, origin, 1)
            for step in far[origin][1 - chunk % 2]:
                za_start(chunk, origin, step, 1)

    def late_on(chunk, part):
        for origin in part:
            za_wait(chunk, origin)
            xa_start(chunk, origin)

    late_on(0, late[:4])
    for chunk in FOLDED:
        fold_on(chunk)
    late_on(0, late[4:])
    late_on(1, late)
    late_on(2, late)

    lane = lax.broadcasted_iota(jnp.int32, (rows, 128), 1)
    low = lane < 64
    origins = (0, 1, -1, 2, -2, 3, -3, 4, -4) + late

    def all_blocks(chunk):
        several = bufs[chunk].at[pl.ds(0, NZ * len(shifts(chunk)))]
        move(several, out_sem.at[chunk], xa_recv.at[chunk], at_x(1)).wait_recv()
        if chunk in FOLDED:
            several = bufs[chunk].at[pl.ds(0, NZ - 3)]
            move(several, out_sem.at[chunk], za_recv.at[chunk, 9], at_x(1)).wait_recv()

    def sent_all(chunk):
        move(bufs[chunk].at[pl.ds(0, CHIPS - 1)], out_sem.at[chunk], xa_recv.at[chunk], at_x(1)).wait_send()

    all_blocks(0)
    wk[:, :128] = w2[...].reshape(wk.shape[0], 128)
    nb_all = move(nb.at[:, 0], nb_send.at[0], nb_recv.at[0], sibling)
    nb_all.wait_recv()

    def halo(b, group, up):
        reach = REACH[group]
        begin_at, land_at = (rows, 0) if up else (reach, reach + rows)
        return pltpu.make_async_remote_copy(
            src_ref=wins[group].at[b, pl.ds(begin_at, reach), :],
            dst_ref=wins[group].at[b, pl.ds(land_at, reach), :],
            send_sem=halo_send.at[group],
            recv_sem=halo_recv.at[b, group],
            device_id=at_chip(1 if up else -1),
            device_id_type=MESH,
        )

    def halo_wait(b, only=(2, 1, 0)):
        for group in only:
            both = wins[group].at[b, pl.ds(0, 2 * REACH[group]), :]
            move(both, halo_send.at[group], halo_recv.at[b, group], at_chip(1)).wait_recv()

    ones = jnp.ones((1, 64), jnp.float32)
    zeros = jnp.zeros((1, 64), jnp.float32)

    def key_norm(out, place, group):
        seg = out[:, 128 * place : 128 * (place + 1)].astype(jnp.bfloat16).astype(jnp.float32)
        mean = jnp.sum(jnp.where(low, seg * seg, 0.0), axis=-1, keepdims=True) / 64.0
        gain = jnp.concatenate([kg_ref[group : group + 1, :], ones], axis=1)
        return (seg * jnp.where(low, lax.rsqrt(mean + EPS), 1.0) * gain).astype(jnp.bfloat16)

    def key_step(b, first, order):
        out = jnp.dot(nb[b].reshape(rows, -1), wk[:, first : first + 128 * len(order)], preferred_element_type=jnp.float32)
        for place, group in enumerate(order):
            wins[group][b, REACH[group] : REACH[group] + rows, :] = key_norm(out, place, group)
        for group in order:
            for up in (True, False):
                if group != 2:
                    halo(b, group, up).start()
                elif b < 2:

                    @pl.when(x != (NX - 1 if up else 0))
                    def _(up=up):
                        halo(b, 2, up).start()

    for b in range(batch):
        key_step(b, 0, (2,))
    all_blocks(1)
    sent_all(2)

    for up in (True, False):

        @pl.when(x == (NX - 1 if up else 0))
        def _(up=up):
            for b in range(2):
                halo(b, 2, up).start()

    wk[:, 128:] = w01[...].reshape(wk.shape[0], 256)
    for b in range(batch):
        key_step(b, 128, (0, 1))
        if 1 <= b < batch - 1:
            for up in (True, False):
                halo(b + 1, 2, up).start()

    all_blocks(2)
    wq[...] = wb[...].reshape(wq.shape)

    tile = wq[:, 128:].astype(jnp.float32)
    high = lax.broadcasted_iota(jnp.int32, tile.shape, 1) >= 64
    tile = jnp.where(high, tile, 0.0)
    tile = jnp.where(core == 0, pltpu.roll(tile, 64, 1), tile)
    oown[...] = tile.astype(jnp.bfloat16)
    o_pair = pltpu.make_async_remote_copy(
        src_ref=oown,
        dst_ref=orecv,
        send_sem=o_send.at[0],
        recv_sem=o_recv.at[0],
        device_id=sibling,
        device_id_type=MESH,
    )
    o_pair.start()

    factor = LOG2E / 8.0

    def q_step(b, carry):
        out = jnp.dot(nb[b].reshape(rows, -1), wq[...], preferred_element_type=jnp.float32)
        out = out.astype(jnp.bfloat16).astype(jnp.float32)
        first, second = out[:, :128], out[:, 128:]
        for group, seg, here in ((0, first, low), (1, first, ~low), (2, second, low)):
            mean = jnp.sum(jnp.where(here, seg * seg, 0.0), axis=-1, keepdims=True) / 64.0
            gain = qg_ref[group : group + 1, :] * factor
            gain = jnp.concatenate([zeros, gain] if group == 1 else [gain, zeros], axis=1)
            scaled = jnp.where(here, seg * lax.rsqrt(mean + EPS) * gain, 0.0)
            if group == 1:
                scaled = pltpu.roll(scaled, 64, 1)
            qn[group, b] = scaled.astype(jnp.bfloat16)
        return carry

    for i in range(batch):
        q_step(i, 0)

    span = wo.shape[1]
    o_pair.wait_recv()
    osum[...] = (oown[...] + orecv[...]).reshape(osum.shape)
    wo[mine] = osum[mine]

    def o_copy(shift):
        return move(osum.at[(mine + shift) % tp], oy_send.at[0], oy_recv.at[0], at_y(shift), wo.at[mine])

    o_all = move(wo.at[pl.ds(0, tp - 1)], oy_send.at[0], oy_recv.at[0], at_y(1))

    for shift in range(1, tp):
        o_copy(shift).start()

    def merge(total, summed):
        merged = jnp.where(lax.broadcasted_iota(jnp.int32, summed.shape, 1) >= 64, summed / total, 0.0)
        return jnp.where(core == 0, pltpu.roll(merged, 64, 1), merged).astype(jnp.bfloat16)

    def close_part(b, block):
        begin = block * length if isinstance(block, int) else pl.multiple_of(block * length, length)
        window = win0[b, pl.ds(begin, length + 2 * REACH[0]), :]
        query = qn[0, b, pl.ds(begin, length), :]
        scores = lax.dot_general(query, window, (((1,), (1,)), ((), ())), preferred_element_type=jnp.float32)
        grown = jnp.exp2(scores + bias0[block])
        total = jnp.sum(grown, axis=-1, keepdims=True)
        return total, jnp.dot(grown.astype(jnp.bfloat16), window, preferred_element_type=jnp.float32)

    def wide_part(b, group, begin, count):
        window = wins[group][b, pl.ds(begin, count + 2 * REACH[group]), :]
        query = qn[group, b, pl.ds(begin, count), :]
        scores = lax.dot_general(query, window, (((1,), (1,)), ((), ())), preferred_element_type=jnp.float32)
        first = begin if isinstance(begin, int) else pl.multiple_of(begin, length)
        bias = biases[group][pl.ds(0, count), pl.ds(0, count + 2 * REACH[group])]
        if count != rows:
            bias = biases[group][pl.ds(first, count), pl.ds(first, count + 2 * REACH[group])]
        grown = jnp.exp2(scores + bias)
        total = jnp.sum(grown, axis=-1, keepdims=True)
        return total, jnp.dot(grown.astype(jnp.bfloat16), window, preferred_element_type=jnp.float32)

    def attend(b):
        total, summed = wide_part(b, 2, 0, rows)
        for part_total, part_sum in [
            wide_part(b, 1, 0, rows),
            [jnp.concatenate(both, axis=0) for both in zip(close_part(b, 0), close_part(b, 1))],
        ]:
            total, summed = total + part_total, summed + part_sum
        mboth[b] = merge(total, summed).reshape(2, length, 128)

    def attend_block(b, block, total, summed):
        begin = pl.multiple_of(block * length, length)
        for part_total, part_sum in (wide_part(b, 1, begin, length), close_part(b, block)):
            total, summed = total + part_total, summed + part_sum
        mboth[b, block] = merge(total, summed)

    def m_copy(b):
        return move(mboth.at[b, other], m_send.at[0], m_recv.at[b], sibling, mrecv.at[b])

    def y_copy(b, shift):
        return move(mg.at[mine, b], y_send.at[0], y_recv.at[b], at_y(shift))

    def y_wait(b):
        move(mg.at[pl.ds(0, tp - 1), b], y_send.at[0], y_recv.at[b], at_y(1)).wait_recv()

    def pass_on(b):
        m_copy(b).wait_recv()
        mg[mine, b] = mboth[b, core] + mrecv[b]
        for shift in (2, 1, 3):
            y_copy(b, shift).start()

    def attend_step(i, carry):
        b = i
        halo_wait(b)
        attend(b)
        m_copy(b).start()

        @pl.when(i >= 1)
        def _():
            pass_on(i - 1)

        return carry

    lax.fori_loop(0, batch - 1, attend_step, 0)
    last = batch - 1
    halo_wait(last, (2,))
    far_parts = [wide_part(last, 2, pl.multiple_of(block * length, length), length) for block in (other, core)]
    pass_on(last - 1)
    halo_wait(last, (1, 0))
    attend_block(last, other, *far_parts[0])
    m_copy(last).start()
    attend_block(last, core, *far_parts[1])
    pass_on(batch - 1)
    o_all.wait_recv()

    def out_copy(b):
        return pltpu.make_async_copy(outs.at[b], out_ref.at[b], out_move.at[0])

    def finish(b, carry):
        y_wait(b)
        final = jnp.zeros((length, span), jnp.float32)
        for part in range(tp):
            final = final + lax.dot_general(
                mg[part, b], wo[part], (((1,), (1,)), ((), ())), preferred_element_type=jnp.float32
            )
        outs[b] = final.astype(jnp.bfloat16)
        out_copy(b).start()
        return carry

    lax.fori_loop(0, batch, finish, 0)
    pltpu.make_async_copy(outs, out_ref, out_move.at[0]).wait()
    pair_all.wait_send()
    for chunk in range(2):
        sent_all(chunk)
    nb_all.wait_send()
    for group in range(groups):
        both = wins[group].at[:, pl.ds(0, 2 * REACH[group]), :]
        move(both, halo_send.at[group], halo_recv.at[0, group], at_chip(1)).wait_send()
    o_pair.wait_send()
    o_all.wait_send()
    move(mrecv, m_send.at[0], m_recv.at[0], sibling).wait_send()
    move(mg.at[pl.ds(0, tp - 1)], y_send.at[0], y_recv.at[0], at_y(1)).wait_send()


def body(tp, inputs, norm_gain, query_weight, key_weight, value_weight, query_gain, key_gain, out_weight):
    batch, length, model = inputs.shape
    share, groups, heads, width = query_weight.shape
    span = model // tp
    rows = 2 * length
    bf16 = jnp.bfloat16
    dma = pltpu.SemaphoreType.DMA
    operands = (
        inputs,
        norm_gain.reshape(1, model),
        query_weight,
        key_weight,
        value_weight,
        out_weight.transpose(0, 2, 1),
        query_gain,
        key_gain,
    )
    return pl.pallas_call(
        functools.partial(layer_kernel, tp, batch, length),
        out_shape=jax.ShapeDtypeStruct((batch, length, span), bf16),
        in_specs=[pl.BlockSpec(memory_space=pltpu.HBM)] * len(operands),
        out_specs=pl.BlockSpec(memory_space=pl.ANY),
        scratch_shapes=[
            *[pltpu.VMEM(operand.shape, operand.dtype) for operand in operands],
            pltpu.VMEM((heads, share, 384 + WB), bf16),
            pltpu.VMEM((CHIPS, 2, share, 128), bf16),
            pltpu.VMEM((CHIPS, 2, share, 256), bf16),
            pltpu.VMEM((CHIPS, 2, share, WB), bf16),
            pltpu.VMEM((model, 384), bf16),
            pltpu.VMEM((model, WB), bf16),
            pltpu.VMEM((batch, 2, length, model), bf16),
            *[pltpu.VMEM((batch, rows + 2 * r, 128), bf16) for r in REACH],
            pltpu.VMEM((groups, batch, rows, 128), bf16),
            pltpu.VMEM((2, length, length + 2 * REACH[0]), jnp.float32),
            *[pltpu.VMEM((rows, rows + 2 * r), jnp.float32) for r in REACH[1:]],
            pltpu.VMEM((tp, span, 128), bf16),
            pltpu.VMEM((model, 128), bf16),
            pltpu.VMEM((model, 128), bf16),
            pltpu.VMEM((tp, span, 128), bf16),
            pltpu.VMEM((batch, 2, length, 128), bf16),
            pltpu.VMEM((batch, length, 128), bf16),
            pltpu.VMEM((tp, batch, length, 128), bf16),
            dma((len(operands),)),
            dma((1,)),
            dma((1,)),
            dma((1,)),
            dma((3,)),
            dma((3, 8)),
            dma((3,)),
            dma((3, 10)),
            dma((3,)),
            dma((1,)),
            dma((1,)),
            dma((groups,)),
            dma((batch, groups)),
            dma((1,)),
            dma((1,)),
            dma((1,)),
            dma((1,)),
            dma((1,)),
            dma((batch,)),
            dma((1,)),
            dma((batch,)),
            pltpu.VMEM((batch, length, span), bf16),
            dma((1,)),
        ],
        compiler_params=pltpu.CompilerParams(collective_id=0, has_side_effects=True, vmem_limit_bytes=24 * 1024 * 1024),
        name="layer",
    )(*[pltpu.with_memory_space_constraint(operand, pltpu.HBM) for operand in operands])


def solution(mesh):
    in_specs = (
        P(None, "sp", None),
        P(),
        P("sp", None, "tp", None),
        P("sp", None, "tp", None),
        P("sp", None, "tp", None),
        P(),
        P(),
        P("tp", None, "sp"),
    )
    out_specs = P(None, "sp", "tp")
    run = functools.partial(body, mesh.shape["tp"])
    return jax.shard_map(run, mesh=mesh, in_specs=in_specs, out_specs=out_specs, check_vma=False)
```
